128 devices in a mesh: ep: 16 (over z, x), tp: 8 (over y, core).
Axes of the slice: x: 4, y: 4, z: 4, core: 2. Of those that a mesh axis runs over, the one named last changes fastest.
Arguments:
- residual: bfloat16 [2048, 2048], P('ep', 'tp'), may hold values from -61 to 61
- in_gain: float32 [2048], replicated, may hold values from 0.1 to 1.9
- in_weight: bfloat16 [2048, 1024], P(None, 'tp'), may hold values from -0.125 to 0.125
- state: float32 [2, 2048, 4096], P(None, 'ep', 'tp'), may hold values from -3 to 3
- decay_rate: float32 [64, 64], P('tp'), may hold values from 0.1 to 1
- frequency: float32 [64, 64], P('tp'), may hold values from 0 to 200
- log_step: float32 [64], P('tp'), may hold values from -3 to -0.7
- in_coef: float32 [2, 64, 64, 16], P(None, 'tp'), may hold values from -1 to 1
- out_coef: float32 [2, 64, 16, 64], P(None, 'tp'), may hold values from -0.75 to 0.75
- skip_gain: float32 [1024], P('tp'), may hold values from -3 to 3
- out_weight: bfloat16 [1024, 2048], replicated, may hold values from -0.1875 to 0.1875
- mid_gain: float32 [2048], replicated, may hold values from 0.1 to 1.9
- gate_vector: bfloat16 [2048], replicated, may hold values from -0.125 to 0.125
- routes: int32 [2048, 4], P('ep'), may hold values from 0 to 127, all different within a row; in each aligned block of 128 rows (0 to 127, 128 to 255, ...) at most 8 rows name the same one
- route_weight: float32 [2048, 4], P('ep'), may hold values from 0.1 to 1
- expert_gate: bfloat16 [128, 2048, 512], P(('ep', 'tp')), may hold values from -0.125 to 0.125
- expert_up: bfloat16 [128, 2048, 512], P(('ep', 'tp')), may hold values from -0.125 to 0.125
- expert_down: bfloat16 [128, 512, 2048], P(('ep', 'tp')), may hold values from -0.25 to 0.25
- shared_gate: bfloat16 [2048, 4096], P(None, 'ep'), may hold values from -0.125 to 0.125
- shared_up: bfloat16 [2048, 4096], P(None, 'ep'), may hold values from -0.125 to 0.125
- shared_down: bfloat16 [4096, 2048], P('ep'), may hold values from -0.09375 to 0.09375
Outputs:
- layer_out: bfloat16 [2048, 2048], P(('ep', 'tp'))
- new_state: float32 [2, 2048, 4096], P(None, 'ep', 'tp')
The draws below stay inside these ranges and needn't reach their ends.
Inputs may be any that keep to these rules, and one draw needn't show every extreme that they name: `routes`: each row names 4 different experts. Among the rows of one index of ep no expert is named more than 8 times, a bound that some block reaches.
All inputs are finite; a program needn't handle non-finite values.
Results may differ from the reference program's by a relative error of at most 0.0085.
Values may be sent and summed in bfloat16 or wider, within the bound.
A program may use at most 128 MiB of HBM per device.

```python
import math
import jax
import jax.numpy as jnp
import numpy as np
from jax import lax

D = 2048
SW = 1024
GROUP_CH = 16
STATE = 64
GROUPS = 64
GS = 4096
FF = 512
SFF = 4096
TOP = 4
SEQ_DEV = 128
SEQS = 2048
EXPERTS = 128
CAP = 8
N_EP = 16


def draw_residual(key, part):
    first_key, second_key = jax.random.split(jax.random.fold_in(key, 11))
    columns = jnp.arange(D, dtype=jnp.float32)
    col_scale = 10.0 ** (columns / D - 0.5)
    row_scale = 10.0 ** jax.random.uniform(second_key, (SEQS, 1), jnp.float32, -0.5, 0.5)
    base_draw = jnp.clip(jax.random.normal(first_key, (SEQS, D), jnp.float32), -6.0, 6.0)
    return (base_draw * col_scale * row_scale).astype(jnp.bfloat16)


def levels(stream_key, shape, cuts, low, high):
    def one(axis_at, blocks):
        draws = jax.random.uniform(jax.random.fold_in(jax.random.fold_in(stream_key, 6), axis_at), (blocks,), jnp.float32, low / len(cuts), high / len(cuts))
        return jnp.repeat(jnp.exp(draws), shape[axis_at] // blocks).reshape((-1,) + (1,) * (len(shape) - axis_at - 1))

    gain = one(*cuts[0])
    for cut in cuts[1:]:
        gain = gain * one(*cut)
    return gain


def deal_out(stream_key, own, number, rows, number_of, top, most, slope):
    order = jax.random.permutation(stream_key, number_of)
    crowded, common = load_shares(number_of, rows * top, most, slope, True), load_shares(number_of, rows * top, most, slope, False)
    places = jnp.arange(number_of)

    def named(sizes, offset_by):
        used = int((sizes > 0).sum())
        fixed = max(1, used // 4)
        moved = fixed + (places - fixed + offset_by * (used - fixed)) % max(1, number_of - fixed)
        return jnp.zeros((number_of,), jnp.int32).at[order[jnp.where(places < fixed, places, moved)]].set(jnp.asarray(sizes, jnp.int32))

    sizes = jnp.where(number % 4 == 0, named(crowded, number // 4), named(common, number - number // 4 - 1))
    mixed = jax.random.permutation(jax.random.fold_in(own, 3), number_of)
    giver, receiver = mixed[0:number_of // 2 * 2:2], mixed[1:number_of // 2 * 2:2]
    room = jnp.minimum(sizes[giver] - 1, most - sizes[receiver]) // 2
    room = jnp.where((giver == order[0]) | (receiver == order[0]) | (sizes[receiver] == 0), 0, jnp.maximum(room, 0))
    moved = jax.random.randint(jax.random.fold_in(own, 4), (number_of // 2,), 0, 1 << 20) % (room + 1)
    sizes = sizes.at[giver].add(-moved).at[receiver].add(moved)
    labels = jnp.searchsorted(jnp.cumsum(sizes), jnp.arange(rows * top), side="right").astype(jnp.int32)
    grid = labels.reshape(top, rows).T
    grid = grid[jax.random.permutation(jax.random.fold_in(own, 1), rows)]
    offset_by = jax.random.randint(jax.random.fold_in(own, 2), (rows, 1), 0, top)
    return jnp.take_along_axis(grid, (jnp.arange(top)[None, :] + offset_by) % top, axis=1)


def load_shares(amount, total, bound, lean, full):
    loads = [(1 << 20) // math.isqrt(standing ** lean) + 1 for standing in range(1, amount + 1)]
    largest = bound if full else min(bound, max(-(-total // amount), total * loads[0] // sum(loads)))
    least = 1 if total - largest >= amount - 1 else 0
    holding, spare = [largest] + [least] * (amount - 1), total - largest - least * (amount - 1)
    while spare > 0:
        free = [i for i in range(1, amount) if holding[i] < largest] or [i for i in range(1, amount) if holding[i] < bound]
        pool, left = sum([loads[i] for i in free]), spare
        for i in free:
            extra = min(bound - holding[i], max(1, left * loads[i] // pool), spare)
            holding[i] = holding[i] + extra
            spare = spare - extra
    return np.array(holding)


def noise(stream_key, dims, deviation, limit, pieces=(), kind=jnp.bfloat16):
    drawn = deviation * jax.random.normal(stream_key, dims, jnp.float32)
    if pieces:
        drawn = drawn * levels(stream_key, dims, pieces, -0.22, 0.18)
    return jnp.clip(drawn, -limit, limit).astype(kind)


def setup_inputs(seed: int = 0) -> dict:
    seeds = jax.random.split(jax.random.key(seed), 22)
    residual = draw_residual(jax.random.fold_in(seeds[21], 71), 0)
    in_gain = jnp.clip(1.0 + 0.18 * jax.random.normal(seeds[1], (D,), jnp.float32), 0.1, 1.9)
    in_weight = noise(seeds[2], (D, SW), D ** -0.5, 0.125, ((1, 8),))
    state = noise(seeds[3], (2, SEQS, GS), 0.5, 3.0, ((1, 16), (2, 8)), jnp.float32)
    decay_rate = jnp.clip(jnp.exp(math.log(1.0) - 2.3025851 * jax.random.uniform(seeds[4], (GROUPS, STATE), jnp.float32) ** levels(seeds[4], (GROUPS, STATE), ((0, 8),), -0.2, 0.2)), 0.1, 1.0)
    frequency = jnp.clip(200.0 * jax.random.uniform(seeds[5], (GROUPS, STATE), jnp.float32) ** levels(seeds[5], (GROUPS, STATE), ((0, 8),), -0.2, 0.2), 0.0, 200.0)
    log_step = jnp.clip(-3.0 + 2.3 * jax.random.uniform(seeds[6], (GROUPS,), jnp.float32) ** levels(seeds[6], (GROUPS,), ((0, 8),), -0.2, 0.2), -3.0, -0.7)
    in_coef = noise(seeds[7], (2, GROUPS, STATE, GROUP_CH), (2 * GROUP_CH) ** -0.5, 1.0, ((1, 8),), jnp.float32)
    out_coef = noise(seeds[8], (2, GROUPS, GROUP_CH, STATE), STATE ** -0.5, 0.75, ((1, 8),), jnp.float32)
    skip_gain = noise(seeds[9], (SW,), 0.5, 3.0, ((0, 8),), jnp.float32)
    out_weight = noise(seeds[10], (SW, D), SW ** -0.5, 0.1875)
    mid_gain = jnp.clip(1.0 + 0.18 * jax.random.normal(seeds[11], (D,), jnp.float32), 0.1, 1.9)
    gate_vector = noise(seeds[12], (D,), D ** -0.5, 0.125)
    routes_keys = jax.random.split(jax.random.fold_in(seeds[13], 1), SEQS // SEQ_DEV)
    routes_turns = jax.random.permutation(jax.random.fold_in(seeds[13], 3), SEQS // SEQ_DEV)
    routes = jax.vmap(lambda own, number: deal_out(jax.random.fold_in(seeds[13], 2), own, number, SEQ_DEV, EXPERTS, TOP, CAP, 2))(routes_keys, routes_turns).reshape((SEQS, TOP))
    route_weight = jnp.clip(jnp.exp(math.log(1.0) - 2.3025851 * jax.random.uniform(seeds[14], (SEQS, TOP), jnp.float32) ** levels(seeds[14], (SEQS, TOP), ((0, 16),), -0.2, 0.2)), 0.1, 1.0)
    expert_gate = noise(seeds[15], (EXPERTS, D, FF), D ** -0.5, 0.125, ((0, 128),))
    expert_up = noise(seeds[16], (EXPERTS, D, FF), D ** -0.5, 0.125, ((0, 128),))
    expert_down = noise(seeds[17], (EXPERTS, FF, D), FF ** -0.5, 0.25, ((0, 128),))
    shared_gate = noise(seeds[18], (D, SFF), D ** -0.5, 0.125, ((1, 16),))
    shared_up = noise(seeds[19], (D, SFF), D ** -0.5, 0.125, ((1, 16),))
    shared_down = noise(seeds[20], (SFF, D), SFF ** -0.5, 0.09375, ((0, 16),))
    return dict(residual=residual, in_gain=in_gain, in_weight=in_weight, state=state, decay_rate=decay_rate, frequency=frequency, log_step=log_step, in_coef=in_coef, out_coef=out_coef, skip_gain=skip_gain, out_weight=out_weight, mid_gain=mid_gain, gate_vector=gate_vector, routes=routes, route_weight=route_weight, expert_gate=expert_gate, expert_up=expert_up, expert_down=expert_down, shared_gate=shared_gate, shared_up=shared_up, shared_down=shared_down)


norm_eps = 1e-05
routed_scale = 2.5

def layer_norm(values, gain_vec):
    row_mean = lax.optimization_barrier(jnp.mean(values, axis=-1, keepdims=True))
    row_square = lax.optimization_barrier(jnp.mean(values * values, axis=-1, keepdims=True))
    return (values - row_mean) * lax.rsqrt(row_square - row_mean * row_mean + norm_eps) * gain_vec.astype(jnp.float32)

def coefficients(decay_rate, frequency, log_step, in_coef):
    time_step = jnp.exp(log_step)[:, None]
    real_rate = -decay_rate
    magnitude = jnp.exp(real_rate * time_step)
    keep_re = magnitude * jnp.cos(frequency * time_step)
    keep_im = magnitude * jnp.sin(frequency * time_step)
    denominator = real_rate * real_rate + frequency * frequency
    factor_re = ((keep_re - 1.0) * real_rate + keep_im * frequency) / denominator
    factor_im = (keep_im * real_rate - (keep_re - 1.0) * frequency) / denominator
    push_re = factor_re[..., None] * in_coef[0] - factor_im[..., None] * in_coef[1]
    push_im = factor_re[..., None] * in_coef[1] + factor_im[..., None] * in_coef[0]
    return (keep_re, keep_im, push_re, push_im)

def mixer_step(normed, in_weight, state, decay_rate, frequency, log_step, in_coef, out_coef, skip_gain):
    row_count = normed.shape[0]
    group_count, state_count = decay_rate.shape
    keep_re, keep_im, push_re, push_im = coefficients(decay_rate, frequency, log_step, in_coef)
    drive = jnp.dot(normed, in_weight, preferred_element_type=jnp.float32).astype(jnp.bfloat16)
    drive_f = drive.astype(jnp.float32).reshape(row_count, group_count, -1)
    highest = lax.Precision.HIGHEST
    input_re = jnp.einsum('tgh,gph->tgp', drive_f, push_re, precision=highest)
    input_im = jnp.einsum('tgh,gph->tgp', drive_f, push_im, precision=highest)
    old_re = state[0].reshape(row_count, group_count, state_count)
    old_im = state[1].reshape(row_count, group_count, state_count)
    new_re = keep_re * old_re - keep_im * old_im + input_re
    new_im = keep_re * old_im + keep_im * old_re + input_im
    read_out = jnp.einsum('ghp,tgp->tgh', out_coef[0], new_re, precision=highest) - jnp.einsum('ghp,tgp->tgh', out_coef[1], new_im, precision=highest)
    read_out = read_out.reshape(row_count, -1) + skip_gain * drive_f.reshape(row_count, -1)
    mixed_rows = jax.nn.gelu(read_out, approximate=True).astype(jnp.bfloat16)
    updated = jnp.stack([new_re.reshape(row_count, -1), new_im.reshape(row_count, -1)])
    return (mixed_rows, updated)

def route_slots(routes, experts):
    flat_routes = routes.reshape(-1)
    onehot = (flat_routes[:, None] == jnp.arange(experts, dtype=jnp.int32)[None, :]).astype(jnp.int32)
    before = jnp.cumsum(onehot, axis=0) - onehot
    return lax.optimization_barrier(jnp.sum(before * onehot, axis=1)).reshape(routes.shape)

def expert_block(row_block, gate_weight, up_weight, down_weight):
    gate_part = jnp.dot(row_block, gate_weight, preferred_element_type=jnp.float32)
    up_part = jnp.dot(row_block, up_weight, preferred_element_type=jnp.float32)
    hidden = (jax.nn.silu(gate_part) * up_part).astype(jnp.bfloat16)
    return jnp.dot(hidden, down_weight, preferred_element_type=jnp.float32).astype(jnp.bfloat16)

def reference(residual, in_gain, in_weight, state, decay_rate, frequency, log_step, in_coef, out_coef, skip_gain, out_weight, mid_gain, gate_vector, routes, route_weight, expert_gate, expert_up, expert_down, shared_gate, shared_up, shared_down):
    resid_f = residual.astype(jnp.float32)
    normed = layer_norm(resid_f, in_gain).astype(jnp.bfloat16)
    mixed_rows, new_state = mixer_step(normed, in_weight, state, decay_rate, frequency, log_step, in_coef, out_coef, skip_gain)
    after_mix = resid_f + jnp.dot(mixed_rows, out_weight, preferred_element_type=jnp.float32)
    normed_mid = layer_norm(after_mix, mid_gain).astype(jnp.bfloat16)
    slot_rank = jax.vmap(route_slots, in_axes=(0, None))(routes.reshape(N_EP, SEQ_DEV, TOP), EXPERTS).reshape(SEQS, TOP)
    group_of = (jnp.arange(SEQS, dtype=jnp.int32) // SEQ_DEV)[:, None]
    slot_place = routes * (N_EP * CAP) + group_of * CAP + slot_rank
    token_ids = jnp.broadcast_to(jnp.arange(SEQS, dtype=jnp.int32)[:, None], slot_place.shape)
    slot_token = jnp.zeros((EXPERTS * N_EP * CAP,), jnp.int32).at[slot_place.reshape(-1)].set(token_ids.reshape(-1))
    buffer = normed_mid[slot_token].reshape(EXPERTS, N_EP * CAP, D)
    outputs = lax.map(lambda packed: expert_block(*packed), (buffer, expert_gate, expert_up, expert_down)).reshape(EXPERTS * N_EP * CAP, D)
    weights = route_weight / lax.optimization_barrier(jnp.sum(route_weight, axis=-1, keepdims=True)) * routed_scale
    routed = lax.optimization_barrier(jnp.sum(weights[..., None] * outputs[slot_place].astype(jnp.float32), axis=1))
    gate_part = jnp.dot(normed_mid, shared_gate, preferred_element_type=jnp.float32)
    up_part = jnp.dot(normed_mid, shared_up, preferred_element_type=jnp.float32)
    shared_hidden = (jax.nn.silu(gate_part) * up_part).astype(jnp.bfloat16)
    shared = jnp.dot(shared_hidden, shared_down, preferred_element_type=jnp.float32)
    gate_value = jax.nn.sigmoid(jnp.dot(normed_mid, gate_vector, preferred_element_type=jnp.float32))
    layer_out = (after_mix + routed + gate_value[:, None] * shared).astype(jnp.bfloat16)
    return (layer_out, new_state)
```

```python
import jax
import jax.numpy as jnp
from jax import lax
from jax.experimental import pallas as pl
from jax.experimental.pallas import tpu as pltpu
from jax.sharding import PartitionSpec as P

MESH = pl.DeviceIdType.MESH
norm_eps = 1e-05
routed_scale = 2.5
f32, bf16 = jnp.float32, jnp.bfloat16

TP, EP = 8, 16
ROWS, WIDTH, FEAT = 128, 2048, 256
CH, GROUPS, STATE, GCH = 128, 8, 64, 16
GS = GROUPS * STATE
CAP, OWN = 8, 16
SLOTS = EP * CAP
FF, SF = 512, 256
MIX = CH * TP


def dot(a, b):
    return jnp.dot(a, b, preferred_element_type=f32)


def dot_nt(a, b):
    return lax.dot_general(a, b, (((1,), (1,)), ((), ())), preferred_element_type=f32)


def dot_tn(a, b):
    return lax.dot_general(a, b, (((0,), (0,)), ((), ())), preferred_element_type=f32)


def halves(a):
    high = a.astype(bf16)
    return high, (a - high.astype(f32)).astype(bf16)


def lanes_of_groups(a):
    return jnp.concatenate([a[g : g + 1, :] for g in range(GROUPS)], axis=1)


def block_diagonal(a):
    wide = jnp.concatenate([a] * GROUPS, axis=1)
    row = lax.broadcasted_iota(jnp.int32, (CH, GS), 0) // GCH
    col = lax.broadcasted_iota(jnp.int32, (CH, GS), 1) // STATE
    return jnp.where(row == col, wide, 0.0)


def per_group_rows(a):
    return jnp.broadcast_to(a[:, None, :], (GROUPS, GCH, STATE)).reshape(CH, STATE)


def kernel(
    resid_ref, in_gain_ref, in_w_hbm, state_hbm, decay_ref, freq_ref, step_ref, in_coef_ref,
    out_coef_ref, skip_ref, out_w_hbm, mid_gain_ref, gate_vec_ref, routes_ref, weights_ref,
    eg_hbm, eu_hbm, ed_hbm, sg_hbm, su_hbm, sd_hbm,
    out_ref, new_state_hbm,
    full, in_w, state, new_state, out_w, eg, eu, ed, sg, su, sd,
    mixed, after, mid, outgoing, slots_in, rows_in, hidden, result, returned,
    shidden, partial, partial_in, routed_part, routed_in,
    local_sem, out_sem, s1, r1, s2, r2, s3, r3, s4, r4, s5, r5, s6, r6, s7, r7,
):
    e = lax.axis_index("ep")
    t = lax.axis_index("tp")
    tp_peers = [(d, (e, lax.rem(t + d, TP))) for d in range(1, TP)]
    ep_peers = [(d, (lax.rem(e + d, EP), t)) for d in range(1, EP)]

    barrier = pltpu.get_barrier_semaphore()
    for _, dev in tp_peers + ep_peers:
        pl.semaphore_signal(barrier, inc=1, device_id=dev, device_id_type=MESH)

    fetches = {}
    for i, (name, src, dst) in enumerate([
        ("in_w", in_w_hbm, in_w), ("state", state_hbm, state), ("out_w", out_w_hbm, out_w),
        ("eg", eg_hbm, eg), ("eu", eu_hbm, eu), ("ed", ed_hbm, ed),
        ("sg", sg_hbm, sg), ("su", su_hbm, su), ("sd", sd_hbm, sd),
    ]):
        fetches[name] = pltpu.make_async_copy(src, dst, local_sem.at[i])
        fetches[name].start()

    def send(src, dst, ss, rs, d, dev):
        return pltpu.make_async_remote_copy(
            src_ref=src, dst_ref=dst, send_sem=ss.at[d - 1], recv_sem=rs.at[d - 1],
            device_id=dev, device_id_type=MESH,
        )

    row8 = lax.broadcasted_iota(jnp.int32, (GROUPS, STATE), 0)
    log_step = jnp.zeros((GROUPS, STATE), f32)
    for g in range(GROUPS):
        log_step = jnp.where(row8 == g, step_ref[g], log_step)
    dt = jnp.exp(log_step)
    rate = -decay_ref[...]
    freq = freq_ref[...]
    magnitude = jnp.exp(rate * dt)
    keep_re = magnitude * jnp.cos(freq * dt)
    keep_im = magnitude * jnp.sin(freq * dt)
    denominator = rate * rate + freq * freq
    factor_re = ((keep_re - 1.0) * rate + keep_im * freq) / denominator
    factor_im = (keep_im * rate - (keep_re - 1.0) * freq) / denominator
    fr, fi = per_group_rows(factor_re), per_group_rows(factor_im)
    push_re = block_diagonal(fr * in_coef_ref[0] - fi * in_coef_ref[1])
    push_im = block_diagonal(fr * in_coef_ref[1] + fi * in_coef_ref[0])
    pr_hi, pr_lo = halves(push_re)
    pi_hi, pi_lo = halves(push_im)
    out_re = block_diagonal(out_coef_ref[0]).astype(bf16)
    out_im = block_diagonal(out_coef_ref[1]).astype(bf16)
    kr, ki = lanes_of_groups(keep_re), lanes_of_groups(keep_im)

    slot_row = lax.broadcasted_iota(jnp.int32, (SLOTS, ROWS), 0)
    expert = (slot_row // CAP) * TP + t
    weight_sum = jnp.sum(weights_ref[...], axis=0, keepdims=True)
    weights = weights_ref[...] / weight_sum * routed_scale
    chosen = jnp.zeros((SLOTS, ROWS), f32)
    chosen_weight = jnp.zeros((SLOTS, ROWS), f32)
    for k in range(4):
        same = routes_ref[k : k + 1, :] == expert
        chosen = jnp.where(same, 1.0, chosen)
        chosen_weight = jnp.where(same, weights[k : k + 1, :], chosen_weight)
    earlier = (
        lax.broadcasted_iota(jnp.int32, (ROWS, ROWS), 0)
        < lax.broadcasted_iota(jnp.int32, (ROWS, ROWS), 1)
    )
    before = dot(chosen.astype(bf16), jnp.where(earlier, 1.0, 0.0).astype(bf16))
    rank = (slot_row % CAP).astype(f32)
    holds = (chosen > 0.5) & (before == rank)
    pick = jnp.where(holds, 1.0, 0.0).astype(bf16)
    combine = jnp.where(holds, chosen_weight, 0.0).T
    comb_hi, comb_lo = halves(combine)

    pl.semaphore_wait(barrier, TP - 1 + EP - 1)

    cols = pl.ds(pl.multiple_of(t * FEAT, FEAT), FEAT)
    phase1 = [send(resid_ref, full.at[:, cols], s1, r1, d, dev) for d, dev in tp_peers]
    for c in phase1:
        c.start()
    full[:, cols] = resid_ref[...]
    fetches["state"].wait()
    old_re, old_im = state[0], state[1]
    new_state[0] = kr * old_re - ki * old_im
    new_state[1] = kr * old_im + ki * old_re
    fetches["in_w"].wait()
    for c in phase1:
        c.wait_recv()
    values = full[...].astype(f32)
    mean = jnp.sum(values, axis=1, keepdims=True) * (1.0 / WIDTH)
    square = jnp.sum(values * values, axis=1, keepdims=True) * (1.0 / WIDTH)
    scale = lax.rsqrt(square - mean * mean + norm_eps)
    normed = ((values - mean) * scale * in_gain_ref[...]).astype(bf16)
    drive = dot(normed, in_w[...]).astype(bf16)
    new_re = new_state[0] + (dot(drive, pr_hi) + dot(drive, pr_lo))
    new_im = new_state[1] + (dot(drive, pi_hi) + dot(drive, pi_lo))
    new_state[0] = new_re
    new_state[1] = new_im
    read = dot_nt(new_re.astype(bf16), out_re) - dot_nt(new_im.astype(bf16), out_im)
    read = read + skip_ref[...] * drive.astype(f32)
    mixed_cols = pl.ds(pl.multiple_of(t * CH, CH), CH)
    mixed[:, mixed_cols] = jax.nn.gelu(read, approximate=True).astype(bf16)

    phase2 = [send(mixed.at[:, mixed_cols], mixed.at[:, mixed_cols], s2, r2, d, dev) for d, dev in tp_peers]
    for c in phase2:
        c.start()
    state_out = pltpu.make_async_copy(new_state, new_state_hbm, out_sem)
    state_out.start()
    fetches["out_w"].wait()
    for c in phase2:
        c.wait_recv()

    def mix_columns(j, carry):
        at = pl.ds(pl.multiple_of(j * 256, 256), 256)
        part = full[:, at].astype(f32) + dot(mixed[...], out_w[:, at])
        after[:, at] = part
        return (
            carry[0] + part[:, :128] + part[:, 128:],
            carry[1] + part[:, :128] * part[:, :128] + part[:, 128:] * part[:, 128:],
        )

    zero = jnp.zeros((ROWS, 128), f32)
    total, squares = lax.fori_loop(0, WIDTH // 256, mix_columns, (zero, zero))
    mean = jnp.sum(total, axis=1, keepdims=True) * (1.0 / WIDTH)
    square = jnp.sum(squares, axis=1, keepdims=True) * (1.0 / WIDTH)
    scale = lax.rsqrt(square - mean * mean + norm_eps)

    def norm_columns(j, carry):
        at = pl.ds(pl.multiple_of(j * 256, 256), 256)
        part = ((after[:, at] - mean) * scale * mid_gain_ref[:, at]).astype(bf16)
        mid[:, :, at] = part.reshape(TP, OWN, 256)
        outgoing[:, :, at] = dot(pick, part).astype(bf16).reshape(EP, CAP, 256)
        return carry

    lax.fori_loop(0, WIDTH // 256, norm_columns, 0)

    phase3 = [send(outgoing.at[dev[0]], slots_in.at[e], s3, r3, d, dev) for d, dev in ep_peers]
    phase4 = [send(mid.at[t], rows_in.at[e], s4, r4, d, dev) for d, dev in ep_peers]
    for c in phase3:
        c.start()
    for c in phase4:
        c.start()
    slots_in[e] = outgoing[e]
    own_mid = mid[t]
    rows_in[e] = own_mid
    gate_value = jax.nn.sigmoid(
        jnp.sum(own_mid.astype(f32) * gate_vec_ref[...].astype(f32), axis=1, keepdims=True)
    )

    for name in ("eg", "eu", "ed"):
        fetches[name].wait()
    for c in phase3:
        c.wait_recv()
    rows = slots_in[...].reshape(SLOTS, WIDTH)
    for j in range(FF // 256):
        at = pl.ds(j * 256, 256)
        gate_part = dot(rows, eg[:, at])
        up_part = dot(rows, eu[:, at])
        hidden[:, at] = (jax.nn.silu(gate_part) * up_part).astype(bf16)

    def down_columns(j, carry):
        at = pl.ds(pl.multiple_of(j * 256, 256), 256)
        result[:, :, at] = dot(hidden[...], ed[:, at]).astype(bf16).reshape(EP, CAP, 256)
        return carry

    lax.fori_loop(0, WIDTH // 256, down_columns, 0)
    phase5 = [send(result.at[dev[0]], returned.at[e], s5, r5, d, dev) for d, dev in ep_peers]
    for c in phase5:
        c.start()
    returned[e] = result[e]

    for name in ("sg", "su", "sd"):
        fetches[name].wait()
    for c in phase4:
        c.wait_recv()
    piece = rows_in[...].reshape(EP * OWN, WIDTH)
    gate_part = dot(piece, sg[...])
    up_part = dot(piece, su[...])
    shidden[...] = (jax.nn.silu(gate_part) * up_part).astype(bf16)

    def shared_columns(j, carry):
        at = pl.ds(pl.multiple_of(j * 256, 256), 256)
        partial[:, :, at] = dot(shidden[...], sd[:, at]).astype(bf16).reshape(EP, OWN, 256)
        return carry

    lax.fori_loop(0, WIDTH // 256, shared_columns, 0)
    phase6 = [send(partial.at[dev[0]], partial_in.at[e], s6, r6, d, dev) for d, dev in ep_peers]
    for c in phase6:
        c.start()
    partial_in[e] = partial[e]

    for c in phase5:
        c.wait_recv()

    def combine_columns(j, carry):
        at = pl.ds(pl.multiple_of(j * 256, 256), 256)
        back = returned[:, :, at].reshape(SLOTS, 256)
        part = dot(comb_hi, back) + dot(comb_lo, back)
        routed_part[:, :, at] = part.astype(bf16).reshape(TP, OWN, 256)
        return carry

    lax.fori_loop(0, WIDTH // 256, combine_columns, 0)
    phase7 = [send(routed_part.at[dev[1]], routed_in.at[t], s7, r7, d, dev) for d, dev in tp_peers]
    for c in phase7:
        c.start()
    routed_in[t] = routed_part[t]
    for c in phase7:
        c.wait_recv()
    for c in phase6:
        c.wait_recv()

    own_rows = pl.ds(pl.multiple_of(t * OWN, OWN), OWN)
    routed = jnp.sum(routed_in[...].astype(f32), axis=0)
    shared = jnp.sum(partial_in[...].astype(f32), axis=0)
    out_ref[...] = (after[own_rows, :] + routed + gate_value * shared).astype(bf16)

    for c in phase1 + phase2 + phase3 + phase4 + phase5 + phase6 + phase7:
        c.wait_send()
    state_out.wait()


def per_device(
    residual, in_gain, in_weight, state, decay_rate, frequency, log_step, in_coef, out_coef,
    skip_gain, out_weight, mid_gain, gate_vector, routes, route_weight, expert_gate, expert_up,
    expert_down, shared_gate, shared_up, shared_down,
):
    vmem = pl.BlockSpec(memory_space=pltpu.VMEM)
    smem = pl.BlockSpec(memory_space=pltpu.SMEM)
    hbm = pl.BlockSpec(memory_space=pl.ANY)
    dma = pltpu.SemaphoreType.DMA
    in_coef_rows = jnp.swapaxes(in_coef, 2, 3).reshape(2, CH, STATE)
    out_coef_rows = out_coef.reshape(2, CH, STATE)
    return pl.pallas_call(
        kernel,
        name="layer_step",
        out_shape=(
            jax.ShapeDtypeStruct((OWN, WIDTH), bf16),
            jax.ShapeDtypeStruct((2, ROWS, GS), f32),
        ),
        in_specs=[
            vmem, vmem, hbm, hbm, vmem, vmem, smem, vmem, vmem, vmem, hbm, vmem, vmem, vmem, vmem,
            hbm, hbm, hbm, hbm, hbm, hbm,
        ],
        out_specs=(vmem, hbm),
        scratch_shapes=[
            pltpu.VMEM((ROWS, WIDTH), bf16),
            pltpu.VMEM((WIDTH, CH), bf16),
            pltpu.VMEM((2, ROWS, GS), f32),
            pltpu.VMEM((2, ROWS, GS), f32),
            pltpu.VMEM((MIX, WIDTH), bf16),
            pltpu.VMEM((WIDTH, FF), bf16),
            pltpu.VMEM((WIDTH, FF), bf16),
            pltpu.VMEM((FF, WIDTH), bf16),
            pltpu.VMEM((WIDTH, SF), bf16),
            pltpu.VMEM((WIDTH, SF), bf16),
            pltpu.VMEM((SF, WIDTH), bf16),
            pltpu.VMEM((ROWS, MIX), bf16),
            pltpu.VMEM((ROWS, WIDTH), f32),
            pltpu.VMEM((TP, OWN, WIDTH), bf16),
            pltpu.VMEM((EP, CAP, WIDTH), bf16),
            pltpu.VMEM((EP, CAP, WIDTH), bf16),
            pltpu.VMEM((EP, OWN, WIDTH), bf16),
            pltpu.VMEM((SLOTS, FF), bf16),
            pltpu.VMEM((EP, CAP, WIDTH), bf16),
            pltpu.VMEM((EP, CAP, WIDTH), bf16),
            pltpu.VMEM((EP * OWN, SF), bf16),
            pltpu.VMEM((EP, OWN, WIDTH), bf16),
            pltpu.VMEM((EP, OWN, WIDTH), bf16),
            pltpu.VMEM((TP, OWN, WIDTH), bf16),
            pltpu.VMEM((TP, OWN, WIDTH), bf16),
            dma((9,)), dma,
            dma((TP - 1,)), dma((TP - 1,)),
            dma((TP - 1,)), dma((TP - 1,)),
            dma((EP - 1,)), dma((EP - 1,)),
            dma((EP - 1,)), dma((EP - 1,)),
            dma((EP - 1,)), dma((EP - 1,)),
            dma((EP - 1,)), dma((EP - 1,)),
            dma((TP - 1,)), dma((TP - 1,)),
        ],
        compiler_params=pltpu.CompilerParams(
            collective_id=0, has_side_effects=True, vmem_limit_bytes=60 * 1024 * 1024
        ),
    )(
        residual, in_gain.reshape(1, WIDTH), in_weight, state, decay_rate, frequency, log_step,
        in_coef_rows, out_coef_rows, skip_gain.reshape(1, CH), out_weight,
        mid_gain.reshape(1, WIDTH), gate_vector.reshape(1, WIDTH), routes.T, route_weight.T,
        expert_gate[0], expert_up[0], expert_down[0], shared_gate, shared_up, shared_down,
    )


def solution(mesh):
    return jax.shard_map(
        per_device,
        mesh=mesh,
        in_specs=(
            P("ep", "tp"), P(), P(None, "tp"), P(None, "ep", "tp"), P("tp", None), P("tp", None),
            P("tp"), P(None, "tp", None, None), P(None, "tp", None, None), P("tp"), P(), P(), P(),
            P("ep", None), P("ep", None), P(("ep", "tp"), None, None), P(("ep", "tp"), None, None),
            P(("ep", "tp"), None, None), P(None, "ep"), P(None, "ep"), P("ep", None),
        ),
        out_specs=(P(("ep", "tp"), None), P(None, "ep", "tp")),
        check_vma=False,
    )
```

```python
import jax
import jax.numpy as jnp
from jax import lax
from jax.experimental import pallas as pl
from jax.experimental.pallas import tpu as pltpu
from jax.sharding import PartitionSpec as P

MESH = pl.DeviceIdType.MESH
norm_eps = 1e-05
routed_scale = 2.5
f32, bf16 = jnp.float32, jnp.bfloat16

TP, EP = 8, 16
ROWS, WIDTH, FEAT = 128, 2048, 256
CH, GROUPS, STATE, GCH = 128, 8, 64, 16
GS = GROUPS * STATE
CAP, OWN = 8, 16
SIDE = 4
HALF = WIDTH // 2
SLOTS = EP * CAP
FF, SF = 512, 256
MIX = CH * TP
VMEM_MIB = 48


def dot(a, b):
    return jnp.dot(a, b, preferred_element_type=f32)


def dot_nt(a, b):
    return lax.dot_general(a, b, (((1,), (1,)), ((), ())), preferred_element_type=f32)


def dot_tn(a, b):
    return lax.dot_general(a, b, (((0,), (0,)), ((), ())), preferred_element_type=f32)


def halves(a):
    high = a.astype(bf16)
    return high, (a - high.astype(f32)).astype(bf16)


def lanes_of_groups(a):
    return jnp.concatenate([a[g : g + 1, :] for g in range(GROUPS)], axis=1)


def block_diagonal(a):
    wide = jnp.concatenate([a] * GROUPS, axis=1)
    row = lax.broadcasted_iota(jnp.int32, (CH, GS), 0) // GCH
    col = lax.broadcasted_iota(jnp.int32, (CH, GS), 1) // STATE
    return jnp.where(row == col, wide, 0.0)


def per_group_rows(a):
    return jnp.broadcast_to(a[:, None, :], (GROUPS, GCH, STATE)).reshape(CH, STATE)


def kernel(
    resid_hbm, in_gain_hbm, in_w_hbm, state_hbm, decay_hbm, freq_hbm, step_hbm, in_coef_hbm,
    out_coef_hbm, skip_hbm, out_w_hbm, mid_gain_hbm, gate_vec_hbm, routes_hbm, weights_hbm,
    eg_hbm, eu_hbm, ed_hbm, sg_hbm, su_hbm, sd_hbm,
    out_ref, new_state_ref,
    resid_ref, in_gain_ref, decay_ref, freq_ref, step_ref, in_coef_ref, out_coef_ref, skip_ref,
    mid_gain_ref, gate_vec_ref, routes_ref, weights_ref,
    full, in_w, state, out_w, eg, eu, ed, sg, su, sd,
    mixed, after, mid, outgoing, slots_in, rows_in, hidden, result, returned,
    shidden, partial, stage_a, stage_b, sum_a, sum_b, final_a, final_b, routed_part, routed_in,
    local_sem, s1, r1, s2, r2, s3, r3, s4, r4, s4f, r4f, s5, r5, s6, r6, s6f, r6f, s7, r7,
):
    e = lax.axis_index("ep")
    t = lax.axis_index("tp")
    z, x = e // SIDE, e % SIDE
    y, core = t // 2, t % 2
    tp_peers = [
        (dy * 2 + dc, (e, ((y + dy) % SIDE) * 2 + (core + dc) % 2))
        for dy in (1, 3, 2, 0) for dc in (0, 1) if dy + dc
    ]
    ep_peers = [
        (dz * SIDE + dx, (((z + dz) % SIDE) * SIDE + (x + dx) % SIDE, t))
        for dz in range(SIDE) for dx in range(SIDE) if dz + dx
    ]
    x_peers = [(d, (z * SIDE + (x + d) % SIDE, t), (x + d) % SIDE) for d in (1, 3, 2)]
    z_peers = [(d, (((z + d) % SIDE) * SIDE + x, t), (z + d) % SIDE) for d in (1, 3, 2)]

    barrier = pltpu.get_barrier_semaphore()
    for _, dev in tp_peers + ep_peers:
        pl.semaphore_signal(barrier, inc=1, device_id=dev, device_id_type=MESH)

    fetches = {}
    for i, (name, src, dst) in enumerate([
        ("resid", resid_hbm, resid_ref), ("decay", decay_hbm, decay_ref),
        ("freq", freq_hbm, freq_ref), ("step", step_hbm, step_ref),
        ("in_coef", in_coef_hbm, in_coef_ref), ("out_coef", out_coef_hbm, out_coef_ref),
        ("routes", routes_hbm, routes_ref), ("weights", weights_hbm, weights_ref),
        ("skip", skip_hbm, skip_ref), ("in_gain", in_gain_hbm, in_gain_ref),
        ("state", state_hbm, state), ("in_w", in_w_hbm, in_w),
        ("mid_gain", mid_gain_hbm, mid_gain_ref), ("gate_vec", gate_vec_hbm, gate_vec_ref),
        ("out_w", out_w_hbm, out_w),
        ("eg", eg_hbm, eg), ("eu", eu_hbm, eu), ("ed", ed_hbm, ed),
        ("sg", sg_hbm, sg), ("su", su_hbm, su), ("sd", sd_hbm, sd),
    ]):
        fetches[name] = pltpu.make_async_copy(src, dst, local_sem.at[i])
        fetches[name].start()

    def fetched(*names):
        for name in names:
            fetches[name].wait()

    def send(src, dst, ss, rs, d, dev):
        return pltpu.make_async_remote_copy(
            src_ref=src, dst_ref=dst, send_sem=ss.at[d], recv_sem=rs.at[d],
            device_id=dev, device_id_type=MESH,
        )

    fetched("decay", "freq", "step", "in_coef", "out_coef")
    own_lane = (
        lax.broadcasted_iota(jnp.int32, (GROUPS, GROUPS), 0)
        == lax.broadcasted_iota(jnp.int32, (GROUPS, GROUPS), 1)
    )
    log_step = jnp.sum(jnp.where(own_lane, step_ref[...], 0.0), axis=1, keepdims=True)
    dt = jnp.exp(log_step)
    rate = -decay_ref[...]
    freq = freq_ref[...]
    magnitude = jnp.exp(rate * dt)
    keep_re = magnitude * jnp.cos(freq * dt)
    keep_im = magnitude * jnp.sin(freq * dt)
    denominator = rate * rate + freq * freq
    factor_re = ((keep_re - 1.0) * rate + keep_im * freq) / denominator
    factor_im = (keep_im * rate - (keep_re - 1.0) * freq) / denominator
    fr, fi = per_group_rows(factor_re), per_group_rows(factor_im)
    push_re = block_diagonal(fr * in_coef_ref[0] - fi * in_coef_ref[1])
    push_im = block_diagonal(fr * in_coef_ref[1] + fi * in_coef_ref[0])
    pr_hi, pr_lo = halves(push_re)
    pi_hi, pi_lo = halves(push_im)
    out_re = block_diagonal(out_coef_ref[0]).astype(bf16)
    out_im = block_diagonal(out_coef_ref[1]).astype(bf16)
    kr, ki = lanes_of_groups(keep_re), lanes_of_groups(keep_im)

    fetched("routes", "weights")
    slot_row = lax.broadcasted_iota(jnp.int32, (SLOTS, ROWS), 0)
    expert = (slot_row // CAP) * TP + t
    weight_sum = jnp.sum(weights_ref[...], axis=0, keepdims=True)
    weights = weights_ref[...] / weight_sum * routed_scale
    chosen = jnp.zeros((SLOTS, ROWS), f32)
    chosen_weight = jnp.zeros((SLOTS, ROWS), f32)
    for k in range(4):
        same = routes_ref[k : k + 1, :] == expert
        chosen = jnp.where(same, 1.0, chosen)
        chosen_weight = jnp.where(same, weights[k : k + 1, :], chosen_weight)
    earlier = (
        lax.broadcasted_iota(jnp.int32, (ROWS, ROWS), 0)
        < lax.broadcasted_iota(jnp.int32, (ROWS, ROWS), 1)
    )
    before = dot(chosen.astype(bf16), jnp.where(earlier, 1.0, 0.0).astype(bf16))
    rank = (slot_row % CAP).astype(f32)
    holds = (chosen > 0.5) & (before == rank)
    pick = jnp.where(holds, 1.0, 0.0).astype(bf16)
    combine = jnp.where(holds, chosen_weight, 0.0).T
    comb_hi, comb_lo = halves(combine)

    pl.semaphore_wait(barrier, TP - 1 + EP - 1)

    cols = pl.ds(pl.multiple_of(t * FEAT, FEAT), FEAT)
    fetched("resid")
    phase1 = [send(resid_ref, full.at[:, cols], s1, r1, d, dev) for d, dev in tp_peers]
    for c in phase1:
        c.start()
    full[:, cols] = resid_ref[...]
    fetched("state", "in_w", "in_gain", "skip")
    old_re, old_im = state[0], state[1]
    new_state_ref[0] = kr * old_re - ki * old_im
    new_state_ref[1] = kr * old_im + ki * old_re
    for c in phase1:
        c.wait_recv()
    values = full[...].astype(f32)
    mean = jnp.sum(values, axis=1, keepdims=True) * (1.0 / WIDTH)
    square = jnp.sum(values * values, axis=1, keepdims=True) * (1.0 / WIDTH)
    scale = lax.rsqrt(square - mean * mean + norm_eps)
    normed = ((values - mean) * scale * in_gain_ref[...]).astype(bf16)
    drive = dot(normed, in_w[...]).astype(bf16)
    new_re = new_state_ref[0] + (dot(drive, pr_hi) + dot(drive, pr_lo))
    new_im = new_state_ref[1] + (dot(drive, pi_hi) + dot(drive, pi_lo))
    new_state_ref[0] = new_re
    new_state_ref[1] = new_im
    read = dot_nt(new_re.astype(bf16), out_re) - dot_nt(new_im.astype(bf16), out_im)
    read = read + skip_ref[...] * drive.astype(f32)
    mixed_cols = pl.ds(pl.multiple_of(t * CH, CH), CH)
    mixed[:, mixed_cols] = jax.nn.gelu(read, approximate=True).astype(bf16)

    phase2 = [send(mixed.at[:, mixed_cols], mixed.at[:, mixed_cols], s2, r2, d, dev) for d, dev in tp_peers]
    for c in phase2:
        c.start()
    fetched("out_w", "mid_gain")
    arrivals = {d: c for (d, _), c in zip(tp_peers, phase2, strict=True)}
    sums = [jnp.zeros((ROWS, 128), f32), jnp.zeros((ROWS, 128), f32)]
    for dy in (0, 1, 3, 2):
        for dc in (0, 1):
            if dy + dc:
                arrivals[dy * 2 + dc].wait_recv()
        deep = pl.ds(pl.multiple_of(((y + SIDE - dy) % SIDE) * 256, 256), 256)
        block = mixed[:, deep]
        for j in range(WIDTH // 256):
            at = pl.ds(j * 256, 256)
            base = full[:, at].astype(f32) if dy == 0 else after[:, at]
            part = base + dot(block, out_w[deep, at])
            after[:, at] = part
            if dy == 2:
                for piece in (part[:, :128], part[:, 128:]):
                    sums[0] = sums[0] + piece
                    sums[1] = sums[1] + piece * piece
    mean = jnp.sum(sums[0], axis=1, keepdims=True) * (1.0 / WIDTH)
    square = jnp.sum(sums[1], axis=1, keepdims=True) * (1.0 / WIDTH)
    scale = lax.rsqrt(square - mean * mean + norm_eps)
    for j in range(WIDTH // 256):
        at = pl.ds(j * 256, 256)
        part = ((after[:, at] - mean) * scale * mid_gain_ref[:, at]).astype(bf16)
        mid[:, :, at] = part.reshape(TP, OWN, 256)
        outgoing[:, :, at] = dot(pick, part).astype(bf16).reshape(EP, CAP, 256)

    half_a, half_b = pl.ds(0, HALF), pl.ds(HALF, HALF)
    phase4 = []
    for k, (a, b) in enumerate(((half_a, half_b), (half_b, half_a))):
        for (d, dev, _), (_, dev_z, _) in zip(x_peers, z_peers, strict=True):
            phase4 += [
                send(mid.at[t, :, a], rows_in.at[e, :, a], s4, r4, k * 8 + d, dev),
                send(mid.at[t, :, b], rows_in.at[e, :, b], s4, r4, k * 8 + 4 + d, dev_z),
            ]
    phase3 = [send(outgoing.at[dev[0]], slots_in.at[e], s3, r3, d, dev) for d, dev in ep_peers]
    for c in phase4:
        c.start()
    for c in phase3:
        c.start()
    slots_in[e] = outgoing[e]
    own_mid = mid[t]
    rows_in[e] = own_mid
    fetched("gate_vec")
    gate_vec = jnp.concatenate([gate_vec_ref[i : i + 1, :] for i in range(WIDTH // 128)], axis=1)
    gate_value = jax.nn.sigmoid(
        jnp.sum(own_mid.astype(f32) * gate_vec.astype(f32), axis=1, keepdims=True)
    )
    forwards = []
    for i, d in enumerate((1, 3, 2)):
        phase4[2 * i].wait_recv()
        from_x = z * SIDE + (x + SIDE - d) % SIDE
        for dz, dev, _ in z_peers:
            block = rows_in.at[from_x, :, half_a]
            forwards.append(send(block, block, s4f, r4f, d * 4 + dz, dev))
            forwards[-1].start()
        phase4[2 * i + 1].wait_recv()
        from_z = ((z + SIDE - d) % SIDE) * SIDE + x
        for dx, dev, _ in x_peers:
            block = rows_in.at[from_z, :, half_b]
            forwards.append(send(block, block, s4f, r4f, 16 + d * 4 + dx, dev))
            forwards[-1].start()

    fetched("eg", "eu", "ed")
    for c in phase3:
        c.wait_recv()
    rows = slots_in[...].reshape(SLOTS, WIDTH)
    for j in range(FF // 256):
        at = pl.ds(j * 256, 256)
        gate_part = dot(rows, eg[:, at])
        up_part = dot(rows, eu[:, at])
        hidden[:, at] = (jax.nn.silu(gate_part) * up_part).astype(bf16)

    for j in range(WIDTH // 256):
        at = pl.ds(j * 256, 256)
        result[:, :, at] = dot(hidden[...], ed[:, at]).astype(bf16).reshape(EP, CAP, 256)

    phase5 = [send(result.at[dev[0]], returned.at[e], s5, r5, d, dev) for d, dev in ep_peers]
    for c in phase5:
        c.start()
    returned[e] = result[e]

    fetched("sg", "su", "sd")
    for c in phase4[6:] + forwards:
        c.wait_recv()
    piece = rows_in[...].reshape(EP * OWN, WIDTH)
    gate_part = dot(piece, sg[...])
    up_part = dot(piece, su[...])
    shidden[...] = (jax.nn.silu(gate_part) * up_part).astype(bf16)

    grid = (SIDE, SIDE, OWN)
    phase6 = []
    for half in (0, 1):
        for j in range(HALF // 256):
            at = pl.ds(half * HALF + j * 256, 256)
            partial[:, :, :, at] = dot(shidden[...], sd[:, at]).astype(bf16).reshape(*grid, 256)
        if half == 0:
            begun = [
                send(partial.at[there, :, :, half_a], stage_a.at[d - 1], s6, r6, d, dev)
                for d, dev, there in z_peers
            ]
        else:
            begun = [
                send(partial.at[:, there, :, half_b], stage_b.at[d - 1], s6, r6, 4 + d, dev)
                for d, dev, there in x_peers
            ]
        for c in begun:
            c.start()
        phase6 += begun

    for c in phase5:
        c.wait_recv()

    for j in range(WIDTH // 256):
        at = pl.ds(j * 256, 256)
        back = returned[:, :, at].reshape(SLOTS, 256)
        part = dot(comb_hi, back) + dot(comb_lo, back)
        routed_part[:, :, at] = part.astype(bf16).reshape(TP, OWN, 256)

    phase7 = [send(routed_part.at[dev[1]], routed_in.at[t], s7, r7, d, dev) for d, dev in tp_peers]
    for c in phase7:
        c.start()
    routed_in[t] = routed_part[t]
    for c in phase6[:3]:
        c.wait_recv()
    total = partial[z, :, :, half_a].astype(f32)
    for d in range(3):
        total = total + stage_a[d].astype(f32)
    sum_a[...] = total.astype(bf16)
    phase6f = [send(sum_a.at[there], final_a.at[d - 1], s6f, r6f, d, dev) for d, dev, there in x_peers]
    for c in phase6f:
        c.start()
    for c in phase6[3:]:
        c.wait_recv()
    total = partial[:, x, :, half_b].astype(f32)
    for d in range(3):
        total = total + stage_b[d].astype(f32)
    sum_b[...] = total.astype(bf16)
    begun = [send(sum_b.at[there], final_b.at[d - 1], s6f, r6f, 4 + d, dev) for d, dev, there in z_peers]
    for c in begun:
        c.start()
    phase6f += begun
    for c in phase7:
        c.wait_recv()
    own_rows = pl.ds(pl.multiple_of(t * OWN, OWN), OWN)
    routed = jnp.sum(routed_in[...].astype(f32), axis=0) + after[own_rows, :]
    for c in phase6f:
        c.wait_recv()
    for at, own, others in (
        (half_a, sum_a[x], final_a), (half_b, sum_b[z], final_b),
    ):
        shared = own.astype(f32) + jnp.sum(others[...].astype(f32), axis=0)
        begin = at.start
        out_ref[:, at] = (routed[:, begin : begin + HALF] + gate_value * shared).astype(bf16)

    everything = phase1 + phase2 + phase3 + phase4 + forwards + phase5 + phase6 + phase6f + phase7
    for c in everything:
        c.wait_send()


def per_device(
    residual, in_gain, in_weight, state, decay_rate, frequency, log_step, in_coef, out_coef,
    skip_gain, out_weight, mid_gain, gate_vector, routes, route_weight, expert_gate, expert_up,
    expert_down, shared_gate, shared_up, shared_down,
):
    vmem = pl.BlockSpec(memory_space=pltpu.VMEM)
    hbm = pl.BlockSpec(memory_space=pltpu.HBM)
    dma = pltpu.SemaphoreType.DMA
    in_coef_rows = jnp.swapaxes(in_coef, 2, 3).reshape(2, CH, STATE)
    out_coef_rows = out_coef.reshape(2, CH, STATE)
    call = pl.pallas_call(
        kernel,
        name="layer_step",
        out_shape=(
            pltpu.VMEM((OWN, WIDTH), bf16),
            pltpu.VMEM((2, ROWS, GS), f32),
        ),
        in_specs=[hbm] * 21,
        out_specs=(vmem, vmem),
        scratch_shapes=[
            pltpu.VMEM((ROWS, FEAT), bf16),
            pltpu.VMEM((1, WIDTH), f32),
            pltpu.VMEM((GROUPS, STATE), f32),
            pltpu.VMEM((GROUPS, STATE), f32),
            pltpu.VMEM((1, GROUPS), f32),
            pltpu.VMEM((2, CH, STATE), f32),
            pltpu.VMEM((2, CH, STATE), f32),
            pltpu.VMEM((1, CH), f32),
            pltpu.VMEM((1, WIDTH), f32),
            pltpu.VMEM((WIDTH // 128, 128), bf16),
            pltpu.VMEM((4, ROWS), jnp.int32),
            pltpu.VMEM((4, ROWS), f32),
            pltpu.VMEM((ROWS, WIDTH), bf16),
            pltpu.VMEM((WIDTH, CH), bf16),
            pltpu.VMEM((2, ROWS, GS), f32),
            pltpu.VMEM((MIX, WIDTH), bf16),
            pltpu.VMEM((WIDTH, FF), bf16),
            pltpu.VMEM((WIDTH, FF), bf16),
            pltpu.VMEM((FF, WIDTH), bf16),
            pltpu.VMEM((WIDTH, SF), bf16),
            pltpu.VMEM((WIDTH, SF), bf16),
            pltpu.VMEM((SF, WIDTH), bf16),
            pltpu.VMEM((ROWS, MIX), bf16),
            pltpu.VMEM((ROWS, WIDTH), f32),
            pltpu.VMEM((TP, OWN, WIDTH), bf16),
            pltpu.VMEM((EP, CAP, WIDTH), bf16),
            pltpu.VMEM((EP, CAP, WIDTH), bf16),
            pltpu.VMEM((EP, OWN, WIDTH), bf16),
            pltpu.VMEM((SLOTS, FF), bf16),
            pltpu.VMEM((EP, CAP, WIDTH), bf16),
            pltpu.VMEM((EP, CAP, WIDTH), bf16),
            pltpu.VMEM((EP * OWN, SF), bf16),
            pltpu.VMEM((SIDE, SIDE, OWN, WIDTH), bf16),
            pltpu.VMEM((SIDE - 1, SIDE, OWN, HALF), bf16),
            pltpu.VMEM((SIDE - 1, SIDE, OWN, HALF), bf16),
            pltpu.VMEM((SIDE, OWN, HALF), bf16),
            pltpu.VMEM((SIDE, OWN, HALF), bf16),
            pltpu.VMEM((SIDE - 1, OWN, HALF), bf16),
            pltpu.VMEM((SIDE - 1, OWN, HALF), bf16),
            pltpu.VMEM((TP, OWN, WIDTH), bf16),
            pltpu.VMEM((TP, OWN, WIDTH), bf16),
            dma((21,)),
            dma((TP,)), dma((TP,)),
            dma((TP,)), dma((TP,)),
            dma((EP,)), dma((EP,)),
            dma((16,)), dma((16,)),
            dma((32,)), dma((32,)),
            dma((EP,)), dma((EP,)),
            dma((8,)), dma((8,)),
            dma((8,)), dma((8,)),
            dma((TP,)), dma((TP,)),
        ],
        compiler_params=pltpu.CompilerParams(
            collective_id=0, has_side_effects=True, vmem_limit_bytes=VMEM_MIB * 1024 * 1024
        ),
    )
    operands = (
        residual, in_gain.reshape(1, WIDTH), in_weight, state, decay_rate, frequency,
        log_step.reshape(1, GROUPS), in_coef_rows, out_coef_rows, skip_gain.reshape(1, CH),
        out_weight, mid_gain.reshape(1, WIDTH), gate_vector.reshape(WIDTH // 128, 128), routes.T,
        route_weight.T, expert_gate[0], expert_up[0], expert_down[0], shared_gate, shared_up,
        shared_down,
    )
    return call(*[pltpu.with_memory_space_constraint(a, pltpu.HBM) for a in operands])


def solution(mesh):
    return jax.shard_map(
        per_device,
        mesh=mesh,
        in_specs=(
            P("ep", "tp"), P(), P(None, "tp"), P(None, "ep", "tp"), P("tp", None), P("tp", None),
            P("tp"), P(None, "tp", None, None), P(None, "tp", None, None), P("tp"), P(), P(), P(),
            P("ep", None), P("ep", None), P(("ep", "tp"), None, None), P(("ep", "tp"), None, None),
            P(("ep", "tp"), None, None), P(None, "ep"), P(None, "ep"), P("ep", None),
        ),
        out_specs=(P(("ep", "tp"), None), P(None, "ep", "tp")),
        check_vma=False,
    )
```

```python
import jax
import jax.numpy as jnp
from jax import lax
from jax.experimental import pallas as pl
from jax.experimental.pallas import tpu as pltpu
from jax.sharding import PartitionSpec as P

MESH = pl.DeviceIdType.MESH
norm_eps = 1e-05
routed_scale = 2.5
f32, bf16 = jnp.float32, jnp.bfloat16

TP, EP = 8, 16
ROWS, WIDTH, FEAT = 128, 2048, 256
CH, GROUPS, STATE, GCH = 128, 8, 64, 16
GS = GROUPS * STATE
CAP, OWN = 8, 16
SIDE = 4
HALF = WIDTH // 2
SLOTS = EP * CAP
FF, SF = 512, 256
MIX = CH * TP
VMEM_MIB = 48


def dot(a, b):
    return jnp.dot(a, b, preferred_element_type=f32)


def dot_nt(a, b):
    return lax.dot_general(a, b, (((1,), (1,)), ((), ())), preferred_element_type=f32)


def dot_tn(a, b):
    return lax.dot_general(a, b, (((0,), (0,)), ((), ())), preferred_element_type=f32)


def halves(a):
    high = a.astype(bf16)
    return high, (a - high.astype(f32)).astype(bf16)


def lanes_of_groups(a):
    return jnp.concatenate([a[g : g + 1, :] for g in range(GROUPS)], axis=1)


def block_diagonal(a):
    wide = jnp.concatenate([a] * GROUPS, axis=1)
    row = lax.broadcasted_iota(jnp.int32, (CH, GS), 0) // GCH
    col = lax.broadcasted_iota(jnp.int32, (CH, GS), 1) // STATE
    return jnp.where(row == col, wide, 0.0)


def per_group_rows(a):
    return jnp.broadcast_to(a[:, None, :], (GROUPS, GCH, STATE)).reshape(CH, STATE)


def kernel(
    resid_hbm, in_gain_hbm, in_w_hbm, state_hbm, decay_hbm, freq_hbm, step_hbm, in_coef_hbm,
    out_coef_hbm, skip_hbm, out_w_hbm, mid_gain_hbm, gate_vec_hbm, routes_hbm, weights_hbm,
    eg_hbm, eu_hbm, ed_hbm, sg_hbm, su_hbm, sd_hbm,
    out_ref, new_state_ref,
    resid_ref, in_gain_ref, decay_ref, freq_ref, step_ref, in_coef_ref, out_coef_ref, skip_ref,
    mid_gain_ref, gate_vec_ref, routes_ref, weights_ref,
    full, in_w, state, out_w, eg, eu, ed, sg, su, sd,
    mixed, after, mid, outgoing, slots_in, resid_in, mixed_in, after_in, piece, hidden, result, returned,
    shidden, partial, stage_a, stage_b, sum_a, sum_b, final_a, final_b,
    routed_part, core_in, core_sum, routed_in,
    local_sem, s1, r1, s2, r2, se, re, sl, rl, s3, r3, s5, r5, s6, r6, s6f, r6f, s7, r7,
):
    e = lax.axis_index("ep")
    t = lax.axis_index("tp")
    z, x = e // SIDE, e % SIDE
    y, core = t // 2, t % 2
    tp_peers = [
        (dy * 2 + dc, (e, ((y + dy) % SIDE) * 2 + (core + dc) % 2))
        for dy in (1, 3, 2, 0) for dc in (0, 1) if dy + dc
    ]
    ep_peers = [
        (dz * SIDE + dx, (((z + dz) % SIDE) * SIDE + (x + dx) % SIDE, t))
        for dz in range(SIDE) for dx in range(SIDE) if dz + dx
    ]
    x_peers = [(d, (z * SIDE + (x + d) % SIDE, t), (x + d) % SIDE) for d in (1, 3, 2)]
    z_peers = [(d, (((z + d) % SIDE) * SIDE + x, t), (z + d) % SIDE) for d in (1, 3, 2)]
    y_peers = [(d, (e, ((y + d) % SIDE) * 2 + core), (y + d) % SIDE) for d in (1, 3, 2)]
    partner = (e, y * 2 + (1 - core))

    barrier = pltpu.get_barrier_semaphore()
    for _, dev in tp_peers + ep_peers:
        pl.semaphore_signal(barrier, inc=1, device_id=dev, device_id_type=MESH)

    fetches = {}
    for i, (name, src, dst) in enumerate([
        ("resid", resid_hbm, resid_ref), ("decay", decay_hbm, decay_ref),
        ("freq", freq_hbm, freq_ref), ("step", step_hbm, step_ref),
        ("in_coef", in_coef_hbm, in_coef_ref), ("out_coef", out_coef_hbm, out_coef_ref),
        ("routes", routes_hbm, routes_ref), ("weights", weights_hbm, weights_ref),
        ("skip", skip_hbm, skip_ref), ("in_gain", in_gain_hbm, in_gain_ref),
        ("state", state_hbm, state), ("in_w", in_w_hbm, in_w),
        ("mid_gain", mid_gain_hbm, mid_gain_ref), ("gate_vec", gate_vec_hbm, gate_vec_ref),
        ("out_w", out_w_hbm, out_w),
        ("eg", eg_hbm, eg), ("eu", eu_hbm, eu), ("ed", ed_hbm, ed),
        ("sg", sg_hbm, sg), ("su", su_hbm, su), ("sd", sd_hbm, sd),
    ]):
        fetches[name] = pltpu.make_async_copy(src, dst, local_sem.at[i])
        fetches[name].start()

    def fetched(*names):
        for name in names:
            fetches[name].wait()

    def send(src, dst, ss, rs, d, dev):
        copy = pltpu.make_async_remote_copy(
            src_ref=src, dst_ref=dst, send_sem=ss, recv_sem=rs.at[d],
            device_id=dev, device_id_type=MESH,
        )
        copy.start()

    def all_of(ref, sem):
        pltpu.make_async_copy(ref, ref, sem).wait()

    own_rows = pl.ds(pl.multiple_of(t * OWN, OWN), OWN)

    pl.semaphore_wait(barrier, TP - 1 + EP - 1)

    fetched("resid")
    cols = pl.ds(pl.multiple_of(t * FEAT, FEAT), FEAT)
    for d, dev, _ in y_peers:
        send(resid_ref, full.at[:, cols], s1, r1, d, dev)
    send(resid_ref, full.at[:, cols], s1, r1, 0, partner)
    full[:, cols] = resid_ref[...]

    fetched("decay", "freq", "step", "in_coef", "out_coef")
    own_lane = (
        lax.broadcasted_iota(jnp.int32, (GROUPS, GROUPS), 0)
        == lax.broadcasted_iota(jnp.int32, (GROUPS, GROUPS), 1)
    )
    log_step = jnp.sum(jnp.where(own_lane, step_ref[...], 0.0), axis=1, keepdims=True)
    dt = jnp.exp(log_step)
    rate = -decay_ref[...]
    freq = freq_ref[...]
    magnitude = jnp.exp(rate * dt)
    keep_re = magnitude * jnp.cos(freq * dt)
    keep_im = magnitude * jnp.sin(freq * dt)
    denominator = rate * rate + freq * freq
    factor_re = ((keep_re - 1.0) * rate + keep_im * freq) / denominator
    factor_im = (keep_im * rate - (keep_re - 1.0) * freq) / denominator
    fr, fi = per_group_rows(factor_re), per_group_rows(factor_im)
    push_re = block_diagonal(fr * in_coef_ref[0] - fi * in_coef_ref[1])
    push_im = block_diagonal(fr * in_coef_ref[1] + fi * in_coef_ref[0])
    pr_hi, pr_lo = halves(push_re)
    pi_hi, pi_lo = halves(push_im)
    out_re = block_diagonal(out_coef_ref[0]).astype(bf16)
    out_im = block_diagonal(out_coef_ref[1]).astype(bf16)
    kr, ki = lanes_of_groups(keep_re), lanes_of_groups(keep_im)

    fetched("routes", "weights")
    slot_row = lax.broadcasted_iota(jnp.int32, (SLOTS, ROWS), 0)
    expert = (slot_row // CAP) * TP + t
    weight_sum = jnp.sum(weights_ref[...], axis=0, keepdims=True)
    weights = weights_ref[...] / weight_sum * routed_scale
    chosen = jnp.zeros((SLOTS, ROWS), f32)
    chosen_weight = jnp.zeros((SLOTS, ROWS), f32)
    for k in range(4):
        same = routes_ref[k : k + 1, :] == expert
        chosen = jnp.where(same, 1.0, chosen)
        chosen_weight = jnp.where(same, weights[k : k + 1, :], chosen_weight)
    earlier = (
        lax.broadcasted_iota(jnp.int32, (ROWS, ROWS), 0)
        < lax.broadcasted_iota(jnp.int32, (ROWS, ROWS), 1)
    )
    before = dot(chosen.astype(bf16), jnp.where(earlier, 1.0, 0.0).astype(bf16))
    rank = (slot_row % CAP).astype(f32)
    holds = (chosen > 0.5) & (before == rank)
    pick = jnp.where(holds, 1.0, 0.0).astype(bf16)
    combine = jnp.where(holds, chosen_weight, 0.0).T
    comb_hi, comb_lo = halves(combine)

    fetched("state", "in_w", "in_gain", "skip")
    old_re, old_im = state[0], state[1]
    new_state_ref[0] = kr * old_re - ki * old_im
    new_state_ref[1] = kr * old_im + ki * old_re
    for d in (1, 3, 2):
        theirs = pl.ds(pl.multiple_of((((y + SIDE - d) % SIDE) * 2 + core) * FEAT, FEAT), FEAT)
        all_of(full.at[:, theirs], r1.at[d])
        send(full.at[:, theirs], full.at[:, theirs], s1, r1, 0, partner)
    all_of(full.at[:, pl.ds(0, SIDE * FEAT)], r1.at[0])

    def first_step(src, dst, width, ss, rs):
        left, right = pl.ds(0, width), pl.ds(width, width)
        for k, (a, b) in enumerate(((left, right), (right, left))):
            for (d, dev_x, _), (_, dev_z, _) in zip(x_peers, z_peers, strict=True):
                send(src.at[own_rows, a], dst.at[e, :, a], ss, rs, d if k == 0 else 0, dev_x)
                send(src.at[own_rows, b], dst.at[e, :, b], ss, rs, 4 + d if k == 0 else 0, dev_z)

    def second_step(dst, width, ss, rs):
        left, right = pl.ds(0, width), pl.ds(width, width)
        for d in (1, 3, 2):
            block = dst.at[z * SIDE + (x + SIDE - d) % SIDE, :, left]
            all_of(block, rs.at[d])
            for _, dev, _ in z_peers:
                send(block, block, ss, rs, 0, dev)
            block = dst.at[((z + SIDE - d) % SIDE) * SIDE + x, :, right]
            all_of(block, rs.at[4 + d])
            for _, dev, _ in x_peers:
                send(block, block, ss, rs, 0, dev)

    first_step(full, resid_in, HALF, se, re)
    values = full[...].astype(f32)
    mean = jnp.sum(values, axis=1, keepdims=True) * (1.0 / WIDTH)
    square = jnp.sum(values * values, axis=1, keepdims=True) * (1.0 / WIDTH)
    scale = lax.rsqrt(square - mean * mean + norm_eps)
    normed = ((values - mean) * scale * in_gain_ref[...]).astype(bf16)
    drive = dot(normed, in_w[...]).astype(bf16)
    new_re = new_state_ref[0] + (dot(drive, pr_hi) + dot(drive, pr_lo))
    new_im = new_state_ref[1] + (dot(drive, pi_hi) + dot(drive, pi_lo))
    new_state_ref[0] = new_re
    new_state_ref[1] = new_im
    read = dot_nt(new_re.astype(bf16), out_re) - dot_nt(new_im.astype(bf16), out_im)
    read = read + skip_ref[...] * drive.astype(f32)
    mixed_cols = pl.ds(pl.multiple_of(t * CH, CH), CH)
    mixed[:, mixed_cols] = jax.nn.gelu(read, approximate=True).astype(bf16)

    for d, dev in tp_peers:
        send(mixed.at[:, mixed_cols], mixed.at[:, mixed_cols], s2, r2, d // 2, dev)
    resid_in[e] = full[own_rows, :]
    fetched("out_w", "mid_gain")
    sums = [jnp.zeros((ROWS, 128), f32), jnp.zeros((ROWS, 128), f32)]
    for dy in (0, 1, 3, 2):
        deep = pl.ds(pl.multiple_of(((y + SIDE - dy) % SIDE) * 256, 256), 256)
        if dy:
            all_of(mixed.at[:, deep], r2.at[dy])
        else:
            other = pl.ds(pl.multiple_of((y * 2 + (1 - core)) * CH, CH), CH)
            all_of(mixed.at[:, other], r2.at[0])
        if dy == 2:
            first_step(mixed, mixed_in, MIX // 2, sl, rl)
            mixed_in[e] = mixed[own_rows, :]
        block = mixed[:, deep]
        for j in range(WIDTH // 256):
            at = pl.ds(j * 256, 256)
            base = full[:, at].astype(f32) if dy == 0 else after[:, at]
            part = base + dot(block, out_w[deep, at])
            after[:, at] = part
            if dy == 2:
                for lanes in (part[:, :128], part[:, 128:]):
                    sums[0] = sums[0] + lanes
                    sums[1] = sums[1] + lanes * lanes
        if dy == 0:
            second_step(resid_in, HALF, se, re)
    mean = jnp.sum(sums[0], axis=1, keepdims=True) * (1.0 / WIDTH)
    square = jnp.sum(sums[1], axis=1, keepdims=True) * (1.0 / WIDTH)
    scale = lax.rsqrt(square - mean * mean + norm_eps)
    for j in range(WIDTH // 256):
        at = pl.ds(j * 256, 256)
        part = ((after[:, at] - mean) * scale * mid_gain_ref[:, at]).astype(bf16)
        mid[:, :, at] = part.reshape(TP, OWN, 256)
        outgoing[:, :, at] = dot(pick, part).astype(bf16).reshape(EP, CAP, 256)

    for d, dev in ep_peers:
        send(outgoing.at[dev[0]], slots_in.at[e], s3, r3, 0, dev)
    slots_in[e] = outgoing[e]
    own_mid = mid[t]
    fetched("gate_vec")
    gate_vec = jnp.concatenate([gate_vec_ref[i : i + 1, :] for i in range(WIDTH // 128)], axis=1)
    gate_value = jax.nn.sigmoid(
        jnp.sum(own_mid.astype(f32) * gate_vec.astype(f32), axis=1, keepdims=True)
    )
    second_step(mixed_in, MIX // 2, sl, rl)

    fetched("eg", "eu", "ed")
    all_of(slots_in.at[pl.ds(0, EP - 1)], r3.at[0])
    rows = slots_in[...].reshape(SLOTS, WIDTH)
    for j in range(FF // 256):
        at = pl.ds(j * 256, 256)
        gate_part = dot(rows, eg[:, at])
        up_part = dot(rows, eu[:, at])
        hidden[:, at] = (jax.nn.silu(gate_part) * up_part).astype(bf16)

    for j in range(WIDTH // 256):
        at = pl.ds(j * 256, 256)
        result[:, :, at] = dot(hidden[...], ed[:, at]).astype(bf16).reshape(EP, CAP, 256)

    for d, dev in ep_peers:
        send(result.at[dev[0]], returned.at[e], s5, r5, 0, dev)
    returned[e] = result[e]

    fetched("sg", "su", "sd")
    all_of(resid_in.at[pl.ds(0, 12)], re.at[0])
    all_of(mixed_in.at[pl.ds(0, 12)], rl.at[0])
    channels = mixed_in[...].reshape(EP * OWN, MIX)
    sums = [jnp.zeros((EP * OWN, 128), f32), jnp.zeros((EP * OWN, 128), f32)]
    for j in range(WIDTH // 256):
        at = pl.ds(j * 256, 256)
        part = resid_in[:, :, at].reshape(EP * OWN, 256).astype(f32) + dot(channels, out_w[:, at])
        after_in[:, at] = part
        for lanes in (part[:, :128], part[:, 128:]):
            sums[0] = sums[0] + lanes
            sums[1] = sums[1] + lanes * lanes
    mean = jnp.sum(sums[0], axis=1, keepdims=True) * (1.0 / WIDTH)
    square = jnp.sum(sums[1], axis=1, keepdims=True) * (1.0 / WIDTH)
    scale = lax.rsqrt(square - mean * mean + norm_eps)
    for j in range(WIDTH // 256):
        at = pl.ds(j * 256, 256)
        piece[:, at] = ((after_in[:, at] - mean) * scale * mid_gain_ref[:, at]).astype(bf16)
    gate_part = dot(piece[...], sg[...])
    up_part = dot(piece[...], su[...])
    shidden[...] = (jax.nn.silu(gate_part) * up_part).astype(bf16)

    grid = (SIDE, SIDE, OWN)
    half_a, half_b = pl.ds(0, HALF), pl.ds(HALF, HALF)
    for half in (0, 1):
        for j in range(HALF // 256):
            at = pl.ds(half * HALF + j * 256, 256)
            partial[:, :, :, at] = dot(shidden[...], sd[:, at]).astype(bf16).reshape(*grid, 256)
        if half == 0:
            for d, dev, there in z_peers:
                send(partial.at[there, :, :, half_a], stage_a.at[d - 1], s6.at[0], r6, 0, dev)
        else:
            for d, dev, there in x_peers:
                send(partial.at[:, there, :, half_b], stage_b.at[d - 1], s6.at[1], r6, 1, dev)

    all_of(returned.at[pl.ds(0, EP - 1)], r5.at[0])

    for j in range(WIDTH // 256):
        at = pl.ds(j * 256, 256)
        back = returned[:, :, at].reshape(SLOTS, 256)
        part = dot(comb_hi, back) + dot(comb_lo, back)
        routed_part[:, :, :, at] = part.astype(bf16).reshape(SIDE, 2, OWN, 256)

    send(routed_part.at[:, 1 - core], core_in, s7.at[0], r7, 0, partner)
    all_of(core_in, r7.at[0])
    core_sum[...] = (routed_part[:, core].astype(f32) + core_in[...].astype(f32)).astype(bf16)
    for d, dev, there in y_peers:
        send(core_sum.at[there], routed_in.at[d - 1], s7.at[1], r7, 1, dev)
    all_of(stage_a, r6.at[0])
    total = partial[z, :, :, half_a].astype(f32)
    for d in range(3):
        total = total + stage_a[d].astype(f32)
    sum_a[...] = total.astype(bf16)
    for d, dev, there in x_peers:
        send(sum_a.at[there], final_a.at[d - 1], s6f.at[0], r6f, 0, dev)
    all_of(stage_b, r6.at[1])
    total = partial[:, x, :, half_b].astype(f32)
    for d in range(3):
        total = total + stage_b[d].astype(f32)
    sum_b[...] = total.astype(bf16)
    for d, dev, there in z_peers:
        send(sum_b.at[there], final_b.at[d - 1], s6f.at[1], r6f, 1, dev)
    all_of(routed_in, r7.at[1])
    routed = core_sum[y].astype(f32) + jnp.sum(routed_in[...].astype(f32), axis=0) + after[own_rows, :]
    all_of(final_a, r6f.at[0])
    all_of(final_b, r6f.at[1])
    for at, own, others in (
        (half_a, sum_a[x], final_a), (half_b, sum_b[z], final_b),
    ):
        shared = own.astype(f32) + jnp.sum(others[...].astype(f32), axis=0)
        begin = at.start
        out_ref[:, at] = (routed[:, begin : begin + HALF] + gate_value * shared).astype(bf16)

    all_of(full.at[:, pl.ds(0, 7 * FEAT)], s1)
    all_of(mixed.at[:, pl.ds(0, 7 * CH)], s2)
    all_of(resid_in.at[pl.ds(0, 15)], se)
    all_of(mixed_in.at[pl.ds(0, 15)], sl)
    all_of(slots_in.at[pl.ds(0, EP - 1)], s3)
    all_of(returned.at[pl.ds(0, EP - 1)], s5)
    all_of(stage_a, s6.at[0])
    all_of(stage_b, s6.at[1])
    all_of(final_a, s6f.at[0])
    all_of(final_b, s6f.at[1])
    all_of(core_in, s7.at[0])
    all_of(routed_in, s7.at[1])


def per_device(
    residual, in_gain, in_weight, state, decay_rate, frequency, log_step, in_coef, out_coef,
    skip_gain, out_weight, mid_gain, gate_vector, routes, route_weight, expert_gate, expert_up,
    expert_down, shared_gate, shared_up, shared_down,
):
    vmem = pl.BlockSpec(memory_space=pltpu.VMEM)
    hbm = pl.BlockSpec(memory_space=pltpu.HBM)
    dma = pltpu.SemaphoreType.DMA
    in_coef_rows = jnp.swapaxes(in_coef, 2, 3).reshape(2, CH, STATE)
    out_coef_rows = out_coef.reshape(2, CH, STATE)
    call = pl.pallas_call(
        kernel,
        name="layer_step",
        out_shape=(
            pltpu.VMEM((OWN, WIDTH), bf16),
            pltpu.VMEM((2, ROWS, GS), f32),
        ),
        in_specs=[hbm] * 21,
        out_specs=(vmem, vmem),
        scratch_shapes=[
            pltpu.VMEM((ROWS, FEAT), bf16),
            pltpu.VMEM((1, WIDTH), f32),
            pltpu.VMEM((GROUPS, STATE), f32),
            pltpu.VMEM((GROUPS, STATE), f32),
            pltpu.VMEM((1, GROUPS), f32),
            pltpu.VMEM((2, CH, STATE), f32),
            pltpu.VMEM((2, CH, STATE), f32),
            pltpu.VMEM((1, CH), f32),
            pltpu.VMEM((1, WIDTH), f32),
            pltpu.VMEM((WIDTH // 128, 128), bf16),
            pltpu.VMEM((4, ROWS), jnp.int32),
            pltpu.VMEM((4, ROWS), f32),
            pltpu.VMEM((ROWS, WIDTH), bf16),
            pltpu.VMEM((WIDTH, CH), bf16),
            pltpu.VMEM((2, ROWS, GS), f32),
            pltpu.VMEM((MIX, WIDTH), bf16),
            pltpu.VMEM((WIDTH, FF), bf16),
            pltpu.VMEM((WIDTH, FF), bf16),
            pltpu.VMEM((FF, WIDTH), bf16),
            pltpu.VMEM((WIDTH, SF), bf16),
            pltpu.VMEM((WIDTH, SF), bf16),
            pltpu.VMEM((SF, WIDTH), bf16),
            pltpu.VMEM((ROWS, MIX), bf16),
            pltpu.VMEM((ROWS, WIDTH), f32),
            pltpu.VMEM((TP, OWN, WIDTH), bf16),
            pltpu.VMEM((EP, CAP, WIDTH), bf16),
            pltpu.VMEM((EP, CAP, WIDTH), bf16),
            pltpu.VMEM((EP, OWN, WIDTH), bf16),
            pltpu.VMEM((EP, OWN, MIX), bf16),
            pltpu.VMEM((EP * OWN, WIDTH), f32),
            pltpu.VMEM((EP * OWN, WIDTH), bf16),
            pltpu.VMEM((SLOTS, FF), bf16),
            pltpu.VMEM((EP, CAP, WIDTH), bf16),
            pltpu.VMEM((EP, CAP, WIDTH), bf16),
            pltpu.VMEM((EP * OWN, SF), bf16),
            pltpu.VMEM((SIDE, SIDE, OWN, WIDTH), bf16),
            pltpu.VMEM((SIDE - 1, SIDE, OWN, HALF), bf16),
            pltpu.VMEM((SIDE - 1, SIDE, OWN, HALF), bf16),
            pltpu.VMEM((SIDE, OWN, HALF), bf16),
            pltpu.VMEM((SIDE, OWN, HALF), bf16),
            pltpu.VMEM((SIDE - 1, OWN, HALF), bf16),
            pltpu.VMEM((SIDE - 1, OWN, HALF), bf16),
            pltpu.VMEM((SIDE, 2, OWN, WIDTH), bf16),
            pltpu.VMEM((SIDE, OWN, WIDTH), bf16),
            pltpu.VMEM((SIDE, OWN, WIDTH), bf16),
            pltpu.VMEM((SIDE - 1, OWN, WIDTH), bf16),
            dma((21,)),
            dma, dma((4,)),
            dma, dma((4,)),
            dma, dma((8,)),
            dma, dma((8,)),
            dma, dma((1,)),
            dma, dma((1,)),
            dma((2,)), dma((2,)),
            dma((2,)), dma((2,)),
            dma((2,)), dma((2,)),
        ],
        compiler_params=pltpu.CompilerParams(
            collective_id=0, has_side_effects=True, vmem_limit_bytes=VMEM_MIB * 1024 * 1024
        ),
    )
    operands = (
        residual, in_gain.reshape(1, WIDTH), in_weight, state, decay_rate, frequency,
        log_step.reshape(1, GROUPS), in_coef_rows, out_coef_rows, skip_gain.reshape(1, CH),
        out_weight, mid_gain.reshape(1, WIDTH), gate_vector.reshape(WIDTH // 128, 128), routes.T,
        route_weight.T, expert_gate[0], expert_up[0], expert_down[0], shared_gate, shared_up,
        shared_down,
    )
    return call(*[pltpu.with_memory_space_constraint(a, pltpu.HBM) for a in operands])


def solution(mesh):
    return jax.shard_map(
        per_device,
        mesh=mesh,
        in_specs=(
            P("ep", "tp"), P(), P(None, "tp"), P(None, "ep", "tp"), P("tp", None), P("tp", None),
            P("tp"), P(None, "tp", None, None), P(None, "tp", None, None), P("tp"), P(), P(), P(),
            P("ep", None), P("ep", None), P(("ep", "tp"), None, None), P(("ep", "tp"), None, None),
            P(("ep", "tp"), None, None), P(None, "ep"), P(None, "ep"), P("ep", None),
        ),
        out_specs=(P(("ep", "tp"), None), P(None, "ep", "tp")),
        check_vma=False,
    )
```

```python
import jax
import jax.numpy as jnp
from jax import lax
from jax.experimental import pallas as pl
from jax.experimental.pallas import tpu as pltpu
from jax.sharding import PartitionSpec as P

MESH = pl.DeviceIdType.MESH
norm_eps = 1e-05
routed_scale = 2.5
f32, bf16 = jnp.float32, jnp.bfloat16

TP, EP = 8, 16
ROWS, WIDTH, FEAT = 128, 2048, 256
CH, GROUPS, STATE, GCH = 128, 8, 64, 16
GS = GROUPS * STATE
CAP, OWN = 8, 16
SIDE = 4
HALF = WIDTH // 2
SLOTS = EP * CAP
FF, SF = 512, 256
MIX = CH * TP
FARTHEST_FIRST = sorted(
    [(dz, dx) for dz in range(SIDE) for dx in range(SIDE) if dz + dx],
    key=lambda s: -min(s[0], SIDE - s[0]) - min(s[1], SIDE - s[1]),
)
VMEM_MIB = 48
EARLY_COLS = 512
EARLY_PEERS = 15


def dot(a, b):
    return jnp.dot(a, b, preferred_element_type=f32)


def dot_nt(a, b):
    return lax.dot_general(a, b, (((1,), (1,)), ((), ())), preferred_element_type=f32)


def dot_tn(a, b):
    return lax.dot_general(a, b, (((0,), (0,)), ((), ())), preferred_element_type=f32)


def halves(a):
    high = a.astype(bf16)
    return high, (a - high.astype(f32)).astype(bf16)


def lanes_of_groups(a):
    return jnp.concatenate([a[g : g + 1, :] for g in range(GROUPS)], axis=1)


def block_diagonal(a):
    wide = jnp.concatenate([a] * GROUPS, axis=1)
    row = lax.broadcasted_iota(jnp.int32, (CH, GS), 0) // GCH
    col = lax.broadcasted_iota(jnp.int32, (CH, GS), 1) // STATE
    return jnp.where(row == col, wide, 0.0)


def per_group_rows(a):
    return jnp.broadcast_to(a[:, None, :], (GROUPS, GCH, STATE)).reshape(CH, STATE)


def kernel(
    resid_hbm, in_gain_hbm, in_w_hbm, state_hbm, decay_hbm, freq_hbm, step_hbm, in_coef_hbm,
    out_coef_hbm, skip_hbm, out_w_hbm, mid_gain_hbm, gate_vec_hbm, routes_hbm, weights_hbm,
    eg_hbm, eu_hbm, ed_hbm, sg_hbm, su_hbm, sd_hbm,
    out_ref, new_state_ref,
    resid_ref, in_gain_ref, decay_ref, freq_ref, step_ref, in_coef_ref, out_coef_ref, skip_ref,
    mid_gain_ref, gate_vec_ref, routes_ref, weights_ref,
    full, in_w, state, out_w, eg, eu, ed, sg, su, sd,
    own_resid, own_mixed, mixed, after, mid, outgoing, slots_in, resid_in, mixed_in, after_in, piece, hidden, result, returned,
    shidden, partial, stage_a, stage_b, sum_a, sum_b, final_a, final_b,
    routed_part, core_in, core_sum, routed_in,
    local_sem, so, ro, s1, r1, s2, r2, se, re, sl, rl, s3, r3, s5, r5, s6, r6, s6f, r6f, s7, r7,
):
    e = lax.axis_index("ep")
    t = lax.axis_index("tp")
    z, x = e // SIDE, e % SIDE
    y, core = t // 2, t % 2
    tp_peers = [
        (dy * 2 + dc, (e, ((y + dy) % SIDE) * 2 + (core + dc) % 2))
        for dy in (1, 3, 2, 0) for dc in (0, 1) if dy + dc
    ]
    ep_peers = [
        (dz * SIDE + dx, (((z + dz) % SIDE) * SIDE + (x + dx) % SIDE, t))
        for dz, dx in FARTHEST_FIRST
    ]
    x_peers = [(d, (z * SIDE + (x + d) % SIDE, t), (x + d) % SIDE) for d in (1, 3, 2)]
    z_peers = [(d, (((z + d) % SIDE) * SIDE + x, t), (z + d) % SIDE) for d in (1, 3, 2)]
    y_peers = [(d, (e, ((y + d) % SIDE) * 2 + core), (y + d) % SIDE) for d in (1, 3, 2)]
    partner = (e, y * 2 + (1 - core))

    barrier = pltpu.get_barrier_semaphore()
    for _, dev in tp_peers + ep_peers:
        pl.semaphore_signal(barrier, inc=1, device_id=dev, device_id_type=MESH)

    fetches = {}
    for i, (name, src, dst) in enumerate([
        ("resid", resid_hbm, resid_ref), ("decay", decay_hbm, decay_ref),
        ("freq", freq_hbm, freq_ref), ("step", step_hbm, step_ref),
        ("in_coef", in_coef_hbm, in_coef_ref), ("out_coef", out_coef_hbm, out_coef_ref),
        ("routes", routes_hbm, routes_ref), ("weights", weights_hbm, weights_ref),
        ("skip", skip_hbm, skip_ref), ("in_gain", in_gain_hbm, in_gain_ref),
        ("state", state_hbm, state), ("in_w", in_w_hbm, in_w),
        ("mid_gain", mid_gain_hbm, mid_gain_ref), ("gate_vec", gate_vec_hbm, gate_vec_ref),
        ("out_w", out_w_hbm, out_w),
        ("eg", eg_hbm, eg), ("eu", eu_hbm, eu), ("ed", ed_hbm, ed),
        ("sg", sg_hbm, sg), ("su", su_hbm, su), ("sd", sd_hbm, sd),
    ]):
        fetches[name] = pltpu.make_async_copy(src, dst, local_sem.at[i])
        fetches[name].start()

    def fetched(*names):
        for name in names:
            fetches[name].wait()

    def send(src, dst, ss, rs, d, dev):
        copy = pltpu.make_async_remote_copy(
            src_ref=src, dst_ref=dst, send_sem=ss, recv_sem=rs.at[d],
            device_id=dev, device_id_type=MESH,
        )
        copy.start()

    def all_of(ref, sem):
        pltpu.make_async_copy(ref, ref, sem).wait()

    own_rows = pl.ds(pl.multiple_of(t * OWN, OWN), OWN)

    pl.semaphore_wait(barrier, TP - 1 + EP - 1)

    fetched("resid")
    cols = pl.ds(pl.multiple_of(t * FEAT, FEAT), FEAT)
    for _, dev in tp_peers:
        rows = pl.ds(pl.multiple_of(dev[1] * OWN, OWN), OWN)
        send(resid_ref.at[rows], own_resid.at[:, cols], so.at[0], ro, 0, dev)
    full[:, cols] = resid_ref[...]
    own_resid[:, cols] = resid_ref[own_rows, :]

    fetched("decay", "freq", "step", "in_coef", "out_coef")
    own_lane = (
        lax.broadcasted_iota(jnp.int32, (GROUPS, GROUPS), 0)
        == lax.broadcasted_iota(jnp.int32, (GROUPS, GROUPS), 1)
    )
    log_step = jnp.sum(jnp.where(own_lane, step_ref[...], 0.0), axis=1, keepdims=True)
    dt = jnp.exp(log_step)
    rate = -decay_ref[...]
    freq = freq_ref[...]
    magnitude = jnp.exp(rate * dt)
    keep_re = magnitude * jnp.cos(freq * dt)
    keep_im = magnitude * jnp.sin(freq * dt)
    denominator = rate * rate + freq * freq
    factor_re = ((keep_re - 1.0) * rate + keep_im * freq) / denominator
    factor_im = (keep_im * rate - (keep_re - 1.0) * freq) / denominator
    fr, fi = per_group_rows(factor_re), per_group_rows(factor_im)
    push_re = block_diagonal(fr * in_coef_ref[0] - fi * in_coef_ref[1])
    push_im = block_diagonal(fr * in_coef_ref[1] + fi * in_coef_ref[0])
    pr_hi, pr_lo = halves(push_re)
    pi_hi, pi_lo = halves(push_im)
    out_re = block_diagonal(out_coef_ref[0]).astype(bf16)
    out_im = block_diagonal(out_coef_ref[1]).astype(bf16)
    kr, ki = lanes_of_groups(keep_re), lanes_of_groups(keep_im)

    fetched("routes", "weights")
    slot_row = lax.broadcasted_iota(jnp.int32, (SLOTS, ROWS), 0)
    expert = (slot_row // CAP) * TP + t
    weight_sum = jnp.sum(weights_ref[...], axis=0, keepdims=True)
    weights = weights_ref[...] / weight_sum * routed_scale
    chosen = jnp.zeros((SLOTS, ROWS), f32)
    chosen_weight = jnp.zeros((SLOTS, ROWS), f32)
    for k in range(4):
        same = routes_ref[k : k + 1, :] == expert
        chosen = jnp.where(same, 1.0, chosen)
        chosen_weight = jnp.where(same, weights[k : k + 1, :], chosen_weight)
    earlier = (
        lax.broadcasted_iota(jnp.int32, (ROWS, ROWS), 0)
        < lax.broadcasted_iota(jnp.int32, (ROWS, ROWS), 1)
    )
    before = dot(chosen.astype(bf16), jnp.where(earlier, 1.0, 0.0).astype(bf16))
    rank = (slot_row % CAP).astype(f32)
    holds = (chosen > 0.5) & (before == rank)
    pick = jnp.where(holds, 1.0, 0.0).astype(bf16)
    combine = jnp.where(holds, chosen_weight, 0.0).T
    comb_hi, comb_lo = halves(combine)

    for d, dev, _ in y_peers:
        send(resid_ref, full.at[:, cols], s1, r1, d, dev)
    send(resid_ref, full.at[:, cols], s1, r1, 0, partner)
    fetched("state", "in_w", "in_gain", "skip")
    old_re, old_im = state[0], state[1]
    new_state_ref[0] = kr * old_re - ki * old_im
    new_state_ref[1] = kr * old_im + ki * old_re
    def first_step(src, dst, width, ss, rs):
        left, right = pl.ds(0, width), pl.ds(width, width)
        for k, (a, b) in enumerate(((left, right), (right, left))):
            for (d, dev_x, _), (_, dev_z, _) in zip(x_peers, z_peers, strict=True):
                send(src.at[:, a], dst.at[e, :, a], ss, rs, d if k == 0 else 0, dev_x)
                send(src.at[:, b], dst.at[e, :, b], ss, rs, 4 + d if k == 0 else 0, dev_z)

    def second_step(dst, width, ss, rs):
        left, right = pl.ds(0, width), pl.ds(width, width)
        for d in (1, 3, 2):
            block = dst.at[z * SIDE + (x + SIDE - d) % SIDE, :, left]
            all_of(block, rs.at[d])
            for _, dev, _ in z_peers:
                send(block, block, ss, rs, 0, dev)
            block = dst.at[((z + SIDE - d) % SIDE) * SIDE + x, :, right]
            all_of(block, rs.at[4 + d])
            for _, dev, _ in x_peers:
                send(block, block, ss, rs, 0, dev)

    all_of(own_resid.at[:, pl.ds(0, 7 * FEAT)], ro.at[0])
    first_step(own_resid, resid_in, HALF, se, re)
    resid_in[e] = own_resid[...]
    for d in (1, 3, 2):
        theirs = pl.ds(pl.multiple_of((((y + SIDE - d) % SIDE) * 2 + core) * FEAT, FEAT), FEAT)
        all_of(full.at[:, theirs], r1.at[d])
        send(full.at[:, theirs], full.at[:, theirs], s1, r1, 0, partner)
    all_of(full.at[:, pl.ds(0, SIDE * FEAT)], r1.at[0])

    values = full[...].astype(f32)
    mean = jnp.sum(values, axis=1, keepdims=True) * (1.0 / WIDTH)
    square = jnp.sum(values * values, axis=1, keepdims=True) * (1.0 / WIDTH)
    scale = lax.rsqrt(square - mean * mean + norm_eps)
    normed = ((values - mean) * scale * in_gain_ref[...]).astype(bf16)
    drive = dot(normed, in_w[...]).astype(bf16)
    new_re = new_state_ref[0] + (dot(drive, pr_hi) + dot(drive, pr_lo))
    new_im = new_state_ref[1] + (dot(drive, pi_hi) + dot(drive, pi_lo))
    new_state_ref[0] = new_re
    new_state_ref[1] = new_im
    read = dot_nt(new_re.astype(bf16), out_re) - dot_nt(new_im.astype(bf16), out_im)
    read = read + skip_ref[...] * drive.astype(f32)
    mixed_cols = pl.ds(pl.multiple_of(t * CH, CH), CH)
    mixed_part = jax.nn.gelu(read, approximate=True).astype(bf16)
    mixed[:, mixed_cols] = mixed_part

    for _, dev in tp_peers:
        rows = pl.ds(pl.multiple_of(dev[1] * OWN, OWN), OWN)
        send(mixed.at[rows, mixed_cols], own_mixed.at[:, mixed_cols], so.at[1], ro, 1, dev)
    own_mixed[:, mixed_cols] = mixed[own_rows, mixed_cols]
    for d, dev in tp_peers:
        send(mixed.at[:, mixed_cols], mixed.at[:, mixed_cols], s2, r2, d // 2, dev)
    second_step(resid_in, HALF, se, re)
    fetched("out_w", "mid_gain")
    sums = [jnp.zeros((ROWS, 128), f32), jnp.zeros((ROWS, 128), f32)]
    for dy in (0, 1, 3, 2):
        deep = pl.ds(pl.multiple_of(((y + SIDE - dy) % SIDE) * 256, 256), 256)
        if dy:
            all_of(mixed.at[:, deep], r2.at[dy])
        else:
            other = pl.ds(pl.multiple_of((y * 2 + (1 - core)) * CH, CH), CH)
            all_of(mixed.at[:, other], r2.at[0])
        block = mixed[:, deep]
        for j in range(WIDTH // 256):
            at = pl.ds(j * 256, 256)
            base = full[:, at].astype(f32) if dy == 0 else after[:, at]
            part = base + dot(block, out_w[deep, at])
            after[:, at] = part
            if dy == 2:
                for lanes in (part[:, :128], part[:, 128:]):
                    sums[0] = sums[0] + lanes
                    sums[1] = sums[1] + lanes * lanes
        if dy == 0:
            all_of(own_mixed.at[:, pl.ds(0, 7 * CH)], ro.at[1])
            first_step(own_mixed, mixed_in, MIX // 2, sl, rl)
            mixed_in[e] = own_mixed[...]
    mean = jnp.sum(sums[0], axis=1, keepdims=True) * (1.0 / WIDTH)
    square = jnp.sum(sums[1], axis=1, keepdims=True) * (1.0 / WIDTH)
    scale = lax.rsqrt(square - mean * mean + norm_eps)
    for j in range(WIDTH // 256):
        at = pl.ds(j * 256, 256)
        part = ((after[:, at] - mean) * scale * mid_gain_ref[:, at]).astype(bf16)
        mid[:, :, at] = part.reshape(TP, OWN, 256)
        outgoing[:, :, at] = dot(pick, part).astype(bf16).reshape(EP, CAP, 256)

    for d, dev in ep_peers[:EARLY_PEERS]:
        send(outgoing.at[dev[0]], slots_in.at[e], s3, r3, 0, dev)
    slots_in[e] = outgoing[e]
    own_mid = mid[t]
    fetched("gate_vec")
    gate_vec = jnp.concatenate([gate_vec_ref[i : i + 1, :] for i in range(WIDTH // 128)], axis=1)
    gate_value = jax.nn.sigmoid(
        jnp.sum(own_mid.astype(f32) * gate_vec.astype(f32), axis=1, keepdims=True)
    )
    second_step(mixed_in, MIX // 2, sl, rl)
    for d, dev in ep_peers[EARLY_PEERS:]:
        send(outgoing.at[dev[0]], slots_in.at[e], s3, r3, 0, dev)

    fetched("eg", "eu", "ed")
    all_of(slots_in.at[pl.ds(0, EP - 1)], r3.at[0])
    rows = slots_in[...].reshape(SLOTS, WIDTH)
    for j in range(FF // 256):
        at = pl.ds(j * 256, 256)
        gate_part = dot(rows, eg[:, at])
        up_part = dot(rows, eu[:, at])
        hidden[:, at] = (jax.nn.silu(gate_part) * up_part).astype(bf16)

    for j in range(WIDTH // 256):
        at = pl.ds(j * 256, 256)
        result[:, :, at] = dot(hidden[...], ed[:, at]).astype(bf16).reshape(EP, CAP, 256)

    for d, dev in ep_peers:
        send(result.at[dev[0]], returned.at[e], s5, r5, 0, dev)
    returned[e] = result[e]

    fetched("sg", "su", "sd")
    all_of(resid_in.at[pl.ds(0, 12)], re.at[0])
    all_of(mixed_in.at[pl.ds(0, 12)], rl.at[0])
    channels = mixed_in[...].reshape(EP * OWN, MIX)
    sums = [jnp.zeros((EP * OWN, 128), f32), jnp.zeros((EP * OWN, 128), f32)]
    for j in range(WIDTH // 256):
        at = pl.ds(j * 256, 256)
        part = resid_in[:, :, at].reshape(EP * OWN, 256).astype(f32) + dot(channels, out_w[:, at])
        after_in[:, at] = part
        for lanes in (part[:, :128], part[:, 128:]):
            sums[0] = sums[0] + lanes
            sums[1] = sums[1] + lanes * lanes
    mean = jnp.sum(sums[0], axis=1, keepdims=True) * (1.0 / WIDTH)
    square = jnp.sum(sums[1], axis=1, keepdims=True) * (1.0 / WIDTH)
    scale = lax.rsqrt(square - mean * mean + norm_eps)
    for j in range(WIDTH // 256):
        at = pl.ds(j * 256, 256)
        piece[:, at] = ((after_in[:, at] - mean) * scale * mid_gain_ref[:, at]).astype(bf16)
    gate_part = dot(piece[...], sg[...])
    up_part = dot(piece[...], su[...])
    shidden[...] = (jax.nn.silu(gate_part) * up_part).astype(bf16)

    grid = (SIDE, SIDE, OWN)
    half_a, half_b = pl.ds(0, HALF), pl.ds(HALF, HALF)
    parts = ((0, EARLY_COLS), (EARLY_COLS, HALF - EARLY_COLS))

    def partial_columns(at):
        partial[:, :, :, at] = dot(shidden[...], sd[:, at]).astype(bf16).reshape(*grid, at.size)

    def first_sums(part):
        begin, size = parts[part]
        at = pl.ds(begin, size)
        left, right = at, pl.ds(HALF + begin, size)
        for d, dev, there in z_peers:
            send(partial.at[there, :, :, left], stage_a.at[d - 1, :, :, at], s6.at[2 * part], r6, 2 * part, dev)
        for d, dev, there in x_peers:
            send(partial.at[:, there, :, right], stage_b.at[d - 1, :, :, at], s6.at[2 * part + 1], r6, 2 * part + 1, dev)

    def second_sums(part):
        begin, size = parts[part]
        at = pl.ds(begin, size)
        left, right = at, pl.ds(HALF + begin, size)
        all_of(stage_a.at[:, :, :, at], r6.at[2 * part])
        total = partial[z, :, :, left].astype(f32)
        for d in range(3):
            total = total + stage_a[d, :, :, at].astype(f32)
        sum_a[:, :, at] = total.astype(bf16)
        for d, dev, there in x_peers:
            send(sum_a.at[there, :, at], final_a.at[d - 1, :, at], s6f.at[2 * part], r6f, 2 * part, dev)
        all_of(stage_b.at[:, :, :, at], r6.at[2 * part + 1])
        total = partial[:, x, :, right].astype(f32)
        for d in range(3):
            total = total + stage_b[d, :, :, at].astype(f32)
        sum_b[:, :, at] = total.astype(bf16)
        for d, dev, there in z_peers:
            send(sum_b.at[there, :, at], final_b.at[d - 1, :, at], s6f.at[2 * part + 1], r6f, 2 * part + 1, dev)

    for begin in range(0, EARLY_COLS, 256):
        partial_columns(pl.ds(begin, 256))
        partial_columns(pl.ds(HALF + begin, 256))
    first_sums(0)
    for begin in range(EARLY_COLS, HALF, 256):
        partial_columns(pl.ds(begin, 256))
        partial_columns(pl.ds(HALF + begin, 256))
    first_sums(1)

    all_of(returned.at[pl.ds(0, EP - 1)], r5.at[0])

    for j in range(WIDTH // 256):
        at = pl.ds(j * 256, 256)
        back = returned[:, :, at].reshape(SLOTS, 256)
        part = dot(comb_hi, back) + dot(comb_lo, back)
        routed_part[:, :, :, at] = part.astype(bf16).reshape(SIDE, 2, OWN, 256)

    send(routed_part.at[:, 1 - core], core_in, s7.at[0], r7, 0, partner)
    all_of(core_in, r7.at[0])
    core_sum[...] = (routed_part[:, core].astype(f32) + core_in[...].astype(f32)).astype(bf16)
    for d, dev, there in y_peers:
        send(core_sum.at[there], routed_in.at[d - 1], s7.at[1], r7, 1, dev)
    second_sums(0)
    second_sums(1)
    all_of(routed_in, r7.at[1])
    routed = core_sum[y].astype(f32) + jnp.sum(routed_in[...].astype(f32), axis=0) + after[own_rows, :]
    for part, (begin, size) in enumerate(parts):
        all_of(final_a.at[:, :, pl.ds(begin, size)], r6f.at[2 * part])
        all_of(final_b.at[:, :, pl.ds(begin, size)], r6f.at[2 * part + 1])
    for at, own, others in (
        (half_a, sum_a[x], final_a), (half_b, sum_b[z], final_b),
    ):
        shared = own.astype(f32) + jnp.sum(others[...].astype(f32), axis=0)
        begin = at.start
        out_ref[:, at] = (routed[:, begin : begin + HALF] + gate_value * shared).astype(bf16)

    all_of(own_resid.at[:, pl.ds(0, 7 * FEAT)], so.at[0])
    all_of(own_mixed.at[:, pl.ds(0, 7 * CH)], so.at[1])
    all_of(full.at[:, pl.ds(0, 7 * FEAT)], s1)
    all_of(mixed.at[:, pl.ds(0, 7 * CH)], s2)
    all_of(resid_in.at[pl.ds(0, 15)], se)
    all_of(mixed_in.at[pl.ds(0, 15)], sl)
    all_of(slots_in.at[pl.ds(0, EP - 1)], s3)
    all_of(returned.at[pl.ds(0, EP - 1)], s5)
    for part, (begin, size) in enumerate(parts):
        at = pl.ds(begin, size)
        all_of(stage_a.at[:, :, :, at], s6.at[2 * part])
        all_of(stage_b.at[:, :, :, at], s6.at[2 * part + 1])
        all_of(final_a.at[:, :, at], s6f.at[2 * part])
        all_of(final_b.at[:, :, at], s6f.at[2 * part + 1])
    all_of(core_in, s7.at[0])
    all_of(routed_in, s7.at[1])


def write_out(out_ref, state_ref, out_hbm, state_hbm, sem):
    copies = [
        pltpu.make_async_copy(state_ref, state_hbm, sem.at[0]),
        pltpu.make_async_copy(out_ref, out_hbm, sem.at[1]),
    ]
    for c in copies:
        c.start()
    for c in copies:
        c.wait()


def per_device(
    residual, in_gain, in_weight, state, decay_rate, frequency, log_step, in_coef, out_coef,
    skip_gain, out_weight, mid_gain, gate_vector, routes, route_weight, expert_gate, expert_up,
    expert_down, shared_gate, shared_up, shared_down,
):
    vmem = pl.BlockSpec(memory_space=pltpu.VMEM)
    hbm = pl.BlockSpec(memory_space=pltpu.HBM)
    dma = pltpu.SemaphoreType.DMA
    in_coef_rows = jnp.swapaxes(in_coef, 2, 3).reshape(2, CH, STATE)
    out_coef_rows = out_coef.reshape(2, CH, STATE)
    call = pl.pallas_call(
        kernel,
        name="layer_step",
        out_shape=(
            pltpu.VMEM((OWN, WIDTH), bf16),
            pltpu.VMEM((2, ROWS, GS), f32),
        ),
        in_specs=[hbm] * 21,
        out_specs=(vmem, vmem),
        scratch_shapes=[
            pltpu.VMEM((ROWS, FEAT), bf16),
            pltpu.VMEM((1, WIDTH), f32),
            pltpu.VMEM((GROUPS, STATE), f32),
            pltpu.VMEM((GROUPS, STATE), f32),
            pltpu.VMEM((1, GROUPS), f32),
            pltpu.VMEM((2, CH, STATE), f32),
            pltpu.VMEM((2, CH, STATE), f32),
            pltpu.VMEM((1, CH), f32),
            pltpu.VMEM((1, WIDTH), f32),
            pltpu.VMEM((WIDTH // 128, 128), bf16),
            pltpu.VMEM((4, ROWS), jnp.int32),
            pltpu.VMEM((4, ROWS), f32),
            pltpu.VMEM((ROWS, WIDTH), bf16),
            pltpu.VMEM((WIDTH, CH), bf16),
            pltpu.VMEM((2, ROWS, GS), f32),
            pltpu.VMEM((MIX, WIDTH), bf16),
            pltpu.VMEM((WIDTH, FF), bf16),
            pltpu.VMEM((WIDTH, FF), bf16),
            pltpu.VMEM((FF, WIDTH), bf16),
            pltpu.VMEM((WIDTH, SF), bf16),
            pltpu.VMEM((WIDTH, SF), bf16),
            pltpu.VMEM((SF, WIDTH), bf16),
            pltpu.VMEM((OWN, WIDTH), bf16),
            pltpu.VMEM((OWN, MIX), bf16),
            pltpu.VMEM((ROWS, MIX), bf16),
            pltpu.VMEM((ROWS, WIDTH), f32),
            pltpu.VMEM((TP, OWN, WIDTH), bf16),
            pltpu.VMEM((EP, CAP, WIDTH), bf16),
            pltpu.VMEM((EP, CAP, WIDTH), bf16),
            pltpu.VMEM((EP, OWN, WIDTH), bf16),
            pltpu.VMEM((EP, OWN, MIX), bf16),
            pltpu.VMEM((EP * OWN, WIDTH), f32),
            pltpu.VMEM((EP * OWN, WIDTH), bf16),
            pltpu.VMEM((SLOTS, FF), bf16),
            pltpu.VMEM((EP, CAP, WIDTH), bf16),
            pltpu.VMEM((EP, CAP, WIDTH), bf16),
            pltpu.VMEM((EP * OWN, SF), bf16),
            pltpu.VMEM((SIDE, SIDE, OWN, WIDTH), bf16),
            pltpu.VMEM((SIDE - 1, SIDE, OWN, HALF), bf16),
            pltpu.VMEM((SIDE - 1, SIDE, OWN, HALF), bf16),
            pltpu.VMEM((SIDE, OWN, HALF), bf16),
            pltpu.VMEM((SIDE, OWN, HALF), bf16),
            pltpu.VMEM((SIDE - 1, OWN, HALF), bf16),
            pltpu.VMEM((SIDE - 1, OWN, HALF), bf16),
            pltpu.VMEM((SIDE, 2, OWN, WIDTH), bf16),
            pltpu.VMEM((SIDE, OWN, WIDTH), bf16),
            pltpu.VMEM((SIDE, OWN, WIDTH), bf16),
            pltpu.VMEM((SIDE - 1, OWN, WIDTH), bf16),
            dma((21,)),
            dma((2,)), dma((2,)),
            dma, dma((4,)),
            dma, dma((4,)),
            dma, dma((8,)),
            dma, dma((8,)),
            dma, dma((1,)),
            dma, dma((1,)),
            dma((4,)), dma((4,)),
            dma((4,)), dma((4,)),
            dma((2,)), dma((2,)),
        ],
        compiler_params=pltpu.CompilerParams(
            collective_id=0, has_side_effects=True, vmem_limit_bytes=VMEM_MIB * 1024 * 1024
        ),
    )
    operands = (
        residual, in_gain.reshape(1, WIDTH), in_weight, state, decay_rate, frequency,
        log_step.reshape(1, GROUPS), in_coef_rows, out_coef_rows, skip_gain.reshape(1, CH),
        out_weight, mid_gain.reshape(1, WIDTH), gate_vector.reshape(WIDTH // 128, 128), routes.T,
        route_weight.T, expert_gate[0], expert_up[0], expert_down[0], shared_gate, shared_up,
        shared_down,
    )
    results = call(*[pltpu.with_memory_space_constraint(a, pltpu.HBM) for a in operands])
    return pl.pallas_call(
        write_out,
        name="write_out",
        out_shape=(
            jax.ShapeDtypeStruct((OWN, WIDTH), bf16),
            jax.ShapeDtypeStruct((2, ROWS, GS), f32),
        ),
        in_specs=[vmem, vmem],
        out_specs=(hbm, hbm),
        scratch_shapes=[dma((2,))],
    )(*[pltpu.with_memory_space_constraint(a, pltpu.VMEM) for a in results])


def solution(mesh):
    return jax.shard_map(
        per_device,
        mesh=mesh,
        in_specs=(
            P("ep", "tp"), P(), P(None, "tp"), P(None, "ep", "tp"), P("tp", None), P("tp", None),
            P("tp"), P(None, "tp", None, None), P(None, "tp", None, None), P("tp"), P(), P(), P(),
            P("ep", None), P("ep", None), P(("ep", "tp"), None, None), P(("ep", "tp"), None, None),
            P(("ep", "tp"), None, None), P(None, "ep"), P(None, "ep"), P("ep", None),
        ),
        out_specs=(P(("ep", "tp"), None), P(None, "ep", "tp")),
        check_vma=False,
    )
```

```python
import jax
import jax.numpy as jnp
from jax import lax
from jax.experimental import pallas as pl
from jax.experimental.pallas import tpu as pltpu
from jax.sharding import PartitionSpec as P

MESH = pl.DeviceIdType.MESH
norm_eps = 1e-05
routed_scale = 2.5
f32, bf16 = jnp.float32, jnp.bfloat16

TP, EP = 8, 16
ROWS, WIDTH, FEAT = 128, 2048, 256
CH, GROUPS, STATE, GCH = 128, 8, 64, 16
GS = GROUPS * STATE
CAP, OWN = 8, 16
SIDE = 4
HALF = WIDTH // 2
SLOTS = EP * CAP
FF, SF = 512, 256
MIX = CH * TP
FARTHEST_FIRST = sorted(
    [(dz, dx) for dz in range(SIDE) for dx in range(SIDE) if dz + dx],
    key=lambda s: -min(s[0], SIDE - s[0]) - min(s[1], SIDE - s[1]),
)
VMEM_MIB = 48
PART = 896
EARLY_COLS = 640
EARLY_PEERS = 15


def dot(a, b):
    return jnp.dot(a, b, preferred_element_type=f32)


def dot_nt(a, b):
    return lax.dot_general(a, b, (((1,), (1,)), ((), ())), preferred_element_type=f32)


def dot_tn(a, b):
    return lax.dot_general(a, b, (((0,), (0,)), ((), ())), preferred_element_type=f32)


def halves(a):
    high = a.astype(bf16)
    return high, (a - high.astype(f32)).astype(bf16)


def lanes_of_groups(a):
    return jnp.concatenate([a[g : g + 1, :] for g in range(GROUPS)], axis=1)


def block_diagonal(a):
    wide = jnp.concatenate([a] * GROUPS, axis=1)
    row = lax.broadcasted_iota(jnp.int32, (CH, GS), 0) // GCH
    col = lax.broadcasted_iota(jnp.int32, (CH, GS), 1) // STATE
    return jnp.where(row == col, wide, 0.0)


def per_group_rows(a):
    return jnp.broadcast_to(a[:, None, :], (GROUPS, GCH, STATE)).reshape(CH, STATE)


def kernel(
    resid_hbm, in_gain_hbm, in_w_hbm, state_hbm, decay_hbm, freq_hbm, step_hbm, in_coef_hbm,
    out_coef_hbm, skip_hbm, out_w_hbm, mid_gain_hbm, gate_vec_hbm, routes_hbm, weights_hbm,
    eg_hbm, eu_hbm, ed_hbm, sg_hbm, su_hbm, sd_hbm,
    out_ref, new_state_ref,
    resid_ref, in_gain_ref, decay_ref, freq_ref, step_ref, in_coef_ref, out_coef_ref, skip_ref,
    mid_gain_ref, gate_vec_ref, routes_ref, weights_ref,
    full, in_w, state, out_w, eg, eu, ed, sg, su, sd,
    own_resid, own_mixed, mixed, after, mid, outgoing, slots_in, resid_in, mixed_in, after_in, piece, hidden, result, returned,
    shidden, partial, stage_a, stage_b, sum_a, sum_b, final_a, final_b, direct_in,
    routed_part, core_in, core_sum, routed_in,
    local_sem, so, ro, s1, r1, s2, r2, se, re, sl, rl, s3, r3, s5, r5, s6, r6, s6d, r6d, s6f, r6f, s7, r7,
):
    e = lax.axis_index("ep")
    t = lax.axis_index("tp")
    z, x = e // SIDE, e % SIDE
    y, core = t // 2, t % 2
    tp_peers = [
        (dy * 2 + dc, (e, ((y + dy) % SIDE) * 2 + (core + dc) % 2))
        for dy in (1, 3, 2, 0) for dc in (0, 1) if dy + dc
    ]
    ep_peers = [
        (dz * SIDE + dx, (((z + dz) % SIDE) * SIDE + (x + dx) % SIDE, t))
        for dz, dx in FARTHEST_FIRST
    ]
    x_peers = [(d, (z * SIDE + (x + d) % SIDE, t), (x + d) % SIDE) for d in (1, 3, 2)]
    z_peers = [(d, (((z + d) % SIDE) * SIDE + x, t), (z + d) % SIDE) for d in (1, 3, 2)]
    y_peers = [(d, (e, ((y + d) % SIDE) * 2 + core), (y + d) % SIDE) for d in (1, 3, 2)]
    partner = (e, y * 2 + (1 - core))

    barrier = pltpu.get_barrier_semaphore()
    near = [dev for _, dev in tp_peers] + [peer[1] for peer in x_peers + z_peers]
    for dev in near:
        pl.semaphore_signal(barrier, inc=1, device_id=dev, device_id_type=MESH)

    fetches = {}
    for i, (name, src, dst) in enumerate([
        ("resid", resid_hbm, resid_ref), ("decay", decay_hbm, decay_ref),
        ("freq", freq_hbm, freq_ref), ("step", step_hbm, step_ref),
        ("in_coef", in_coef_hbm, in_coef_ref), ("out_coef", out_coef_hbm, out_coef_ref),
        ("routes", routes_hbm, routes_ref), ("weights", weights_hbm, weights_ref),
        ("skip", skip_hbm, skip_ref), ("in_gain", in_gain_hbm, in_gain_ref),
        ("state", state_hbm, state), ("in_w", in_w_hbm, in_w),
        ("mid_gain", mid_gain_hbm, mid_gain_ref), ("gate_vec", gate_vec_hbm, gate_vec_ref),
        ("out_w", out_w_hbm, out_w),
        ("eg", eg_hbm, eg), ("eu", eu_hbm, eu), ("ed", ed_hbm, ed),
        ("sg", sg_hbm, sg), ("su", su_hbm, su), ("sd", sd_hbm, sd),
    ]):
        fetches[name] = pltpu.make_async_copy(src, dst, local_sem.at[i])
        fetches[name].start()

    def fetched(*names):
        for name in names:
            fetches[name].wait()

    def send(src, dst, ss, rs, d, dev):
        copy = pltpu.make_async_remote_copy(
            src_ref=src, dst_ref=dst, send_sem=ss, recv_sem=rs.at[d],
            device_id=dev, device_id_type=MESH,
        )
        copy.start()

    def all_of(ref, sem):
        pltpu.make_async_copy(ref, ref, sem).wait()

    own_rows = pl.ds(pl.multiple_of(t * OWN, OWN), OWN)

    pl.semaphore_wait(barrier, len(near))

    fetched("resid")
    cols = pl.ds(pl.multiple_of(t * FEAT, FEAT), FEAT)
    for _, dev in tp_peers:
        rows = pl.ds(pl.multiple_of(dev[1] * OWN, OWN), OWN)
        send(resid_ref.at[rows], own_resid.at[:, cols], so.at[0], ro, 0, dev)
    for d, _, there in y_peers:
        for c in (0, 1):
            @pl.when(core == c)
            def _():
                send(resid_ref, full.at[:, cols], s1, r1, 2 * d + c, (e, there * 2 + 1))
    send(resid_ref, full.at[:, cols], s1, r1, 0, partner)
    full[:, cols] = resid_ref[...]
    own_resid[:, cols] = resid_ref[own_rows, :]

    fetched("decay", "freq", "step", "in_coef", "out_coef")
    own_lane = (
        lax.broadcasted_iota(jnp.int32, (GROUPS, GROUPS), 0)
        == lax.broadcasted_iota(jnp.int32, (GROUPS, GROUPS), 1)
    )
    log_step = jnp.sum(jnp.where(own_lane, step_ref[...], 0.0), axis=1, keepdims=True)
    dt = jnp.exp(log_step)
    rate = -decay_ref[...]
    freq = freq_ref[...]
    magnitude = jnp.exp(rate * dt)
    keep_re = magnitude * jnp.cos(freq * dt)
    keep_im = magnitude * jnp.sin(freq * dt)
    denominator = rate * rate + freq * freq
    factor_re = ((keep_re - 1.0) * rate + keep_im * freq) / denominator
    factor_im = (keep_im * rate - (keep_re - 1.0) * freq) / denominator
    fr, fi = per_group_rows(factor_re), per_group_rows(factor_im)
    push_re = block_diagonal(fr * in_coef_ref[0] - fi * in_coef_ref[1])
    push_im = block_diagonal(fr * in_coef_ref[1] + fi * in_coef_ref[0])
    pr_hi, pr_lo = halves(push_re)
    pi_hi, pi_lo = halves(push_im)
    out_re = block_diagonal(out_coef_ref[0]).astype(bf16)
    out_im = block_diagonal(out_coef_ref[1]).astype(bf16)
    kr, ki = lanes_of_groups(keep_re), lanes_of_groups(keep_im)

    fetched("routes", "weights")
    slot_row = lax.broadcasted_iota(jnp.int32, (SLOTS, ROWS), 0)
    expert = (slot_row // CAP) * TP + t
    weight_sum = jnp.sum(weights_ref[...], axis=0, keepdims=True)
    weights = weights_ref[...] / weight_sum * routed_scale
    chosen = jnp.zeros((SLOTS, ROWS), f32)
    chosen_weight = jnp.zeros((SLOTS, ROWS), f32)
    for k in range(4):
        same = routes_ref[k : k + 1, :] == expert
        chosen = jnp.where(same, 1.0, chosen)
        chosen_weight = jnp.where(same, weights[k : k + 1, :], chosen_weight)
    earlier = (
        lax.broadcasted_iota(jnp.int32, (ROWS, ROWS), 0)
        < lax.broadcasted_iota(jnp.int32, (ROWS, ROWS), 1)
    )
    before = dot(chosen.astype(bf16), jnp.where(earlier, 1.0, 0.0).astype(bf16))
    rank = (slot_row % CAP).astype(f32)
    holds = (chosen > 0.5) & (before == rank)
    pick = jnp.where(holds, 1.0, 0.0).astype(bf16)
    combine = jnp.where(holds, chosen_weight, 0.0).T
    comb_hi, comb_lo = halves(combine)

    fetched("state", "in_w", "in_gain", "skip")
    old_re, old_im = state[0], state[1]
    new_state_ref[0] = kr * old_re - ki * old_im
    new_state_ref[1] = kr * old_im + ki * old_re
    def first_step(src, dst, width, ss, rs):
        left, right = pl.ds(0, width), pl.ds(width, width)
        for k, (a, b) in enumerate(((left, right), (right, left))):
            for (d, dev_x, _), (_, dev_z, _) in zip(x_peers, z_peers, strict=True):
                send(src.at[:, a], dst.at[e, :, a], ss, rs, d if k == 0 else 0, dev_x)
                send(src.at[:, b], dst.at[e, :, b], ss, rs, 4 + d if k == 0 else 0, dev_z)

    def second_step(dst, width, ss, rs):
        left, right = pl.ds(0, width), pl.ds(width, width)
        for d in (1, 3, 2):
            block = dst.at[z * SIDE + (x + SIDE - d) % SIDE, :, left]
            all_of(block, rs.at[d])
            for _, dev, _ in z_peers:
                send(block, block, ss, rs, 0, dev)
            block = dst.at[((z + SIDE - d) % SIDE) * SIDE + x, :, right]
            all_of(block, rs.at[4 + d])
            for _, dev, _ in x_peers:
                send(block, block, ss, rs, 0, dev)

    all_of(own_resid.at[:, pl.ds(0, 7 * FEAT)], ro.at[0])
    first_step(own_resid, resid_in, HALF, se, re)
    resid_in[e] = own_resid[...]
    @pl.when(core == 1)
    def _():
        for d in (1, 3, 2):
            for c in (1, 0):
                at = (((y + SIDE - d) % SIDE) * 2 + c) * FEAT
                theirs = full.at[:, pl.ds(pl.multiple_of(at, FEAT), FEAT)]
                all_of(theirs, r1.at[2 * d + c])
                send(theirs, theirs, s1, r1, 0, partner)
        all_of(full.at[:, pl.ds(0, FEAT)], r1.at[0])
        all_of(full.at[:, pl.ds(0, 6 * FEAT)], s1)

    @pl.when(core == 0)
    def _():
        all_of(full.at[:, pl.ds(0, 7 * FEAT)], r1.at[0])

    values = full[...].astype(f32)
    mean = jnp.sum(values, axis=1, keepdims=True) * (1.0 / WIDTH)
    square = jnp.sum(values * values, axis=1, keepdims=True) * (1.0 / WIDTH)
    scale = lax.rsqrt(square - mean * mean + norm_eps)
    normed = ((values - mean) * scale * in_gain_ref[...]).astype(bf16)
    drive = dot(normed, in_w[...]).astype(bf16)
    new_re = new_state_ref[0] + (dot(drive, pr_hi) + dot(drive, pr_lo))
    new_im = new_state_ref[1] + (dot(drive, pi_hi) + dot(drive, pi_lo))
    new_state_ref[0] = new_re
    new_state_ref[1] = new_im
    read = dot_nt(new_re.astype(bf16), out_re) - dot_nt(new_im.astype(bf16), out_im)
    read = read + skip_ref[...] * drive.astype(f32)
    mixed_cols = pl.ds(pl.multiple_of(t * CH, CH), CH)
    mixed_part = jax.nn.gelu(read, approximate=True).astype(bf16)
    mixed[:, mixed_cols] = mixed_part

    for _, dev in tp_peers:
        rows = pl.ds(pl.multiple_of(dev[1] * OWN, OWN), OWN)
        send(mixed.at[rows, mixed_cols], own_mixed.at[:, mixed_cols], so.at[1], ro, 1, dev)
    own_mixed[:, mixed_cols] = mixed[own_rows, mixed_cols]
    for d, dev in tp_peers:
        send(mixed.at[:, mixed_cols], mixed.at[:, mixed_cols], s2, r2, d // 2, dev)
    second_step(resid_in, HALF, se, re)
    fetched("out_w", "mid_gain")
    sums = [jnp.zeros((ROWS, 128), f32), jnp.zeros((ROWS, 128), f32)]
    for dy in (0, 1, 3, 2):
        deep = pl.ds(pl.multiple_of(((y + SIDE - dy) % SIDE) * 256, 256), 256)
        if dy:
            all_of(mixed.at[:, deep], r2.at[dy])
        else:
            other = pl.ds(pl.multiple_of((y * 2 + (1 - core)) * CH, CH), CH)
            all_of(mixed.at[:, other], r2.at[0])
        block = mixed[:, deep]
        for j in range(WIDTH // 256):
            at = pl.ds(j * 256, 256)
            base = full[:, at].astype(f32) if dy == 0 else after[:, at]
            part = base + dot(block, out_w[deep, at])
            after[:, at] = part
            if dy == 2:
                for lanes in (part[:, :128], part[:, 128:]):
                    sums[0] = sums[0] + lanes
                    sums[1] = sums[1] + lanes * lanes
        if dy == 0:
            all_of(own_mixed.at[:, pl.ds(0, 7 * CH)], ro.at[1])
            first_step(own_mixed, mixed_in, MIX // 2, sl, rl)
            mixed_in[e] = own_mixed[...]
    mean = jnp.sum(sums[0], axis=1, keepdims=True) * (1.0 / WIDTH)
    square = jnp.sum(sums[1], axis=1, keepdims=True) * (1.0 / WIDTH)
    scale = lax.rsqrt(square - mean * mean + norm_eps)
    for j in range(WIDTH // 256):
        at = pl.ds(j * 256, 256)
        part = ((after[:, at] - mean) * scale * mid_gain_ref[:, at]).astype(bf16)
        mid[:, :, at] = part.reshape(TP, OWN, 256)
        outgoing[:, :, at] = dot(pick, part).astype(bf16).reshape(EP, CAP, 256)

    for d, dev in ep_peers[:EARLY_PEERS]:
        send(outgoing.at[dev[0]], slots_in.at[e], s3, r3, 0, dev)
    slots_in[e] = outgoing[e]
    own_mid = mid[t]
    fetched("gate_vec")
    gate_vec = jnp.concatenate([gate_vec_ref[i : i + 1, :] for i in range(WIDTH // 128)], axis=1)
    gate_value = jax.nn.sigmoid(
        jnp.sum(own_mid.astype(f32) * gate_vec.astype(f32), axis=1, keepdims=True)
    )
    second_step(mixed_in, MIX // 2, sl, rl)
    for d, dev in ep_peers[EARLY_PEERS:]:
        send(outgoing.at[dev[0]], slots_in.at[e], s3, r3, 0, dev)

    fetched("eg", "eu", "ed")
    all_of(slots_in.at[pl.ds(0, EP - 1)], r3.at[0])
    rows = slots_in[...].reshape(SLOTS, WIDTH)
    for j in range(FF // 256):
        at = pl.ds(j * 256, 256)
        gate_part = dot(rows, eg[:, at])
        up_part = dot(rows, eu[:, at])
        hidden[:, at] = (jax.nn.silu(gate_part) * up_part).astype(bf16)

    halves_of_rows = (pl.ds(0, HALF), pl.ds(HALF, HALF))

    def send_results(half):
        at = halves_of_rows[half]
        for _, dev in ep_peers:
            send(result.at[dev[0], :, at], returned.at[e, :, at], s5.at[half], r5, half, dev)

    for j in range(WIDTH // 256):
        at = pl.ds(j * 256, 256)
        result[:, :, at] = dot(hidden[...], ed[:, at]).astype(bf16).reshape(EP, CAP, 256)
        if j == HALF // 256 - 1:
            send_results(0)

    returned[e] = result[e]

    fetched("sg", "su", "sd")
    all_of(resid_in.at[pl.ds(0, 12)], re.at[0])
    all_of(mixed_in.at[pl.ds(0, 12)], rl.at[0])
    channels = mixed_in[...].reshape(EP * OWN, MIX)
    sums = [jnp.zeros((EP * OWN, 128), f32), jnp.zeros((EP * OWN, 128), f32)]
    for j in range(WIDTH // 256):
        at = pl.ds(j * 256, 256)
        part = resid_in[:, :, at].reshape(EP * OWN, 256).astype(f32) + dot(channels, out_w[:, at])
        after_in[:, at] = part
        for lanes in (part[:, :128], part[:, 128:]):
            sums[0] = sums[0] + lanes
            sums[1] = sums[1] + lanes * lanes
    mean = jnp.sum(sums[0], axis=1, keepdims=True) * (1.0 / WIDTH)
    square = jnp.sum(sums[1], axis=1, keepdims=True) * (1.0 / WIDTH)
    scale = lax.rsqrt(square - mean * mean + norm_eps)
    for j in range(WIDTH // 256):
        at = pl.ds(j * 256, 256)
        piece[:, at] = ((after_in[:, at] - mean) * scale * mid_gain_ref[:, at]).astype(bf16)
    send_results(1)
    gate_part = dot(piece[...], sg[...])
    up_part = dot(piece[...], su[...])
    shidden[...] = (jax.nn.silu(gate_part) * up_part).astype(bf16)

    grid = (SIDE, SIDE, OWN)
    direct_cols = pl.ds(2 * PART, WIDTH - 2 * PART)
    parts = ((0, EARLY_COLS), (EARLY_COLS, PART - EARLY_COLS))

    def partial_columns(first, last):
        for begin in range(first, last, 256):
            at = pl.ds(begin, min(256, last - begin))
            partial[:, :, :, at] = dot(shidden[...], sd[:, at]).astype(bf16).reshape(*grid, at.size)

    def first_sums(part):
        begin, size = parts[part]
        at = pl.ds(begin, size)
        left, right = at, pl.ds(PART + begin, size)
        for d, dev, there in z_peers:
            send(partial.at[there, :, :, left], stage_a.at[d - 1, :, :, at], s6.at[2 * part], r6, 2 * part, dev)
        for d, dev, there in x_peers:
            send(partial.at[:, there, :, right], stage_b.at[d - 1, :, :, at], s6.at[2 * part + 1], r6, 2 * part + 1, dev)

    def second_sums(part):
        begin, size = parts[part]
        at = pl.ds(begin, size)
        left, right = at, pl.ds(PART + begin, size)
        all_of(stage_a.at[:, :, :, at], r6.at[2 * part])
        total = partial[z, :, :, left].astype(f32)
        for d in range(3):
            total = total + stage_a[d, :, :, at].astype(f32)
        sum_a[:, :, at] = total.astype(bf16)
        for d, dev, there in x_peers:
            send(sum_a.at[there, :, at], final_a.at[d - 1, :, at], s6f.at[2 * part], r6f, 2 * part, dev)
        all_of(stage_b.at[:, :, :, at], r6.at[2 * part + 1])
        total = partial[:, x, :, right].astype(f32)
        for d in range(3):
            total = total + stage_b[d, :, :, at].astype(f32)
        sum_b[:, :, at] = total.astype(bf16)
        for d, dev, there in z_peers:
            send(sum_b.at[there, :, at], final_b.at[d - 1, :, at], s6f.at[2 * part + 1], r6f, 2 * part + 1, dev)

    for part, (begin, size) in enumerate(parts):
        partial_columns(begin, begin + size)
        partial_columns(PART + begin, PART + begin + size)
        first_sums(part)
    partial_columns(2 * PART, WIDTH)

    for half, at in enumerate(halves_of_rows):
        all_of(returned.at[pl.ds(0, EP - 1), :, at], r5.at[half])
        for begin in range(0, HALF, 256):
            part_at = pl.ds(half * HALF + begin, 256)
            back = returned[:, :, part_at].reshape(SLOTS, 256)
            part = dot(comb_hi, back) + dot(comb_lo, back)
            routed_part[:, :, :, part_at] = part.astype(bf16).reshape(SIDE, 2, OWN, 256)
        send(routed_part.at[:, 1 - core, :, at], core_in.at[:, :, at], s7.at[half], r7, half, partner)
        all_of(core_in.at[:, :, at], r7.at[half])
        core_sum[:, :, at] = (
            routed_part[:, core, :, at].astype(f32) + core_in[:, :, at].astype(f32)
        ).astype(bf16)
        for d, dev, there in y_peers:
            send(core_sum.at[there, :, at], routed_in.at[d - 1, :, at], s7.at[2 + half], r7, 2 + half, dev)
    for i, (dz, dx) in enumerate(FARTHEST_FIRST):
        to_z, to_x = (z + dz) % SIDE, (x + dx) % SIDE
        send(
            partial.at[to_z, to_x, :, direct_cols], direct_in.at[i], s6d, r6d, 0,
            (to_z * SIDE + to_x, t),
        )
    second_sums(0)
    second_sums(1)
    for half, at in enumerate(halves_of_rows):
        all_of(routed_in.at[:, :, at], r7.at[2 + half])
    routed = core_sum[y].astype(f32) + jnp.sum(routed_in[...].astype(f32), axis=0) + after[own_rows, :]
    for part, (begin, size) in enumerate(parts):
        all_of(final_a.at[:, :, pl.ds(begin, size)], r6f.at[2 * part])
        all_of(final_b.at[:, :, pl.ds(begin, size)], r6f.at[2 * part + 1])
    all_of(direct_in, r6d.at[0])
    own_direct = partial[z, x, :, direct_cols]
    for at, own, others in (
        (pl.ds(0, PART), sum_a[x], final_a), (pl.ds(PART, PART), sum_b[z], final_b),
        (direct_cols, own_direct, direct_in),
    ):
        shared = own.astype(f32) + jnp.sum(others[...].astype(f32), axis=0)
        begin, size = at.start, at.size
        out_ref[:, at] = (routed[:, begin : begin + size] + gate_value * shared).astype(bf16)

    all_of(own_resid.at[:, pl.ds(0, 7 * FEAT)], so.at[0])
    all_of(own_mixed.at[:, pl.ds(0, 7 * CH)], so.at[1])
    all_of(full.at[:, pl.ds(0, 4 * FEAT)], s1)
    all_of(mixed.at[:, pl.ds(0, 7 * CH)], s2)
    all_of(resid_in.at[pl.ds(0, 15)], se)
    all_of(mixed_in.at[pl.ds(0, 15)], sl)
    all_of(slots_in.at[pl.ds(0, EP - 1)], s3)
    for part, (begin, size) in enumerate(parts):
        at = pl.ds(begin, size)
        all_of(stage_a.at[:, :, :, at], s6.at[2 * part])
        all_of(stage_b.at[:, :, :, at], s6.at[2 * part + 1])
        all_of(final_a.at[:, :, at], s6f.at[2 * part])
        all_of(final_b.at[:, :, at], s6f.at[2 * part + 1])
    for half, at in enumerate(halves_of_rows):
        all_of(returned.at[pl.ds(0, EP - 1), :, at], s5.at[half])
        all_of(core_in.at[:, :, at], s7.at[half])
        all_of(routed_in.at[:, :, at], s7.at[2 + half])
    all_of(direct_in, s6d)


def write_out(out_ref, state_ref, out_hbm, state_hbm, sem):
    copies = [
        pltpu.make_async_copy(state_ref, state_hbm, sem.at[0]),
        pltpu.make_async_copy(out_ref, out_hbm, sem.at[1]),
    ]
    for c in copies:
        c.start()
    for c in copies:
        c.wait()


def per_device(
    residual, in_gain, in_weight, state, decay_rate, frequency, log_step, in_coef, out_coef,
    skip_gain, out_weight, mid_gain, gate_vector, routes, route_weight, expert_gate, expert_up,
    expert_down, shared_gate, shared_up, shared_down,
):
    vmem = pl.BlockSpec(memory_space=pltpu.VMEM)
    hbm = pl.BlockSpec(memory_space=pltpu.HBM)
    dma = pltpu.SemaphoreType.DMA
    in_coef_rows = jnp.swapaxes(in_coef, 2, 3).reshape(2, CH, STATE)
    out_coef_rows = out_coef.reshape(2, CH, STATE)
    call = pl.pallas_call(
        kernel,
        name="layer_step",
        out_shape=(
            pltpu.VMEM((OWN, WIDTH), bf16),
            pltpu.VMEM((2, ROWS, GS), f32),
        ),
        in_specs=[hbm] * 21,
        out_specs=(vmem, vmem),
        scratch_shapes=[
            pltpu.VMEM((ROWS, FEAT), bf16),
            pltpu.VMEM((1, WIDTH), f32),
            pltpu.VMEM((GROUPS, STATE), f32),
            pltpu.VMEM((GROUPS, STATE), f32),
            pltpu.VMEM((1, GROUPS), f32),
            pltpu.VMEM((2, CH, STATE), f32),
            pltpu.VMEM((2, CH, STATE), f32),
            pltpu.VMEM((1, CH), f32),
            pltpu.VMEM((1, WIDTH), f32),
            pltpu.VMEM((WIDTH // 128, 128), bf16),
            pltpu.VMEM((4, ROWS), jnp.int32),
            pltpu.VMEM((4, ROWS), f32),
            pltpu.VMEM((ROWS, WIDTH), bf16),
            pltpu.VMEM((WIDTH, CH), bf16),
            pltpu.VMEM((2, ROWS, GS), f32),
            pltpu.VMEM((MIX, WIDTH), bf16),
            pltpu.VMEM((WIDTH, FF), bf16),
            pltpu.VMEM((WIDTH, FF), bf16),
            pltpu.VMEM((FF, WIDTH), bf16),
            pltpu.VMEM((WIDTH, SF), bf16),
            pltpu.VMEM((WIDTH, SF), bf16),
            pltpu.VMEM((SF, WIDTH), bf16),
            pltpu.VMEM((OWN, WIDTH), bf16),
            pltpu.VMEM((OWN, MIX), bf16),
            pltpu.VMEM((ROWS, MIX), bf16),
            pltpu.VMEM((ROWS, WIDTH), f32),
            pltpu.VMEM((TP, OWN, WIDTH), bf16),
            pltpu.VMEM((EP, CAP, WIDTH), bf16),
            pltpu.VMEM((EP, CAP, WIDTH), bf16),
            pltpu.VMEM((EP, OWN, WIDTH), bf16),
            pltpu.VMEM((EP, OWN, MIX), bf16),
            pltpu.VMEM((EP * OWN, WIDTH), f32),
            pltpu.VMEM((EP * OWN, WIDTH), bf16),
            pltpu.VMEM((SLOTS, FF), bf16),
            pltpu.VMEM((EP, CAP, WIDTH), bf16),
            pltpu.VMEM((EP, CAP, WIDTH), bf16),
            pltpu.VMEM((EP * OWN, SF), bf16),
            pltpu.VMEM((SIDE, SIDE, OWN, WIDTH), bf16),
            pltpu.VMEM((SIDE - 1, SIDE, OWN, PART), bf16),
            pltpu.VMEM((SIDE - 1, SIDE, OWN, PART), bf16),
            pltpu.VMEM((SIDE, OWN, PART), bf16),
            pltpu.VMEM((SIDE, OWN, PART), bf16),
            pltpu.VMEM((SIDE - 1, OWN, PART), bf16),
            pltpu.VMEM((SIDE - 1, OWN, PART), bf16),
            pltpu.VMEM((EP - 1, OWN, WIDTH - 2 * PART), bf16),
            pltpu.VMEM((SIDE, 2, OWN, WIDTH), bf16),
            pltpu.VMEM((SIDE, OWN, WIDTH), bf16),
            pltpu.VMEM((SIDE, OWN, WIDTH), bf16),
            pltpu.VMEM((SIDE - 1, OWN, WIDTH), bf16),
            dma((21,)),
            dma((2,)), dma((2,)),
            dma, dma((8,)),
            dma, dma((4,)),
            dma, dma((8,)),
            dma, dma((8,)),
            dma, dma((1,)),
            dma((2,)), dma((2,)),
            dma((4,)), dma((4,)),
            dma, dma((1,)),
            dma((4,)), dma((4,)),
            dma((4,)), dma((4,)),
        ],
        compiler_params=pltpu.CompilerParams(
            collective_id=0, has_side_effects=True, vmem_limit_bytes=VMEM_MIB * 1024 * 1024
        ),
    )
    operands = (
        residual, in_gain.reshape(1, WIDTH), in_weight, state, decay_rate, frequency,
        log_step.reshape(1, GROUPS), in_coef_rows, out_coef_rows, skip_gain.reshape(1, CH),
        out_weight, mid_gain.reshape(1, WIDTH), gate_vector.reshape(WIDTH // 128, 128), routes.T,
        route_weight.T, expert_gate[0], expert_up[0], expert_down[0], shared_gate, shared_up,
        shared_down,
    )
    results = call(*[pltpu.with_memory_space_constraint(a, pltpu.HBM) for a in operands])
    return pl.pallas_call(
        write_out,
        name="write_out",
        out_shape=(
            jax.ShapeDtypeStruct((OWN, WIDTH), bf16),
            jax.ShapeDtypeStruct((2, ROWS, GS), f32),
        ),
        in_specs=[vmem, vmem],
        out_specs=(hbm, hbm),
        scratch_shapes=[dma((2,))],
    )(*[pltpu.with_memory_space_constraint(a, pltpu.VMEM) for a in results])


def solution(mesh):
    return jax.shard_map(
        per_device,
        mesh=mesh,
        in_specs=(
            P("ep", "tp"), P(), P(None, "tp"), P(None, "ep", "tp"), P("tp", None), P("tp", None),
            P("tp"), P(None, "tp", None, None), P(None, "tp", None, None), P("tp"), P(), P(), P(),
            P("ep", None), P("ep", None), P(("ep", "tp"), None, None), P(("ep", "tp"), None, None),
            P(("ep", "tp"), None, None), P(None, "ep"), P(None, "ep"), P("ep", None),
        ),
        out_specs=(P(("ep", "tp"), None), P(None, "ep", "tp")),
        check_vma=False,
    )
```

```python
import jax
import jax.numpy as jnp
from jax import lax
from jax.experimental import pallas as pl
from jax.experimental.pallas import tpu as pltpu
from jax.sharding import PartitionSpec as P

MESH = pl.DeviceIdType.MESH
norm_eps = 1e-05
routed_scale = 2.5
f32, bf16 = jnp.float32, jnp.bfloat16

TP, EP = 8, 16
ROWS, WIDTH, FEAT = 128, 2048, 256
CH, GROUPS, STATE, GCH = 128, 8, 64, 16
GS = GROUPS * STATE
CAP, OWN = 8, 16
SIDE = 4
HALF = WIDTH // 2
SLOTS = EP * CAP
FF, SF = 512, 256
MIX = CH * TP
FARTHEST_FIRST = sorted(
    [(dz, dx) for dz in range(SIDE) for dx in range(SIDE) if dz + dx],
    key=lambda s: -min(s[0], SIDE - s[0]) - min(s[1], SIDE - s[1]),
)
VMEM_MIB = 48
PART = 896
OWN_AFTER = 3
EARLY_COLS = 640
EARLY_PEERS = 15


def dot(a, b):
    return jnp.dot(a, b, preferred_element_type=f32)


def dot_nt(a, b):
    return lax.dot_general(a, b, (((1,), (1,)), ((), ())), preferred_element_type=f32)


def dot_tn(a, b):
    return lax.dot_general(a, b, (((0,), (0,)), ((), ())), preferred_element_type=f32)


def halves(a):
    high = a.astype(bf16)
    return high, (a - high.astype(f32)).astype(bf16)


def lanes_of_groups(a):
    return jnp.concatenate([a[g : g + 1, :] for g in range(GROUPS)], axis=1)


def block_diagonal(a):
    wide = jnp.concatenate([a] * GROUPS, axis=1)
    row = lax.broadcasted_iota(jnp.int32, (CH, GS), 0) // GCH
    col = lax.broadcasted_iota(jnp.int32, (CH, GS), 1) // STATE
    return jnp.where(row == col, wide, 0.0)


def per_group_rows(a):
    return jnp.broadcast_to(a[:, None, :], (GROUPS, GCH, STATE)).reshape(CH, STATE)


def kernel(
    resid_hbm, in_gain_hbm, in_w_hbm, state_hbm, decay_hbm, freq_hbm, step_hbm, in_coef_hbm,
    out_coef_hbm, skip_hbm, out_w_hbm, mid_gain_hbm, gate_vec_hbm, routes_hbm, weights_hbm,
    eg_hbm, eu_hbm, ed_hbm, sg_hbm, su_hbm, sd_hbm,
    out_ref, new_state_ref,
    resid_ref, in_gain_ref, decay_ref, freq_ref, step_ref, in_coef_ref, out_coef_ref, skip_ref,
    mid_gain_ref, gate_vec_ref, routes_ref, weights_ref,
    full, in_w, state, out_w, eg, eu, ed, sg, su, sd,
    own_resid, own_mixed, mixed, after, outgoing, slots_in, resid_in, mixed_in, after_in, piece, hidden, result, returned,
    shidden, partial, stage_a, stage_b, sum_a, sum_b, final_a, final_b, direct_in,
    routed_part, core_in, core_sum, routed_in,
    local_sem, so, ro, s1, r1, s2, r2, se, re, sl, rl, s3, r3, s5, r5, s6, r6, s6d, r6d, s6f, r6f, s7, r7,
):
    e = lax.axis_index("ep")
    t = lax.axis_index("tp")
    z, x = e // SIDE, e % SIDE
    y, core = t // 2, t % 2
    tp_peers = [
        (dy * 2 + dc, (e, ((y + dy) % SIDE) * 2 + (core + dc) % 2))
        for dy in (2, 1, 3, 0) for dc in (0, 1) if dy + dc
    ]
    ep_peers = [
        (dz * SIDE + dx, (((z + dz) % SIDE) * SIDE + (x + dx) % SIDE, t))
        for dz, dx in FARTHEST_FIRST
    ]
    x_peers = [(d, (z * SIDE + (x + d) % SIDE, t), (x + d) % SIDE) for d in (2, 1, 3)]
    z_peers = [(d, (((z + d) % SIDE) * SIDE + x, t), (z + d) % SIDE) for d in (2, 1, 3)]
    y_peers = [(d, (e, ((y + d) % SIDE) * 2 + core), (y + d) % SIDE) for d in (2, 1, 3)]
    partner = (e, y * 2 + (1 - core))

    barrier = pltpu.get_barrier_semaphore()
    near = [dev for _, dev in tp_peers] + [peer[1] for peer in x_peers + z_peers]
    for dev in near:
        pl.semaphore_signal(barrier, inc=1, device_id=dev, device_id_type=MESH)

    fetches = {}
    for i, (name, src, dst) in enumerate([
        ("resid", resid_hbm, resid_ref), ("decay", decay_hbm, decay_ref),
        ("freq", freq_hbm, freq_ref), ("step", step_hbm, step_ref),
        ("in_coef", in_coef_hbm, in_coef_ref), ("out_coef", out_coef_hbm, out_coef_ref),
        ("routes", routes_hbm, routes_ref), ("weights", weights_hbm, weights_ref),
        ("skip", skip_hbm, skip_ref), ("in_gain", in_gain_hbm, in_gain_ref),
        ("state", state_hbm, state), ("in_w", in_w_hbm, in_w),
        ("mid_gain", mid_gain_hbm, mid_gain_ref), ("gate_vec", gate_vec_hbm, gate_vec_ref),
        ("out_w", out_w_hbm, out_w),
        ("eg", eg_hbm, eg), ("eu", eu_hbm, eu), ("ed", ed_hbm, ed),
        ("sg", sg_hbm, sg), ("su", su_hbm, su), ("sd", sd_hbm, sd),
    ]):
        fetches[name] = pltpu.make_async_copy(src, dst, local_sem.at[i])
        fetches[name].start()

    def fetched(*names):
        for name in names:
            fetches[name].wait()

    def send(src, dst, ss, rs, d, dev):
        copy = pltpu.make_async_remote_copy(
            src_ref=src, dst_ref=dst, send_sem=ss, recv_sem=rs.at[d],
            device_id=dev, device_id_type=MESH,
        )
        copy.start()

    def all_of(ref, sem):
        pltpu.make_async_copy(ref, ref, sem).wait()

    own_rows = pl.ds(pl.multiple_of(t * OWN, OWN), OWN)

    pl.semaphore_wait(barrier, len(near))

    fetched("resid")
    cols = pl.ds(pl.multiple_of(t * FEAT, FEAT), FEAT)
    for _, dev in tp_peers:
        rows = pl.ds(pl.multiple_of(dev[1] * OWN, OWN), OWN)
        send(resid_ref.at[rows], own_resid.at[:, cols], so.at[0], ro, 0, dev)
    for d, _, there in y_peers:
        for c in (0, 1):
            @pl.when(core == c)
            def _():
                send(resid_ref, full.at[:, cols], s1, r1, 2 * d + c, (e, there * 2 + 1))
    send(resid_ref, full.at[:, cols], s1, r1, 0, partner)
    full[:, cols] = resid_ref[...]
    own_resid[:, cols] = resid_ref[own_rows, :]

    fetched("decay", "freq", "step", "in_coef", "out_coef")
    own_lane = (
        lax.broadcasted_iota(jnp.int32, (GROUPS, GROUPS), 0)
        == lax.broadcasted_iota(jnp.int32, (GROUPS, GROUPS), 1)
    )
    log_step = jnp.sum(jnp.where(own_lane, step_ref[...], 0.0), axis=1, keepdims=True)
    dt = jnp.exp(log_step)
    rate = -decay_ref[...]
    freq = freq_ref[...]
    magnitude = jnp.exp(rate * dt)
    keep_re = magnitude * jnp.cos(freq * dt)
    keep_im = magnitude * jnp.sin(freq * dt)
    denominator = rate * rate + freq * freq
    factor_re = ((keep_re - 1.0) * rate + keep_im * freq) / denominator
    factor_im = (keep_im * rate - (keep_re - 1.0) * freq) / denominator
    fr, fi = per_group_rows(factor_re), per_group_rows(factor_im)
    push_re = block_diagonal(fr * in_coef_ref[0] - fi * in_coef_ref[1])
    push_im = block_diagonal(fr * in_coef_ref[1] + fi * in_coef_ref[0])
    pr_hi, pr_lo = halves(push_re)
    pi_hi, pi_lo = halves(push_im)
    out_re = block_diagonal(out_coef_ref[0]).astype(bf16)
    out_im = block_diagonal(out_coef_ref[1]).astype(bf16)
    kr, ki = lanes_of_groups(keep_re), lanes_of_groups(keep_im)

    fetched("routes", "weights")
    slot_row = lax.broadcasted_iota(jnp.int32, (SLOTS, ROWS), 0)
    expert = (slot_row // CAP) * TP + t
    weight_sum = jnp.sum(weights_ref[...], axis=0, keepdims=True)
    weights = weights_ref[...] / weight_sum * routed_scale
    chosen = jnp.zeros((SLOTS, ROWS), f32)
    chosen_weight = jnp.zeros((SLOTS, ROWS), f32)
    for k in range(4):
        same = routes_ref[k : k + 1, :] == expert
        chosen = jnp.where(same, 1.0, chosen)
        chosen_weight = jnp.where(same, weights[k : k + 1, :], chosen_weight)
    earlier = (
        lax.broadcasted_iota(jnp.int32, (ROWS, ROWS), 0)
        < lax.broadcasted_iota(jnp.int32, (ROWS, ROWS), 1)
    )
    before = dot(chosen.astype(bf16), jnp.where(earlier, 1.0, 0.0).astype(bf16))
    rank = (slot_row % CAP).astype(f32)
    holds = (chosen > 0.5) & (before == rank)
    pick = jnp.where(holds, 1.0, 0.0).astype(bf16)
    combine = jnp.where(holds, chosen_weight, 0.0).T
    comb_hi, comb_lo = halves(combine)

    fetched("state", "in_w", "in_gain", "skip")
    old_re, old_im = state[0], state[1]
    kept_re = kr * old_re - ki * old_im
    kept_im = kr * old_im + ki * old_re
    new_state_ref[0] = kept_re
    new_state_ref[1] = kept_im
    read_kept = dot_nt(kept_re.astype(bf16), out_re) - dot_nt(kept_im.astype(bf16), out_im)
    read_push = (dot_nt(pr_hi, out_re) + dot_nt(pr_lo, out_re)) - (dot_nt(pi_hi, out_im) + dot_nt(pi_lo, out_im))
    rp_hi, rp_lo = halves(read_push)
    def first_step(src, dst, width, ss, rs):
        left, right = pl.ds(0, width), pl.ds(width, width)
        for k, (a, b) in enumerate(((left, right), (right, left))):
            for (d, dev_x, _), (_, dev_z, _) in zip(x_peers, z_peers, strict=True):
                send(src.at[:, a], dst.at[e, :, a], ss, rs, d if k == 0 else 0, dev_x)
                send(src.at[:, b], dst.at[e, :, b], ss, rs, 4 + d if k == 0 else 0, dev_z)

    def second_step(dst, width, ss, rs):
        left, right = pl.ds(0, width), pl.ds(width, width)
        for d in (1, 3, 2):
            block = dst.at[z * SIDE + (x + SIDE - d) % SIDE, :, left]
            all_of(block, rs.at[d])
            for _, dev, _ in z_peers:
                send(block, block, ss, rs, 0, dev)
            block = dst.at[((z + SIDE - d) % SIDE) * SIDE + x, :, right]
            all_of(block, rs.at[4 + d])
            for _, dev, _ in x_peers:
                send(block, block, ss, rs, 0, dev)

    all_of(own_resid.at[:, pl.ds(0, 7 * FEAT)], ro.at[0])
    first_step(own_resid, resid_in, HALF, se, re)
    resid_in[e] = own_resid[...]
    @pl.when(core == 1)
    def _():
        for d in (1, 3, 2):
            for c in (1, 0):
                at = (((y + SIDE - d) % SIDE) * 2 + c) * FEAT
                theirs = full.at[:, pl.ds(pl.multiple_of(at, FEAT), FEAT)]
                all_of(theirs, r1.at[2 * d + c])
                send(theirs, theirs, s1, r1, 0, partner)
        all_of(full.at[:, pl.ds(0, FEAT)], r1.at[0])
        all_of(full.at[:, pl.ds(0, 6 * FEAT)], s1)

    @pl.when(core == 0)
    def _():
        all_of(full.at[:, pl.ds(0, 7 * FEAT)], r1.at[0])

    values = full[...].astype(f32)
    mean = jnp.sum(values, axis=1, keepdims=True) * (1.0 / WIDTH)
    square = jnp.sum(values * values, axis=1, keepdims=True) * (1.0 / WIDTH)
    scale = lax.rsqrt(square - mean * mean + norm_eps)
    normed = ((values - mean) * scale * in_gain_ref[...]).astype(bf16)
    drive = dot(normed, in_w[...]).astype(bf16)
    read = read_kept + (dot(drive, rp_hi) + dot(drive, rp_lo)) + skip_ref[...] * drive.astype(f32)
    mixed_cols = pl.ds(pl.multiple_of(t * CH, CH), CH)
    mixed_part = jax.nn.gelu(read, approximate=True).astype(bf16)
    mixed[:, mixed_cols] = mixed_part

    for _, dev in tp_peers:
        rows = pl.ds(pl.multiple_of(dev[1] * OWN, OWN), OWN)
        send(mixed.at[rows, mixed_cols], own_mixed.at[:, mixed_cols], so.at[1], ro, 1, dev)
    own_mixed[:, mixed_cols] = mixed[own_rows, mixed_cols]
    for d, _, there in y_peers:
        send(mixed.at[:, mixed_cols], mixed.at[:, mixed_cols], s2, r2, d, (e, there * 2 + 1))
    send(mixed.at[:, mixed_cols], mixed.at[:, mixed_cols], s2, r2, 0, partner)
    new_state_ref[0] = new_state_ref[0] + (dot(drive, pr_hi) + dot(drive, pr_lo))
    new_state_ref[1] = new_state_ref[1] + (dot(drive, pi_hi) + dot(drive, pi_lo))
    second_step(resid_in, HALF, se, re)
    fetched("out_w", "mid_gain")
    sums = [jnp.zeros((ROWS, 128), f32), jnp.zeros((ROWS, 128), f32)]
    for dy in (0, 1, 3, 2):
        deep = pl.ds(pl.multiple_of(((y + SIDE - dy) % SIDE) * 256, 256), 256)
        if dy:
            all_of(mixed.at[:, deep], r2.at[dy])

            @pl.when(core == 1)
            def _():
                send(mixed.at[:, deep], mixed.at[:, deep], s2, r2, dy, partner)
        else:
            other = pl.ds(pl.multiple_of((y * 2 + (1 - core)) * CH, CH), CH)
            all_of(mixed.at[:, other], r2.at[0])
        block = mixed[:, deep]
        for j in range(WIDTH // 256):
            at = pl.ds(j * 256, 256)
            base = full[:, at].astype(f32) if dy == 0 else after[:, at]
            part = base + dot(block, out_w[deep, at])
            after[:, at] = part
            if dy == 2:
                for lanes in (part[:, :128], part[:, 128:]):
                    sums[0] = sums[0] + lanes
                    sums[1] = sums[1] + lanes * lanes
        if dy == OWN_AFTER:
            all_of(own_mixed.at[:, pl.ds(0, 7 * CH)], ro.at[1])
            first_step(own_mixed, mixed_in, MIX // 2, sl, rl)
            mixed_in[e] = own_mixed[...]
    mean = jnp.sum(sums[0], axis=1, keepdims=True) * (1.0 / WIDTH)
    square = jnp.sum(sums[1], axis=1, keepdims=True) * (1.0 / WIDTH)
    scale = lax.rsqrt(square - mean * mean + norm_eps)
    for j in range(WIDTH // 256):
        at = pl.ds(j * 256, 256)
        part = ((after[:, at] - mean) * scale * mid_gain_ref[:, at]).astype(bf16)
        outgoing[:, :, at] = dot(pick, part).astype(bf16).reshape(EP, CAP, 256)

    for d, dev in ep_peers[:EARLY_PEERS]:
        send(outgoing.at[dev[0]], slots_in.at[e], s3, r3, 0, dev)
    slots_in[e] = outgoing[e]
    own_after = after[own_rows, :]
    mean = jnp.sum(own_after, axis=1, keepdims=True) * (1.0 / WIDTH)
    square = jnp.sum(own_after * own_after, axis=1, keepdims=True) * (1.0 / WIDTH)
    own_mid = ((own_after - mean) * lax.rsqrt(square - mean * mean + norm_eps) * mid_gain_ref[...]).astype(bf16)
    fetched("gate_vec")
    gate_vec = jnp.concatenate([gate_vec_ref[i : i + 1, :] for i in range(WIDTH // 128)], axis=1)
    gate_value = jax.nn.sigmoid(
        jnp.sum(own_mid.astype(f32) * gate_vec.astype(f32), axis=1, keepdims=True)
    )
    second_step(mixed_in, MIX // 2, sl, rl)
    for d, dev in ep_peers[EARLY_PEERS:]:
        send(outgoing.at[dev[0]], slots_in.at[e], s3, r3, 0, dev)

    fetched("eg", "eu", "ed")
    all_of(slots_in.at[pl.ds(0, EP - 1)], r3.at[0])
    rows = slots_in[...].reshape(SLOTS, WIDTH)
    for j in range(FF // 256):
        at = pl.ds(j * 256, 256)
        gate_part = dot(rows, eg[:, at])
        up_part = dot(rows, eu[:, at])
        hidden[:, at] = (jax.nn.silu(gate_part) * up_part).astype(bf16)

    halves_of_rows = (pl.ds(0, HALF), pl.ds(HALF, HALF))

    def send_results(half):
        at = halves_of_rows[half]
        for _, dev in ep_peers:
            send(result.at[dev[0], :, at], returned.at[e, :, at], s5.at[half], r5, half, dev)

    for j in range(WIDTH // 256):
        at = pl.ds(j * 256, 256)
        result[:, :, at] = dot(hidden[...], ed[:, at]).astype(bf16).reshape(EP, CAP, 256)
        if j == HALF // 256 - 1:
            send_results(0)

    returned[e] = result[e]

    fetched("sg", "su", "sd")
    all_of(resid_in.at[pl.ds(0, 12)], re.at[0])
    all_of(mixed_in.at[pl.ds(0, 12)], rl.at[0])
    channels = mixed_in[...].reshape(EP * OWN, MIX)
    sums = [jnp.zeros((EP * OWN, 128), f32), jnp.zeros((EP * OWN, 128), f32)]
    for j in range(WIDTH // 256):
        at = pl.ds(j * 256, 256)
        part = resid_in[:, :, at].reshape(EP * OWN, 256).astype(f32) + dot(channels, out_w[:, at])
        after_in[:, at] = part
        for lanes in (part[:, :128], part[:, 128:]):
            sums[0] = sums[0] + lanes
            sums[1] = sums[1] + lanes * lanes
    mean = jnp.sum(sums[0], axis=1, keepdims=True) * (1.0 / WIDTH)
    square = jnp.sum(sums[1], axis=1, keepdims=True) * (1.0 / WIDTH)
    scale = lax.rsqrt(square - mean * mean + norm_eps)
    for j in range(WIDTH // 256):
        at = pl.ds(j * 256, 256)
        piece[:, at] = ((after_in[:, at] - mean) * scale * mid_gain_ref[:, at]).astype(bf16)
    send_results(1)
    gate_part = dot(piece[...], sg[...])
    up_part = dot(piece[...], su[...])
    shidden[...] = (jax.nn.silu(gate_part) * up_part).astype(bf16)

    grid = (SIDE, SIDE, OWN)
    direct_cols = pl.ds(2 * PART, WIDTH - 2 * PART)
    parts = ((0, EARLY_COLS), (EARLY_COLS, PART - EARLY_COLS))

    def partial_columns(first, last):
        for begin in range(first, last, 256):
            at = pl.ds(begin, min(256, last - begin))
            partial[:, :, :, at] = dot(shidden[...], sd[:, at]).astype(bf16).reshape(*grid, at.size)

    def first_sums(part):
        begin, size = parts[part]
        at = pl.ds(begin, size)
        left, right = at, pl.ds(PART + begin, size)
        for d, dev, there in z_peers:
            send(partial.at[there, :, :, left], stage_a.at[d - 1, :, :, at], s6.at[2 * part], r6, 2 * part, dev)
        for d, dev, there in x_peers:
            send(partial.at[:, there, :, right], stage_b.at[d - 1, :, :, at], s6.at[2 * part + 1], r6, 2 * part + 1, dev)

    def second_sums(part):
        begin, size = parts[part]
        at = pl.ds(begin, size)
        left, right = at, pl.ds(PART + begin, size)
        all_of(stage_a.at[:, :, :, at], r6.at[2 * part])
        total = partial[z, :, :, left].astype(f32)
        for d in range(3):
            total = total + stage_a[d, :, :, at].astype(f32)
        sum_a[:, :, at] = total.astype(bf16)
        for d, dev, there in x_peers:
            send(sum_a.at[there, :, at], final_a.at[d - 1, :, at], s6f.at[2 * part], r6f, 2 * part, dev)
        all_of(stage_b.at[:, :, :, at], r6.at[2 * part + 1])
        total = partial[:, x, :, right].astype(f32)
        for d in range(3):
            total = total + stage_b[d, :, :, at].astype(f32)
        sum_b[:, :, at] = total.astype(bf16)
        for d, dev, there in z_peers:
            send(sum_b.at[there, :, at], final_b.at[d - 1, :, at], s6f.at[2 * part + 1], r6f, 2 * part + 1, dev)

    for part, (begin, size) in enumerate(parts):
        partial_columns(begin, begin + size)
        partial_columns(PART + begin, PART + begin + size)
        first_sums(part)
    partial_columns(2 * PART, WIDTH)

    def combine_half(half):
        at = halves_of_rows[half]
        all_of(returned.at[pl.ds(0, EP - 1), :, at], r5.at[half])
        for begin in range(0, HALF, 256):
            part_at = pl.ds(half * HALF + begin, 256)
            back = returned[:, :, part_at].reshape(SLOTS, 256)
            part = dot(comb_hi, back) + dot(comb_lo, back)
            routed_part[:, :, :, part_at] = part.astype(bf16).reshape(SIDE, 2, OWN, 256)
        send(routed_part.at[:, 1 - core, :, at], core_in.at[:, :, at], s7.at[half], r7, half, partner)

    def sum_over_tp(half):
        at = halves_of_rows[half]
        all_of(core_in.at[:, :, at], r7.at[half])
        core_sum[:, :, at] = (
            routed_part[:, core, :, at].astype(f32) + core_in[:, :, at].astype(f32)
        ).astype(bf16)
        for d, dev, there in y_peers:
            send(core_sum.at[there, :, at], routed_in.at[d - 1, :, at], s7.at[2 + half], r7, 2 + half, dev)

    def send_direct():
        for i, (dz, dx) in enumerate(FARTHEST_FIRST):
            to_z, to_x = (z + dz) % SIDE, (x + dx) % SIDE
            send(
                partial.at[to_z, to_x, :, direct_cols], direct_in.at[i], s6d, r6d, 0,
                (to_z * SIDE + to_x, t),
            )

    combine_half(0)

    @pl.when(core == 0)
    def _():
        sum_over_tp(0)

    combine_half(1)

    @pl.when(core == 1)
    def _():
        second_sums(0)
        send_direct()
        sum_over_tp(0)

    sum_over_tp(1)

    @pl.when(core == 0)
    def _():
        send_direct()
        second_sums(0)

    second_sums(1)
    for half, at in enumerate(halves_of_rows):
        all_of(routed_in.at[:, :, at], r7.at[2 + half])
    routed = core_sum[y].astype(f32) + jnp.sum(routed_in[...].astype(f32), axis=0) + after[own_rows, :]
    for part, (begin, size) in enumerate(parts):
        all_of(final_a.at[:, :, pl.ds(begin, size)], r6f.at[2 * part])
        all_of(final_b.at[:, :, pl.ds(begin, size)], r6f.at[2 * part + 1])
    all_of(direct_in, r6d.at[0])
    own_direct = partial[z, x, :, direct_cols]
    for at, own, others in (
        (pl.ds(0, PART), sum_a[x], final_a), (pl.ds(PART, PART), sum_b[z], final_b),
        (direct_cols, own_direct, direct_in),
    ):
        shared = own.astype(f32) + jnp.sum(others[...].astype(f32), axis=0)
        begin, size = at.start, at.size
        out_ref[:, at] = (routed[:, begin : begin + size] + gate_value * shared).astype(bf16)

    all_of(own_resid.at[:, pl.ds(0, 7 * FEAT)], so.at[0])
    all_of(own_mixed.at[:, pl.ds(0, 7 * CH)], so.at[1])
    all_of(full.at[:, pl.ds(0, 4 * FEAT)], s1)
    all_of(mixed.at[:, pl.ds(0, 4 * CH)], s2)

    @pl.when(core == 1)
    def _():
        all_of(mixed.at[:, pl.ds(0, 6 * CH)], s2)

    all_of(resid_in.at[pl.ds(0, 15)], se)
    all_of(mixed_in.at[pl.ds(0, 15)], sl)
    all_of(slots_in.at[pl.ds(0, EP - 1)], s3)
    for part, (begin, size) in enumerate(parts):
        at = pl.ds(begin, size)
        all_of(stage_a.at[:, :, :, at], s6.at[2 * part])
        all_of(stage_b.at[:, :, :, at], s6.at[2 * part + 1])
        all_of(final_a.at[:, :, at], s6f.at[2 * part])
        all_of(final_b.at[:, :, at], s6f.at[2 * part + 1])
    for half, at in enumerate(halves_of_rows):
        all_of(returned.at[pl.ds(0, EP - 1), :, at], s5.at[half])
        all_of(core_in.at[:, :, at], s7.at[half])
        all_of(routed_in.at[:, :, at], s7.at[2 + half])
    all_of(direct_in, s6d)


def write_out(out_ref, state_ref, out_hbm, state_hbm, sem):
    copies = [
        pltpu.make_async_copy(state_ref, state_hbm, sem.at[0]),
        pltpu.make_async_copy(out_ref, out_hbm, sem.at[1]),
    ]
    for c in copies:
        c.start()
    for c in copies:
        c.wait()


def per_device(
    residual, in_gain, in_weight, state, decay_rate, frequency, log_step, in_coef, out_coef,
    skip_gain, out_weight, mid_gain, gate_vector, routes, route_weight, expert_gate, expert_up,
    expert_down, shared_gate, shared_up, shared_down,
):
    vmem = pl.BlockSpec(memory_space=pltpu.VMEM)
    hbm = pl.BlockSpec(memory_space=pltpu.HBM)
    dma = pltpu.SemaphoreType.DMA
    in_coef_rows = jnp.swapaxes(in_coef, 2, 3).reshape(2, CH, STATE)
    out_coef_rows = out_coef.reshape(2, CH, STATE)
    call = pl.pallas_call(
        kernel,
        name="layer_step",
        out_shape=(
            pltpu.VMEM((OWN, WIDTH), bf16),
            pltpu.VMEM((2, ROWS, GS), f32),
        ),
        in_specs=[hbm] * 21,
        out_specs=(vmem, vmem),
        scratch_shapes=[
            pltpu.VMEM((ROWS, FEAT), bf16),
            pltpu.VMEM((1, WIDTH), f32),
            pltpu.VMEM((GROUPS, STATE), f32),
            pltpu.VMEM((GROUPS, STATE), f32),
            pltpu.VMEM((1, GROUPS), f32),
            pltpu.VMEM((2, CH, STATE), f32),
            pltpu.VMEM((2, CH, STATE), f32),
            pltpu.VMEM((1, CH), f32),
            pltpu.VMEM((1, WIDTH), f32),
            pltpu.VMEM((WIDTH // 128, 128), bf16),
            pltpu.VMEM((4, ROWS), jnp.int32),
            pltpu.VMEM((4, ROWS), f32),
            pltpu.VMEM((ROWS, WIDTH), bf16),
            pltpu.VMEM((WIDTH, CH), bf16),
            pltpu.VMEM((2, ROWS, GS), f32),
            pltpu.VMEM((MIX, WIDTH), bf16),
            pltpu.VMEM((WIDTH, FF), bf16),
            pltpu.VMEM((WIDTH, FF), bf16),
            pltpu.VMEM((FF, WIDTH), bf16),
            pltpu.VMEM((WIDTH, SF), bf16),
            pltpu.VMEM((WIDTH, SF), bf16),
            pltpu.VMEM((SF, WIDTH), bf16),
            pltpu.VMEM((OWN, WIDTH), bf16),
            pltpu.VMEM((OWN, MIX), bf16),
            pltpu.VMEM((ROWS, MIX), bf16),
            pltpu.VMEM((ROWS, WIDTH), f32),
            pltpu.VMEM((EP, CAP, WIDTH), bf16),
            pltpu.VMEM((EP, CAP, WIDTH), bf16),
            pltpu.VMEM((EP, OWN, WIDTH), bf16),
            pltpu.VMEM((EP, OWN, MIX), bf16),
            pltpu.VMEM((EP * OWN, WIDTH), f32),
            pltpu.VMEM((EP * OWN, WIDTH), bf16),
            pltpu.VMEM((SLOTS, FF), bf16),
            pltpu.VMEM((EP, CAP, WIDTH), bf16),
            pltpu.VMEM((EP, CAP, WIDTH), bf16),
            pltpu.VMEM((EP * OWN, SF), bf16),
            pltpu.VMEM((SIDE, SIDE, OWN, WIDTH), bf16),
            pltpu.VMEM((SIDE - 1, SIDE, OWN, PART), bf16),
            pltpu.VMEM((SIDE - 1, SIDE, OWN, PART), bf16),
            pltpu.VMEM((SIDE, OWN, PART), bf16),
            pltpu.VMEM((SIDE, OWN, PART), bf16),
            pltpu.VMEM((SIDE - 1, OWN, PART), bf16),
            pltpu.VMEM((SIDE - 1, OWN, PART), bf16),
            pltpu.VMEM((EP - 1, OWN, WIDTH - 2 * PART), bf16),
            pltpu.VMEM((SIDE, 2, OWN, WIDTH), bf16),
            pltpu.VMEM((SIDE, OWN, WIDTH), bf16),
            pltpu.VMEM((SIDE, OWN, WIDTH), bf16),
            pltpu.VMEM((SIDE - 1, OWN, WIDTH), bf16),
            dma((21,)),
            dma((2,)), dma((2,)),
            dma, dma((8,)),
            dma, dma((4,)),
            dma, dma((8,)),
            dma, dma((8,)),
            dma, dma((1,)),
            dma((2,)), dma((2,)),
            dma((4,)), dma((4,)),
            dma, dma((1,)),
            dma((4,)), dma((4,)),
            dma((4,)), dma((4,)),
        ],
        compiler_params=pltpu.CompilerParams(
            collective_id=0, has_side_effects=True, vmem_limit_bytes=VMEM_MIB * 1024 * 1024
        ),
    )
    operands = (
        residual, in_gain.reshape(1, WIDTH), in_weight, state, decay_rate, frequency,
        log_step.reshape(1, GROUPS), in_coef_rows, out_coef_rows, skip_gain.reshape(1, CH),
        out_weight, mid_gain.reshape(1, WIDTH), gate_vector.reshape(WIDTH // 128, 128), routes.T,
        route_weight.T, expert_gate[0], expert_up[0], expert_down[0], shared_gate, shared_up,
        shared_down,
    )
    results = call(*[pltpu.with_memory_space_constraint(a, pltpu.HBM) for a in operands])
    return pl.pallas_call(
        write_out,
        name="write_out",
        out_shape=(
            jax.ShapeDtypeStruct((OWN, WIDTH), bf16),
            jax.ShapeDtypeStruct((2, ROWS, GS), f32),
        ),
        in_specs=[vmem, vmem],
        out_specs=(hbm, hbm),
        scratch_shapes=[dma((2,))],
    )(*[pltpu.with_memory_space_constraint(a, pltpu.VMEM) for a in results])


def solution(mesh):
    return jax.shard_map(
        per_device,
        mesh=mesh,
        in_specs=(
            P("ep", "tp"), P(), P(None, "tp"), P(None, "ep", "tp"), P("tp", None), P("tp", None),
            P("tp"), P(None, "tp", None, None), P(None, "tp", None, None), P("tp"), P(), P(), P(),
            P("ep", None), P("ep", None), P(("ep", "tp"), None, None), P(("ep", "tp"), None, None),
            P(("ep", "tp"), None, None), P(None, "ep"), P(None, "ep"), P("ep", None),
        ),
        out_specs=(P(("ep", "tp"), None), P(None, "ep", "tp")),
        check_vma=False,
    )
```

```python
import jax
import jax.numpy as jnp
from jax import lax
from jax.experimental import pallas as pl
from jax.experimental.pallas import tpu as pltpu
from jax.sharding import PartitionSpec as P

MESH = pl.DeviceIdType.MESH
norm_eps = 1e-05
routed_scale = 2.5
f32, bf16 = jnp.float32, jnp.bfloat16

TP, EP = 8, 16
ROWS, WIDTH, FEAT = 128, 2048, 256
CH, GROUPS, STATE, GCH = 128, 8, 64, 16
GS = GROUPS * STATE
CAP, OWN = 8, 16
SIDE = 4
HALF = WIDTH // 2
SLOTS = EP * CAP
FF, SF = 512, 256
MIX = CH * TP
OFFSETS = (
    [(2, 1), (2, 3), (1, 2), (3, 2), (0, 1), (0, 3), (1, 0), (3, 0)]
    + [(2, 2), (1, 1), (1, 3), (3, 1), (3, 3), (0, 2), (2, 0)]
)
GROUP = EP // 2
VMEM_MIB = 48
PART = 896
OWN_AFTER = 3
EARLY_COLS = 640
EARLY_PEERS = 15


def dot(a, b):
    return jnp.dot(a, b, preferred_element_type=f32)


def dot_nt(a, b):
    return lax.dot_general(a, b, (((1,), (1,)), ((), ())), preferred_element_type=f32)


def dot_tn(a, b):
    return lax.dot_general(a, b, (((0,), (0,)), ((), ())), preferred_element_type=f32)


def halves(a):
    high = a.astype(bf16)
    return high, (a - high.astype(f32)).astype(bf16)


def lanes_of_groups(a):
    return jnp.concatenate([a[g : g + 1, :] for g in range(GROUPS)], axis=1)


def block_diagonal(a):
    wide = jnp.concatenate([a] * GROUPS, axis=1)
    row = lax.broadcasted_iota(jnp.int32, (CH, GS), 0) // GCH
    col = lax.broadcasted_iota(jnp.int32, (CH, GS), 1) // STATE
    return jnp.where(row == col, wide, 0.0)


def per_group_rows(a):
    return jnp.broadcast_to(a[:, None, :], (GROUPS, GCH, STATE)).reshape(CH, STATE)


def kernel(
    resid_hbm, in_gain_hbm, in_w_hbm, state_hbm, decay_hbm, freq_hbm, step_hbm, in_coef_hbm,
    out_coef_hbm, skip_hbm, out_w_hbm, mid_gain_hbm, gate_vec_hbm, routes_hbm, weights_hbm,
    eg_hbm, eu_hbm, ed_hbm, sg_hbm, su_hbm, sd_hbm,
    out_ref, new_state_ref,
    resid_ref, in_gain_ref, decay_ref, freq_ref, step_ref, in_coef_ref, out_coef_ref, skip_ref,
    mid_gain_ref, gate_vec_ref, routes_ref, weights_ref,
    full, in_w, state, out_w, eg, eu, ed, sg, su, sd,
    own_resid, own_mixed, mixed, after, outgoing, slots_in, resid_in, mixed_in, after_in, piece, hidden, result, returned,
    shidden, partial, stage_a, stage_b, sum_a, sum_b, final_a, final_b, direct_in,
    routed_part, core_in, core_sum, routed_in,
    local_sem, so, ro, s1, r1, s2, r2, se, re, sl, rl, s3, r3, s5, r5, s6, r6, s6d, r6d, s6f, r6f, s7, r7,
):
    e = lax.axis_index("ep")
    t = lax.axis_index("tp")
    z, x = e // SIDE, e % SIDE
    y, core = t // 2, t % 2
    tp_peers = [
        (dy * 2 + dc, (e, ((y + dy) % SIDE) * 2 + (core + dc) % 2))
        for dy in (2, 1, 3, 0) for dc in (0, 1) if dy + dc
    ]
    to_peers = [(((z + dz) % SIDE) * SIDE + (x + dx) % SIDE, t) for dz, dx in OFFSETS]
    from_peers = [(((z + SIDE - dz) % SIDE) * SIDE + (x + SIDE - dx) % SIDE, t) for dz, dx in OFFSETS]
    x_peers = [(d, (z * SIDE + (x + d) % SIDE, t), (x + d) % SIDE) for d in (2, 1, 3)]
    z_peers = [(d, (((z + d) % SIDE) * SIDE + x, t), (z + d) % SIDE) for d in (2, 1, 3)]
    y_peers = [(d, (e, ((y + d) % SIDE) * 2 + core), (y + d) % SIDE) for d in (2, 1, 3)]
    partner = (e, y * 2 + (1 - core))

    barrier = pltpu.get_barrier_semaphore()
    near = [dev for _, dev in tp_peers] + [peer[1] for peer in x_peers + z_peers]
    for dev in near:
        pl.semaphore_signal(barrier, inc=1, device_id=dev, device_id_type=MESH)

    fetches = {}
    for i, (name, src, dst) in enumerate([
        ("resid", resid_hbm, resid_ref), ("decay", decay_hbm, decay_ref),
        ("freq", freq_hbm, freq_ref), ("step", step_hbm, step_ref),
        ("in_coef", in_coef_hbm, in_coef_ref), ("out_coef", out_coef_hbm, out_coef_ref),
        ("routes", routes_hbm, routes_ref), ("weights", weights_hbm, weights_ref),
        ("skip", skip_hbm, skip_ref), ("in_gain", in_gain_hbm, in_gain_ref),
        ("state", state_hbm, state), ("in_w", in_w_hbm, in_w),
        ("mid_gain", mid_gain_hbm, mid_gain_ref), ("gate_vec", gate_vec_hbm, gate_vec_ref),
        ("out_w", out_w_hbm, out_w),
        ("eg", eg_hbm, eg), ("eu", eu_hbm, eu), ("ed", ed_hbm, ed),
        ("sg", sg_hbm, sg), ("su", su_hbm, su), ("sd", sd_hbm, sd),
    ]):
        fetches[name] = pltpu.make_async_copy(src, dst, local_sem.at[i])
        fetches[name].start()

    def fetched(*names):
        for name in names:
            fetches[name].wait()

    def send(src, dst, ss, rs, d, dev):
        copy = pltpu.make_async_remote_copy(
            src_ref=src, dst_ref=dst, send_sem=ss, recv_sem=rs.at[d],
            device_id=dev, device_id_type=MESH,
        )
        copy.start()

    def all_of(ref, sem):
        pltpu.make_async_copy(ref, ref, sem).wait()

    own_rows = pl.ds(pl.multiple_of(t * OWN, OWN), OWN)

    pl.semaphore_wait(barrier, len(near))

    fetched("resid")
    cols = pl.ds(pl.multiple_of(t * FEAT, FEAT), FEAT)
    for _, dev in tp_peers:
        rows = pl.ds(pl.multiple_of(dev[1] * OWN, OWN), OWN)
        send(resid_ref.at[rows], own_resid.at[:, cols], so.at[0], ro, 0, dev)
    for d, _, there in y_peers:
        for c in (0, 1):
            @pl.when(core == c)
            def _():
                send(resid_ref, full.at[:, cols], s1, r1, 2 * d + c, (e, there * 2 + 1))
    send(resid_ref, full.at[:, cols], s1, r1, 0, partner)
    full[:, cols] = resid_ref[...]
    own_resid[:, cols] = resid_ref[own_rows, :]

    fetched("decay", "freq", "step", "in_coef", "out_coef")
    own_lane = (
        lax.broadcasted_iota(jnp.int32, (GROUPS, GROUPS), 0)
        == lax.broadcasted_iota(jnp.int32, (GROUPS, GROUPS), 1)
    )
    log_step = jnp.sum(jnp.where(own_lane, step_ref[...], 0.0), axis=1, keepdims=True)
    dt = jnp.exp(log_step)
    rate = -decay_ref[...]
    freq = freq_ref[...]
    magnitude = jnp.exp(rate * dt)
    keep_re = magnitude * jnp.cos(freq * dt)
    keep_im = magnitude * jnp.sin(freq * dt)
    denominator = rate * rate + freq * freq
    factor_re = ((keep_re - 1.0) * rate + keep_im * freq) / denominator
    factor_im = (keep_im * rate - (keep_re - 1.0) * freq) / denominator
    fr, fi = per_group_rows(factor_re), per_group_rows(factor_im)
    push_re = block_diagonal(fr * in_coef_ref[0] - fi * in_coef_ref[1])
    push_im = block_diagonal(fr * in_coef_ref[1] + fi * in_coef_ref[0])
    pr_hi, pr_lo = halves(push_re)
    pi_hi, pi_lo = halves(push_im)
    out_re = block_diagonal(out_coef_ref[0]).astype(bf16)
    out_im = block_diagonal(out_coef_ref[1]).astype(bf16)
    kr, ki = lanes_of_groups(keep_re), lanes_of_groups(keep_im)

    fetched("routes", "weights")
    slot_row = lax.broadcasted_iota(jnp.int32, (SLOTS, ROWS), 0)
    expert = (slot_row // CAP) * TP + t
    weight_sum = jnp.sum(weights_ref[...], axis=0, keepdims=True)
    weights = weights_ref[...] / weight_sum * routed_scale
    chosen = jnp.zeros((SLOTS, ROWS), f32)
    chosen_weight = jnp.zeros((SLOTS, ROWS), f32)
    for k in range(4):
        same = routes_ref[k : k + 1, :] == expert
        chosen = jnp.where(same, 1.0, chosen)
        chosen_weight = jnp.where(same, weights[k : k + 1, :], chosen_weight)
    earlier = (
        lax.broadcasted_iota(jnp.int32, (ROWS, ROWS), 0)
        < lax.broadcasted_iota(jnp.int32, (ROWS, ROWS), 1)
    )
    before = dot(chosen.astype(bf16), jnp.where(earlier, 1.0, 0.0).astype(bf16))
    rank = (slot_row % CAP).astype(f32)
    holds = (chosen > 0.5) & (before == rank)
    pick = jnp.where(holds, 1.0, 0.0).astype(bf16)
    combine = jnp.where(holds, chosen_weight, 0.0).T
    comb_hi, comb_lo = halves(combine)

    fetched("state", "in_w", "in_gain", "skip")
    old_re, old_im = state[0], state[1]
    kept_re = kr * old_re - ki * old_im
    kept_im = kr * old_im + ki * old_re
    new_state_ref[0] = kept_re
    new_state_ref[1] = kept_im
    read_kept = dot_nt(kept_re.astype(bf16), out_re) - dot_nt(kept_im.astype(bf16), out_im)
    read_push = (dot_nt(pr_hi, out_re) + dot_nt(pr_lo, out_re)) - (dot_nt(pi_hi, out_im) + dot_nt(pi_lo, out_im))
    rp_hi, rp_lo = halves(read_push)
    def first_step(src, dst, width, ss, rs):
        left, right = pl.ds(0, width), pl.ds(width, width)
        for k, (a, b) in enumerate(((left, right), (right, left))):
            for (d, dev_x, _), (_, dev_z, _) in zip(x_peers, z_peers, strict=True):
                send(src.at[:, a], dst.at[e, :, a], ss, rs, d if k == 0 else 0, dev_x)
                send(src.at[:, b], dst.at[e, :, b], ss, rs, 4 + d if k == 0 else 0, dev_z)

    def second_step(dst, width, ss, rs):
        left, right = pl.ds(0, width), pl.ds(width, width)
        for d in (1, 3, 2):
            block = dst.at[z * SIDE + (x + SIDE - d) % SIDE, :, left]
            all_of(block, rs.at[d])
            for _, dev, _ in z_peers:
                send(block, block, ss, rs, 0, dev)
            block = dst.at[((z + SIDE - d) % SIDE) * SIDE + x, :, right]
            all_of(block, rs.at[4 + d])
            for _, dev, _ in x_peers:
                send(block, block, ss, rs, 0, dev)

    all_of(own_resid.at[:, pl.ds(0, 7 * FEAT)], ro.at[0])
    first_step(own_resid, resid_in, HALF, se, re)
    resid_in[e] = own_resid[...]
    @pl.when(core == 1)
    def _():
        for d in (1, 3, 2):
            for c in (1, 0):
                at = (((y + SIDE - d) % SIDE) * 2 + c) * FEAT
                theirs = full.at[:, pl.ds(pl.multiple_of(at, FEAT), FEAT)]
                all_of(theirs, r1.at[2 * d + c])
                send(theirs, theirs, s1, r1, 0, partner)
        all_of(full.at[:, pl.ds(0, FEAT)], r1.at[0])
        all_of(full.at[:, pl.ds(0, 6 * FEAT)], s1)

    @pl.when(core == 0)
    def _():
        all_of(full.at[:, pl.ds(0, 7 * FEAT)], r1.at[0])

    values = full[...].astype(f32)
    mean = jnp.sum(values, axis=1, keepdims=True) * (1.0 / WIDTH)
    square = jnp.sum(values * values, axis=1, keepdims=True) * (1.0 / WIDTH)
    scale = lax.rsqrt(square - mean * mean + norm_eps)
    normed = ((values - mean) * scale * in_gain_ref[...]).astype(bf16)
    drive = dot(normed, in_w[...]).astype(bf16)
    read = read_kept + (dot(drive, rp_hi) + dot(drive, rp_lo)) + skip_ref[...] * drive.astype(f32)
    mixed_cols = pl.ds(pl.multiple_of(t * CH, CH), CH)
    mixed_part = jax.nn.gelu(read, approximate=True).astype(bf16)
    mixed[:, mixed_cols] = mixed_part

    for _, dev in tp_peers:
        rows = pl.ds(pl.multiple_of(dev[1] * OWN, OWN), OWN)
        send(mixed.at[rows, mixed_cols], own_mixed.at[:, mixed_cols], so.at[1], ro, 1, dev)
    own_mixed[:, mixed_cols] = mixed[own_rows, mixed_cols]
    for d, _, there in y_peers:
        send(mixed.at[:, mixed_cols], mixed.at[:, mixed_cols], s2, r2, d, (e, there * 2 + 1))
    send(mixed.at[:, mixed_cols], mixed.at[:, mixed_cols], s2, r2, 0, partner)
    new_state_ref[0] = new_state_ref[0] + (dot(drive, pr_hi) + dot(drive, pr_lo))
    new_state_ref[1] = new_state_ref[1] + (dot(drive, pi_hi) + dot(drive, pi_lo))
    second_step(resid_in, HALF, se, re)
    fetched("out_w", "mid_gain")
    sums = [jnp.zeros((ROWS, 128), f32), jnp.zeros((ROWS, 128), f32)]
    for dy in (0, 1, 3, 2):
        deep = pl.ds(pl.multiple_of(((y + SIDE - dy) % SIDE) * 256, 256), 256)
        if dy:
            all_of(mixed.at[:, deep], r2.at[dy])

            @pl.when(core == 1)
            def _():
                send(mixed.at[:, deep], mixed.at[:, deep], s2, r2, dy, partner)
        else:
            other = pl.ds(pl.multiple_of((y * 2 + (1 - core)) * CH, CH), CH)
            all_of(mixed.at[:, other], r2.at[0])
        block = mixed[:, deep]
        for j in range(WIDTH // 256):
            at = pl.ds(j * 256, 256)
            base = full[:, at].astype(f32) if dy == 0 else after[:, at]
            part = base + dot(block, out_w[deep, at])
            after[:, at] = part
            if dy == 2:
                for lanes in (part[:, :128], part[:, 128:]):
                    sums[0] = sums[0] + lanes
                    sums[1] = sums[1] + lanes * lanes
        if dy == OWN_AFTER:
            all_of(own_mixed.at[:, pl.ds(0, 7 * CH)], ro.at[1])
            first_step(own_mixed, mixed_in, MIX // 2, sl, rl)
            mixed_in[e] = own_mixed[...]
    mean = jnp.sum(sums[0], axis=1, keepdims=True) * (1.0 / WIDTH)
    square = jnp.sum(sums[1], axis=1, keepdims=True) * (1.0 / WIDTH)
    scale = lax.rsqrt(square - mean * mean + norm_eps)
    for j in range(WIDTH // 256):
        at = pl.ds(j * 256, 256)
        part = ((after[:, at] - mean) * scale * mid_gain_ref[:, at]).astype(bf16)
        outgoing[:, :, at] = dot(pick, part).astype(bf16).reshape(EP, CAP, 256)

    def send_slots(group):
        for i in range(GROUP * group, min(GROUP * (group + 1), EP - 1)):
            send(outgoing.at[to_peers[i][0]], slots_in.at[i], s3.at[group], r3, group, to_peers[i])

    send_slots(0)
    slots_in[EP - 1] = outgoing[e]
    own_after = after[own_rows, :]
    mean = jnp.sum(own_after, axis=1, keepdims=True) * (1.0 / WIDTH)
    square = jnp.sum(own_after * own_after, axis=1, keepdims=True) * (1.0 / WIDTH)
    own_mid = ((own_after - mean) * lax.rsqrt(square - mean * mean + norm_eps) * mid_gain_ref[...]).astype(bf16)
    fetched("gate_vec")
    gate_vec = jnp.concatenate([gate_vec_ref[i : i + 1, :] for i in range(WIDTH // 128)], axis=1)
    gate_value = jax.nn.sigmoid(
        jnp.sum(own_mid.astype(f32) * gate_vec.astype(f32), axis=1, keepdims=True)
    )
    all_of(slots_in.at[pl.ds(0, GROUP)], s3.at[0])
    send_slots(1)
    second_step(mixed_in, MIX // 2, sl, rl)

    fetched("eg", "eu", "ed")
    halves_of_rows = (pl.ds(0, HALF), pl.ds(HALF, HALF))

    def send_results(first, last, at, k):
        for i in range(first, last):
            send(result.at[i, :, at], returned.at[e, :, at], s5.at[k], r5, k, from_peers[i])

    for group in (0, 1):
        number = min(GROUP, EP - 1 - GROUP * group)
        all_of(slots_in.at[pl.ds(GROUP * group, number)], r3.at[group])
        blocks, rows_at = pl.ds(GROUP * group, GROUP), pl.ds(GROUP * CAP * group, GROUP * CAP)
        rows = slots_in[blocks].reshape(GROUP * CAP, WIDTH)
        for j in range(FF // 256):
            at = pl.ds(j * 256, 256)
            gate_part = dot(rows, eg[:, at])
            up_part = dot(rows, eu[:, at])
            hidden[rows_at, at] = (jax.nn.silu(gate_part) * up_part).astype(bf16)
        for j in range(WIDTH // 256):
            at = pl.ds(j * 256, 256)
            result[blocks, :, at] = dot(hidden[rows_at, :], ed[:, at]).astype(bf16).reshape(GROUP, CAP, 256)
            if group == 1 and j == HALF // 256 - 1:
                send_results(GROUP, EP - 1, halves_of_rows[0], 1)
        if group == 0:
            send_results(0, GROUP, pl.ds(0, WIDTH), 0)

    returned[e] = result[EP - 1]

    fetched("sg", "su", "sd")
    all_of(resid_in.at[pl.ds(0, 12)], re.at[0])
    all_of(mixed_in.at[pl.ds(0, 12)], rl.at[0])
    channels = mixed_in[...].reshape(EP * OWN, MIX)
    sums = [jnp.zeros((EP * OWN, 128), f32), jnp.zeros((EP * OWN, 128), f32)]
    for j in range(WIDTH // 256):
        at = pl.ds(j * 256, 256)
        part = resid_in[:, :, at].reshape(EP * OWN, 256).astype(f32) + dot(channels, out_w[:, at])
        after_in[:, at] = part
        for lanes in (part[:, :128], part[:, 128:]):
            sums[0] = sums[0] + lanes
            sums[1] = sums[1] + lanes * lanes
    mean = jnp.sum(sums[0], axis=1, keepdims=True) * (1.0 / WIDTH)
    square = jnp.sum(sums[1], axis=1, keepdims=True) * (1.0 / WIDTH)
    scale = lax.rsqrt(square - mean * mean + norm_eps)
    for j in range(WIDTH // 256):
        at = pl.ds(j * 256, 256)
        piece[:, at] = ((after_in[:, at] - mean) * scale * mid_gain_ref[:, at]).astype(bf16)
    send_results(GROUP, EP - 1, halves_of_rows[1], 2)
    gate_part = dot(piece[...], sg[...])
    up_part = dot(piece[...], su[...])
    shidden[...] = (jax.nn.silu(gate_part) * up_part).astype(bf16)

    grid = (SIDE, SIDE, OWN)
    direct_cols = pl.ds(2 * PART, WIDTH - 2 * PART)
    parts = ((0, EARLY_COLS), (EARLY_COLS, PART - EARLY_COLS))

    def partial_columns(first, last):
        for begin in range(first, last, 256):
            at = pl.ds(begin, min(256, last - begin))
            partial[:, :, :, at] = dot(shidden[...], sd[:, at]).astype(bf16).reshape(*grid, at.size)

    def first_sums(part):
        begin, size = parts[part]
        at = pl.ds(begin, size)
        left, right = at, pl.ds(PART + begin, size)
        for d, dev, there in z_peers:
            send(partial.at[there, :, :, left], stage_a.at[d - 1, :, :, at], s6.at[2 * part], r6, 2 * part, dev)
        for d, dev, there in x_peers:
            send(partial.at[:, there, :, right], stage_b.at[d - 1, :, :, at], s6.at[2 * part + 1], r6, 2 * part + 1, dev)

    def second_sums(part):
        begin, size = parts[part]
        at = pl.ds(begin, size)
        left, right = at, pl.ds(PART + begin, size)
        all_of(stage_a.at[:, :, :, at], r6.at[2 * part])
        total = partial[z, :, :, left].astype(f32)
        for d in range(3):
            total = total + stage_a[d, :, :, at].astype(f32)
        sum_a[:, :, at] = total.astype(bf16)
        for d, dev, there in x_peers:
            send(sum_a.at[there, :, at], final_a.at[d - 1, :, at], s6f.at[2 * part], r6f, 2 * part, dev)
        all_of(stage_b.at[:, :, :, at], r6.at[2 * part + 1])
        total = partial[:, x, :, right].astype(f32)
        for d in range(3):
            total = total + stage_b[d, :, :, at].astype(f32)
        sum_b[:, :, at] = total.astype(bf16)
        for d, dev, there in z_peers:
            send(sum_b.at[there, :, at], final_b.at[d - 1, :, at], s6f.at[2 * part + 1], r6f, 2 * part + 1, dev)

    for part, (begin, size) in enumerate(parts):
        partial_columns(begin, begin + size)
        partial_columns(PART + begin, PART + begin + size)
        first_sums(part)
    partial_columns(2 * PART, WIDTH)

    def combine_half(half):
        at = halves_of_rows[half]
        if half == 0:
            all_of(returned.at[pl.ds(0, GROUP)], r5.at[0])
        all_of(returned.at[pl.ds(0, EP - 1 - GROUP), :, at], r5.at[1 + half])
        for begin in range(0, HALF, 256):
            part_at = pl.ds(half * HALF + begin, 256)
            back = returned[:, :, part_at].reshape(SLOTS, 256)
            part = dot(comb_hi, back) + dot(comb_lo, back)
            routed_part[:, :, :, part_at] = part.astype(bf16).reshape(SIDE, 2, OWN, 256)
        send(routed_part.at[:, 1 - core, :, at], core_in.at[:, :, at], s7.at[half], r7, half, partner)

    def sum_over_tp(half):
        at = halves_of_rows[half]
        all_of(core_in.at[:, :, at], r7.at[half])
        core_sum[:, :, at] = (
            routed_part[:, core, :, at].astype(f32) + core_in[:, :, at].astype(f32)
        ).astype(bf16)
        for d, dev, there in y_peers:
            send(core_sum.at[there, :, at], routed_in.at[d - 1, :, at], s7.at[2 + half], r7, 2 + half, dev)

    def send_direct():
        for i, (dz, dx) in enumerate(OFFSETS):
            to_z, to_x = (z + dz) % SIDE, (x + dx) % SIDE
            send(
                partial.at[to_z, to_x, :, direct_cols], direct_in.at[i], s6d, r6d, 0,
                (to_z * SIDE + to_x, t),
            )

    combine_half(0)

    @pl.when(core == 0)
    def _():
        sum_over_tp(0)

    combine_half(1)

    @pl.when(core == 1)
    def _():
        second_sums(0)
        send_direct()
        sum_over_tp(0)

    sum_over_tp(1)

    @pl.when(core == 0)
    def _():
        send_direct()
        second_sums(0)

    second_sums(1)
    for half, at in enumerate(halves_of_rows):
        all_of(routed_in.at[:, :, at], r7.at[2 + half])
    routed = core_sum[y].astype(f32) + jnp.sum(routed_in[...].astype(f32), axis=0) + after[own_rows, :]
    for part, (begin, size) in enumerate(parts):
        all_of(final_a.at[:, :, pl.ds(begin, size)], r6f.at[2 * part])
        all_of(final_b.at[:, :, pl.ds(begin, size)], r6f.at[2 * part + 1])
    all_of(direct_in, r6d.at[0])
    own_direct = partial[z, x, :, direct_cols]
    for at, own, others in (
        (pl.ds(0, PART), sum_a[x], final_a), (pl.ds(PART, PART), sum_b[z], final_b),
        (direct_cols, own_direct, direct_in),
    ):
        shared = own.astype(f32) + jnp.sum(others[...].astype(f32), axis=0)
        begin, size = at.start, at.size
        out_ref[:, at] = (routed[:, begin : begin + size] + gate_value * shared).astype(bf16)

    all_of(own_resid.at[:, pl.ds(0, 7 * FEAT)], so.at[0])
    all_of(own_mixed.at[:, pl.ds(0, 7 * CH)], so.at[1])
    all_of(full.at[:, pl.ds(0, 4 * FEAT)], s1)
    all_of(mixed.at[:, pl.ds(0, 4 * CH)], s2)

    @pl.when(core == 1)
    def _():
        all_of(mixed.at[:, pl.ds(0, 6 * CH)], s2)

    all_of(resid_in.at[pl.ds(0, 15)], se)
    all_of(mixed_in.at[pl.ds(0, 15)], sl)
    all_of(slots_in.at[pl.ds(0, EP - 1 - GROUP)], s3.at[1])
    all_of(returned.at[pl.ds(0, GROUP)], s5.at[0])
    for part, (begin, size) in enumerate(parts):
        at = pl.ds(begin, size)
        all_of(stage_a.at[:, :, :, at], s6.at[2 * part])
        all_of(stage_b.at[:, :, :, at], s6.at[2 * part + 1])
        all_of(final_a.at[:, :, at], s6f.at[2 * part])
        all_of(final_b.at[:, :, at], s6f.at[2 * part + 1])
    for half, at in enumerate(halves_of_rows):
        all_of(returned.at[pl.ds(0, EP - 1 - GROUP), :, at], s5.at[1 + half])
        all_of(core_in.at[:, :, at], s7.at[half])
        all_of(routed_in.at[:, :, at], s7.at[2 + half])
    all_of(direct_in, s6d)


def write_out(out_ref, state_ref, out_hbm, state_hbm, sem):
    copies = [
        pltpu.make_async_copy(state_ref, state_hbm, sem.at[0]),
        pltpu.make_async_copy(out_ref, out_hbm, sem.at[1]),
    ]
    for c in copies:
        c.start()
    for c in copies:
        c.wait()


def per_device(
    residual, in_gain, in_weight, state, decay_rate, frequency, log_step, in_coef, out_coef,
    skip_gain, out_weight, mid_gain, gate_vector, routes, route_weight, expert_gate, expert_up,
    expert_down, shared_gate, shared_up, shared_down,
):
    vmem = pl.BlockSpec(memory_space=pltpu.VMEM)
    hbm = pl.BlockSpec(memory_space=pltpu.HBM)
    dma = pltpu.SemaphoreType.DMA
    in_coef_rows = jnp.swapaxes(in_coef, 2, 3).reshape(2, CH, STATE)
    out_coef_rows = out_coef.reshape(2, CH, STATE)
    call = pl.pallas_call(
        kernel,
        name="layer_step",
        out_shape=(
            pltpu.VMEM((OWN, WIDTH), bf16),
            pltpu.VMEM((2, ROWS, GS), f32),
        ),
        in_specs=[hbm] * 21,
        out_specs=(vmem, vmem),
        scratch_shapes=[
            pltpu.VMEM((ROWS, FEAT), bf16),
            pltpu.VMEM((1, WIDTH), f32),
            pltpu.VMEM((GROUPS, STATE), f32),
            pltpu.VMEM((GROUPS, STATE), f32),
            pltpu.VMEM((1, GROUPS), f32),
            pltpu.VMEM((2, CH, STATE), f32),
            pltpu.VMEM((2, CH, STATE), f32),
            pltpu.VMEM((1, CH), f32),
            pltpu.VMEM((1, WIDTH), f32),
            pltpu.VMEM((WIDTH // 128, 128), bf16),
            pltpu.VMEM((4, ROWS), jnp.int32),
            pltpu.VMEM((4, ROWS), f32),
            pltpu.VMEM((ROWS, WIDTH), bf16),
            pltpu.VMEM((WIDTH, CH), bf16),
            pltpu.VMEM((2, ROWS, GS), f32),
            pltpu.VMEM((MIX, WIDTH), bf16),
            pltpu.VMEM((WIDTH, FF), bf16),
            pltpu.VMEM((WIDTH, FF), bf16),
            pltpu.VMEM((FF, WIDTH), bf16),
            pltpu.VMEM((WIDTH, SF), bf16),
            pltpu.VMEM((WIDTH, SF), bf16),
            pltpu.VMEM((SF, WIDTH), bf16),
            pltpu.VMEM((OWN, WIDTH), bf16),
            pltpu.VMEM((OWN, MIX), bf16),
            pltpu.VMEM((ROWS, MIX), bf16),
            pltpu.VMEM((ROWS, WIDTH), f32),
            pltpu.VMEM((EP, CAP, WIDTH), bf16),
            pltpu.VMEM((EP, CAP, WIDTH), bf16),
            pltpu.VMEM((EP, OWN, WIDTH), bf16),
            pltpu.VMEM((EP, OWN, MIX), bf16),
            pltpu.VMEM((EP * OWN, WIDTH), f32),
            pltpu.VMEM((EP * OWN, WIDTH), bf16),
            pltpu.VMEM((SLOTS, FF), bf16),
            pltpu.VMEM((EP, CAP, WIDTH), bf16),
            pltpu.VMEM((EP, CAP, WIDTH), bf16),
            pltpu.VMEM((EP * OWN, SF), bf16),
            pltpu.VMEM((SIDE, SIDE, OWN, WIDTH), bf16),
            pltpu.VMEM((SIDE - 1, SIDE, OWN, PART), bf16),
            pltpu.VMEM((SIDE - 1, SIDE, OWN, PART), bf16),
            pltpu.VMEM((SIDE, OWN, PART), bf16),
            pltpu.VMEM((SIDE, OWN, PART), bf16),
            pltpu.VMEM((SIDE - 1, OWN, PART), bf16),
            pltpu.VMEM((SIDE - 1, OWN, PART), bf16),
            pltpu.VMEM((EP - 1, OWN, WIDTH - 2 * PART), bf16),
            pltpu.VMEM((SIDE, 2, OWN, WIDTH), bf16),
            pltpu.VMEM((SIDE, OWN, WIDTH), bf16),
            pltpu.VMEM((SIDE, OWN, WIDTH), bf16),
            pltpu.VMEM((SIDE - 1, OWN, WIDTH), bf16),
            dma((21,)),
            dma((2,)), dma((2,)),
            dma, dma((8,)),
            dma, dma((4,)),
            dma, dma((8,)),
            dma, dma((8,)),
            dma((2,)), dma((2,)),
            dma((3,)), dma((3,)),
            dma((4,)), dma((4,)),
            dma, dma((1,)),
            dma((4,)), dma((4,)),
            dma((4,)), dma((4,)),
        ],
        compiler_params=pltpu.CompilerParams(
            collective_id=0, has_side_effects=True, vmem_limit_bytes=VMEM_MIB * 1024 * 1024
        ),
    )
    operands = (
        residual, in_gain.reshape(1, WIDTH), in_weight, state, decay_rate, frequency,
        log_step.reshape(1, GROUPS), in_coef_rows, out_coef_rows, skip_gain.reshape(1, CH),
        out_weight, mid_gain.reshape(1, WIDTH), gate_vector.reshape(WIDTH // 128, 128), routes.T,
        route_weight.T, expert_gate[0], expert_up[0], expert_down[0], shared_gate, shared_up,
        shared_down,
    )
    results = call(*[pltpu.with_memory_space_constraint(a, pltpu.HBM) for a in operands])
    return pl.pallas_call(
        write_out,
        name="write_out",
        out_shape=(
            jax.ShapeDtypeStruct((OWN, WIDTH), bf16),
            jax.ShapeDtypeStruct((2, ROWS, GS), f32),
        ),
        in_specs=[vmem, vmem],
        out_specs=(hbm, hbm),
        scratch_shapes=[dma((2,))],
    )(*[pltpu.with_memory_space_constraint(a, pltpu.VMEM) for a in results])


def solution(mesh):
    return jax.shard_map(
        per_device,
        mesh=mesh,
        in_specs=(
            P("ep", "tp"), P(), P(None, "tp"), P(None, "ep", "tp"), P("tp", None), P("tp", None),
            P("tp"), P(None, "tp", None, None), P(None, "tp", None, None), P("tp"), P(), P(), P(),
            P("ep", None), P("ep", None), P(("ep", "tp"), None, None), P(("ep", "tp"), None, None),
            P(("ep", "tp"), None, None), P(None, "ep"), P(None, "ep"), P("ep", None),
        ),
        out_specs=(P(("ep", "tp"), None), P(None, "ep", "tp")),
        check_vma=False,
    )
```

```python
import jax
import jax.numpy as jnp
from jax import lax
from jax.experimental import pallas as pl
from jax.experimental.pallas import tpu as pltpu
from jax.sharding import PartitionSpec as P

MESH = pl.DeviceIdType.MESH
norm_eps = 1e-05
routed_scale = 2.5
f32, bf16 = jnp.float32, jnp.bfloat16

TP, EP = 8, 16
ROWS, WIDTH, FEAT = 128, 2048, 256
CH, GROUPS, STATE, GCH = 128, 8, 64, 16
GS = GROUPS * STATE
CAP, OWN = 8, 16
SIDE = 4
HALF = WIDTH // 2
SLOTS = EP * CAP
FF, SF = 512, 256
MIX = CH * TP
OFFSETS = (
    [(2, 1), (2, 3), (1, 2), (3, 2), (0, 1), (0, 3), (1, 0), (3, 0)]
    + [(2, 2), (1, 1), (1, 3), (3, 1), (3, 3), (0, 2), (2, 0)]
)
GROUP = EP // 2
VMEM_MIB = 48
PART = 896
OWN_AFTER = 3
EARLY_COLS = 640


def dot(a, b):
    return jnp.dot(a, b, preferred_element_type=f32)


def dot_nt(a, b):
    return lax.dot_general(a, b, (((1,), (1,)), ((), ())), preferred_element_type=f32)


def dot_tn(a, b):
    return lax.dot_general(a, b, (((0,), (0,)), ((), ())), preferred_element_type=f32)


def halves(a):
    high = a.astype(bf16)
    return high, (a - high.astype(f32)).astype(bf16)


def lanes_of_groups(a):
    return jnp.concatenate([a[g : g + 1, :] for g in range(GROUPS)], axis=1)


def block_diagonal(a):
    wide = jnp.concatenate([a] * GROUPS, axis=1)
    row = lax.broadcasted_iota(jnp.int32, (CH, GS), 0) // GCH
    col = lax.broadcasted_iota(jnp.int32, (CH, GS), 1) // STATE
    return jnp.where(row == col, wide, 0.0)


def per_group_rows(a):
    return jnp.broadcast_to(a[:, None, :], (GROUPS, GCH, STATE)).reshape(CH, STATE)


def kernel(
    resid_hbm, in_gain_hbm, in_w_hbm, state_hbm, decay_hbm, freq_hbm, step_hbm, in_coef_hbm,
    out_coef_hbm, skip_hbm, out_w_hbm, mid_gain_hbm, gate_vec_hbm, routes_hbm, weights_hbm,
    eg_hbm, eu_hbm, ed_hbm, sg_hbm, su_hbm, sd_hbm,
    out_ref, new_state_ref,
    resid_ref, in_gain_ref, decay_ref, freq_ref, step_ref, in_coef_ref, out_coef_ref, skip_ref,
    mid_gain_ref, gate_vec_ref, routes_ref, weights_ref,
    full, in_w, state, out_w, eg, eu, ed, sg, su, sd,
    own_resid, own_mixed, mixed, after, outgoing, slots_in, resid_in, mixed_in, after_in, piece, hidden, result, returned,
    shidden, partial, stage_a, stage_b, sum_a, sum_b, final_a, final_b, direct_in,
    routed_part, core_in, core_sum, routed_in,
    local_sem, so, ro, s1, r1, s2, r2, se, re, sl, rl, s3, r3, s5, r5, s6, r6, s6d, r6d, s6f, r6f, s7, r7,
):
    e = lax.axis_index("ep")
    t = lax.axis_index("tp")
    z, x = e // SIDE, e % SIDE
    y, core = t // 2, t % 2
    tp_peers = [
        (dy * 2 + dc, (e, ((y + dy) % SIDE) * 2 + (core + dc) % 2))
        for dy in (2, 1, 3, 0) for dc in (0, 1) if dy + dc
    ]
    to_peers = [(((z + dz) % SIDE) * SIDE + (x + dx) % SIDE, t) for dz, dx in OFFSETS]
    from_peers = [(((z + SIDE - dz) % SIDE) * SIDE + (x + SIDE - dx) % SIDE, t) for dz, dx in OFFSETS]
    x_peers = [(d, (z * SIDE + (x + d) % SIDE, t), (x + d) % SIDE) for d in (2, 1, 3)]
    z_peers = [(d, (((z + d) % SIDE) * SIDE + x, t), (z + d) % SIDE) for d in (2, 1, 3)]
    y_peers = [(d, (e, ((y + d) % SIDE) * 2 + core), (y + d) % SIDE) for d in (2, 1, 3)]
    partner = (e, y * 2 + (1 - core))

    barrier = pltpu.get_barrier_semaphore()
    near = [dev for _, dev in tp_peers] + [peer[1] for peer in x_peers + z_peers]
    for dev in near:
        pl.semaphore_signal(barrier, inc=1, device_id=dev, device_id_type=MESH)

    fetches = {}
    for i, (name, src, dst) in enumerate([
        ("resid", resid_hbm, resid_ref), ("decay", decay_hbm, decay_ref),
        ("freq", freq_hbm, freq_ref), ("step", step_hbm, step_ref),
        ("in_coef", in_coef_hbm, in_coef_ref), ("out_coef", out_coef_hbm, out_coef_ref),
        ("routes", routes_hbm, routes_ref), ("weights", weights_hbm, weights_ref),
        ("skip", skip_hbm, skip_ref), ("in_gain", in_gain_hbm, in_gain_ref),
        ("state", state_hbm, state), ("in_w", in_w_hbm, in_w),
        ("mid_gain", mid_gain_hbm, mid_gain_ref), ("gate_vec", gate_vec_hbm, gate_vec_ref),
        ("out_w", out_w_hbm, out_w),
        ("eg", eg_hbm, eg), ("eu", eu_hbm, eu), ("ed", ed_hbm, ed),
        ("sg", sg_hbm, sg), ("su", su_hbm, su), ("sd", sd_hbm, sd),
    ]):
        fetches[name] = pltpu.make_async_copy(src, dst, local_sem.at[i])
        fetches[name].start()

    def fetched(*names):
        for name in names:
            fetches[name].wait()

    def send(src, dst, ss, rs, d, dev):
        copy = pltpu.make_async_remote_copy(
            src_ref=src, dst_ref=dst, send_sem=ss, recv_sem=rs.at[d],
            device_id=dev, device_id_type=MESH,
        )
        copy.start()

    def all_of(ref, sem):
        pltpu.make_async_copy(ref, ref, sem).wait()

    own_rows = pl.ds(pl.multiple_of(t * OWN, OWN), OWN)

    pl.semaphore_wait(barrier, len(near))

    fetched("resid")
    cols = pl.ds(pl.multiple_of(t * FEAT, FEAT), FEAT)
    for _, dev in tp_peers:
        rows = pl.ds(pl.multiple_of(dev[1] * OWN, OWN), OWN)
        send(resid_ref.at[rows], own_resid.at[:, cols], so.at[0], ro, 0, dev)
    for d, _, there in y_peers:
        for c in (0, 1):
            @pl.when(core == c)
            def _():
                send(resid_ref, full.at[:, cols], s1, r1, 2 * d + c, (e, there * 2 + 1))
    send(resid_ref, full.at[:, cols], s1, r1, 0, partner)
    full[:, cols] = resid_ref[...]
    own_resid[:, cols] = resid_ref[own_rows, :]

    fetched("decay", "freq", "step", "in_coef", "out_coef")
    own_lane = (
        lax.broadcasted_iota(jnp.int32, (GROUPS, GROUPS), 0)
        == lax.broadcasted_iota(jnp.int32, (GROUPS, GROUPS), 1)
    )
    log_step = jnp.sum(jnp.where(own_lane, step_ref[...], 0.0), axis=1, keepdims=True)
    dt = jnp.exp(log_step)
    rate = -decay_ref[...]
    freq = freq_ref[...]
    magnitude = jnp.exp(rate * dt)
    keep_re = magnitude * jnp.cos(freq * dt)
    keep_im = magnitude * jnp.sin(freq * dt)
    denominator = rate * rate + freq * freq
    factor_re = ((keep_re - 1.0) * rate + keep_im * freq) / denominator
    factor_im = (keep_im * rate - (keep_re - 1.0) * freq) / denominator
    fr, fi = per_group_rows(factor_re), per_group_rows(factor_im)
    push_re = block_diagonal(fr * in_coef_ref[0] - fi * in_coef_ref[1])
    push_im = block_diagonal(fr * in_coef_ref[1] + fi * in_coef_ref[0])
    pr_hi, pr_lo = halves(push_re)
    pi_hi, pi_lo = halves(push_im)
    out_re = block_diagonal(out_coef_ref[0]).astype(bf16)
    out_im = block_diagonal(out_coef_ref[1]).astype(bf16)
    kr, ki = lanes_of_groups(keep_re), lanes_of_groups(keep_im)

    fetched("routes", "weights")
    slot_row = lax.broadcasted_iota(jnp.int32, (SLOTS, ROWS), 0)
    expert = (slot_row // CAP) * TP + t
    weight_sum = jnp.sum(weights_ref[...], axis=0, keepdims=True)
    weights = weights_ref[...] / weight_sum * routed_scale
    chosen = jnp.zeros((SLOTS, ROWS), f32)
    chosen_weight = jnp.zeros((SLOTS, ROWS), f32)
    for k in range(4):
        same = routes_ref[k : k + 1, :] == expert
        chosen = jnp.where(same, 1.0, chosen)
        chosen_weight = jnp.where(same, weights[k : k + 1, :], chosen_weight)
    earlier = (
        lax.broadcasted_iota(jnp.int32, (ROWS, ROWS), 0)
        < lax.broadcasted_iota(jnp.int32, (ROWS, ROWS), 1)
    )
    before = dot(chosen.astype(bf16), jnp.where(earlier, 1.0, 0.0).astype(bf16))
    rank = (slot_row % CAP).astype(f32)
    holds = (chosen > 0.5) & (before == rank)
    pick = jnp.where(holds, 1.0, 0.0).astype(bf16)
    combine = jnp.where(holds, chosen_weight, 0.0).T
    comb_hi, comb_lo = halves(combine)

    fetched("state", "in_w", "in_gain", "skip")
    old_re, old_im = state[0], state[1]
    kept_re = kr * old_re - ki * old_im
    kept_im = kr * old_im + ki * old_re
    new_state_ref[0] = kept_re
    new_state_ref[1] = kept_im
    read_kept = dot_nt(kept_re.astype(bf16), out_re) - dot_nt(kept_im.astype(bf16), out_im)
    read_push = (dot_nt(pr_hi, out_re) + dot_nt(pr_lo, out_re)) - (dot_nt(pi_hi, out_im) + dot_nt(pi_lo, out_im))
    rp_hi, rp_lo = halves(read_push)
    def first_step(src, dst, width, ss, rs):
        left, right = pl.ds(0, width), pl.ds(width, width)
        for k, (a, b) in enumerate(((left, right), (right, left))):
            for (d, dev_x, _), (_, dev_z, _) in zip(x_peers, z_peers, strict=True):
                send(src.at[:, a], dst.at[e, :, a], ss, rs, d if k == 0 else 0, dev_x)
                send(src.at[:, b], dst.at[e, :, b], ss, rs, 4 + d if k == 0 else 0, dev_z)

    def second_step(dst, width, ss, rs):
        left, right = pl.ds(0, width), pl.ds(width, width)
        for d in (1, 3, 2):
            block = dst.at[z * SIDE + (x + SIDE - d) % SIDE, :, left]
            all_of(block, rs.at[d])
            for _, dev, _ in z_peers:
                send(block, block, ss, rs, 0, dev)
            block = dst.at[((z + SIDE - d) % SIDE) * SIDE + x, :, right]
            all_of(block, rs.at[4 + d])
            for _, dev, _ in x_peers:
                send(block, block, ss, rs, 0, dev)

    all_of(own_resid.at[:, pl.ds(0, 7 * FEAT)], ro.at[0])
    first_step(own_resid, resid_in, HALF, se, re)
    resid_in[e] = own_resid[...]
    @pl.when(core == 1)
    def _():
        for d in (1, 3, 2):
            for c in (1, 0):
                at = (((y + SIDE - d) % SIDE) * 2 + c) * FEAT
                theirs = full.at[:, pl.ds(pl.multiple_of(at, FEAT), FEAT)]
                all_of(theirs, r1.at[2 * d + c])
                send(theirs, theirs, s1, r1, 0, partner)
        all_of(full.at[:, pl.ds(0, FEAT)], r1.at[0])
        all_of(full.at[:, pl.ds(0, 6 * FEAT)], s1)

    @pl.when(core == 0)
    def _():
        all_of(full.at[:, pl.ds(0, 7 * FEAT)], r1.at[0])

    values = full[...].astype(f32)
    mean = jnp.sum(values, axis=1, keepdims=True) * (1.0 / WIDTH)
    square = jnp.sum(values * values, axis=1, keepdims=True) * (1.0 / WIDTH)
    scale = lax.rsqrt(square - mean * mean + norm_eps)
    normed = ((values - mean) * scale * in_gain_ref[...]).astype(bf16)
    drive = dot(normed, in_w[...]).astype(bf16)
    read = read_kept + (dot(drive, rp_hi) + dot(drive, rp_lo)) + skip_ref[...] * drive.astype(f32)
    mixed_cols = pl.ds(pl.multiple_of(t * CH, CH), CH)
    mixed_part = jax.nn.gelu(read, approximate=True).astype(bf16)
    mixed[:, mixed_cols] = mixed_part

    for _, dev in tp_peers:
        rows = pl.ds(pl.multiple_of(dev[1] * OWN, OWN), OWN)
        send(mixed.at[rows, mixed_cols], own_mixed.at[:, mixed_cols], so.at[1], ro, 1, dev)
    own_mixed[:, mixed_cols] = mixed[own_rows, mixed_cols]
    for d, _, there in y_peers:
        send(mixed.at[:, mixed_cols], mixed.at[:, mixed_cols], s2, r2, d, (e, there * 2 + 1))
    send(mixed.at[:, mixed_cols], mixed.at[:, mixed_cols], s2, r2, 0, partner)
    new_state_ref[0] = new_state_ref[0] + (dot(drive, pr_hi) + dot(drive, pr_lo))
    new_state_ref[1] = new_state_ref[1] + (dot(drive, pi_hi) + dot(drive, pi_lo))
    second_step(resid_in, HALF, se, re)
    fetched("out_w", "mid_gain")
    sums = [jnp.zeros((ROWS, 128), f32), jnp.zeros((ROWS, 128), f32)]
    for dy in (0, 1, 3, 2):
        deep = pl.ds(pl.multiple_of(((y + SIDE - dy) % SIDE) * 256, 256), 256)
        if dy:
            all_of(mixed.at[:, deep], r2.at[dy])

            @pl.when(core == 1)
            def _():
                send(mixed.at[:, deep], mixed.at[:, deep], s2, r2, dy, partner)
        else:
            other = pl.ds(pl.multiple_of((y * 2 + (1 - core)) * CH, CH), CH)
            all_of(mixed.at[:, other], r2.at[0])
        block = mixed[:, deep]
        for j in range(WIDTH // 256):
            at = pl.ds(j * 256, 256)
            base = full[:, at].astype(f32) if dy == 0 else after[:, at]
            part = base + dot(block, out_w[deep, at])
            after[:, at] = part
            if dy == 2:
                for lanes in (part[:, :128], part[:, 128:]):
                    sums[0] = sums[0] + lanes
                    sums[1] = sums[1] + lanes * lanes
        if dy == OWN_AFTER:
            all_of(own_mixed.at[:, pl.ds(0, 7 * CH)], ro.at[1])
            first_step(own_mixed, mixed_in, MIX // 2, sl, rl)
            mixed_in[e] = own_mixed[...]
    mean = jnp.sum(sums[0], axis=1, keepdims=True) * (1.0 / WIDTH)
    square = jnp.sum(sums[1], axis=1, keepdims=True) * (1.0 / WIDTH)
    scale = lax.rsqrt(square - mean * mean + norm_eps)
    for j in range(WIDTH // 256):
        at = pl.ds(j * 256, 256)
        part = ((after[:, at] - mean) * scale * mid_gain_ref[:, at]).astype(bf16)
        outgoing[:, :, at] = dot(pick, part).astype(bf16).reshape(EP, CAP, 256)

    def send_slots(group):
        for i in range(GROUP * group, min(GROUP * (group + 1), EP - 1)):
            send(outgoing.at[to_peers[i][0]], slots_in.at[i], s3.at[group], r3, group, to_peers[i])

    send_slots(0)
    slots_in[EP - 1] = outgoing[e]
    own_after = after[own_rows, :]
    mean = jnp.sum(own_after, axis=1, keepdims=True) * (1.0 / WIDTH)
    square = jnp.sum(own_after * own_after, axis=1, keepdims=True) * (1.0 / WIDTH)
    own_mid = ((own_after - mean) * lax.rsqrt(square - mean * mean + norm_eps) * mid_gain_ref[...]).astype(bf16)
    fetched("gate_vec")
    gate_vec = jnp.concatenate([gate_vec_ref[i : i + 1, :] for i in range(WIDTH // 128)], axis=1)
    gate_value = jax.nn.sigmoid(
        jnp.sum(own_mid.astype(f32) * gate_vec.astype(f32), axis=1, keepdims=True)
    )
    all_of(slots_in.at[pl.ds(0, GROUP)], s3.at[0])
    send_slots(1)
    second_step(mixed_in, MIX // 2, sl, rl)

    fetched("eg", "eu", "ed")
    halves_of_rows = (pl.ds(0, HALF), pl.ds(HALF, HALF))

    def send_results(first, last, at, k):
        for i in range(first, last):
            send(result.at[i, :, at], returned.at[e, :, at], s5.at[k], r5, k, from_peers[i])

    for group in (0, 1):
        number = min(GROUP, EP - 1 - GROUP * group)
        all_of(slots_in.at[pl.ds(GROUP * group, number)], r3.at[group])
        blocks, rows_at = pl.ds(GROUP * group, GROUP), pl.ds(GROUP * CAP * group, GROUP * CAP)
        rows = slots_in[blocks].reshape(GROUP * CAP, WIDTH)
        for j in range(FF // 256):
            at = pl.ds(j * 256, 256)
            gate_part = dot(rows, eg[:, at])
            up_part = dot(rows, eu[:, at])
            hidden[rows_at, at] = (jax.nn.silu(gate_part) * up_part).astype(bf16)
        for j in range(WIDTH // 256):
            at = pl.ds(j * 256, 256)
            result[blocks, :, at] = dot(hidden[rows_at, :], ed[:, at]).astype(bf16).reshape(GROUP, CAP, 256)
            if group == 1 and j == HALF // 256 - 1:
                send_results(GROUP, EP - 1, halves_of_rows[0], 1)
        if group == 0:
            send_results(0, GROUP, pl.ds(0, WIDTH), 0)

    returned[e] = result[EP - 1]

    fetched("sg", "su", "sd")
    all_of(resid_in.at[pl.ds(0, 12)], re.at[0])
    all_of(mixed_in.at[pl.ds(0, 12)], rl.at[0])
    channels = mixed_in[...].reshape(EP * OWN, MIX)
    sums = [jnp.zeros((EP * OWN, 128), f32), jnp.zeros((EP * OWN, 128), f32)]
    for j in range(WIDTH // 256):
        at = pl.ds(j * 256, 256)
        part = resid_in[:, :, at].reshape(EP * OWN, 256).astype(f32) + dot(channels, out_w[:, at])
        after_in[:, at] = part
        for lanes in (part[:, :128], part[:, 128:]):
            sums[0] = sums[0] + lanes
            sums[1] = sums[1] + lanes * lanes
    mean = jnp.sum(sums[0], axis=1, keepdims=True) * (1.0 / WIDTH)
    square = jnp.sum(sums[1], axis=1, keepdims=True) * (1.0 / WIDTH)
    scale = lax.rsqrt(square - mean * mean + norm_eps)
    for j in range(WIDTH // 256):
        at = pl.ds(j * 256, 256)
        piece[:, at] = ((after_in[:, at] - mean) * scale * mid_gain_ref[:, at]).astype(bf16)
    send_results(GROUP, EP - 1, halves_of_rows[1], 2)
    gate_part = dot(piece[...], sg[...])
    up_part = dot(piece[...], su[...])
    shidden[...] = (jax.nn.silu(gate_part) * up_part).astype(bf16)

    grid = (SIDE, SIDE, OWN)
    direct_cols = pl.ds(2 * PART, WIDTH - 2 * PART)
    parts = ((0, EARLY_COLS), (EARLY_COLS, PART - EARLY_COLS))

    def partial_columns(first, last):
        for begin in range(first, last, 256):
            at = pl.ds(begin, min(256, last - begin))
            partial[:, :, :, at] = dot(shidden[...], sd[:, at]).astype(bf16).reshape(*grid, at.size)

    def first_sums(part):
        begin, size = parts[part]
        at = pl.ds(begin, size)
        left, right = at, pl.ds(PART + begin, size)
        for d, dev, there in z_peers:
            send(partial.at[there, :, :, left], stage_a.at[d - 1, :, :, at], s6.at[0], r6, 2 * part, dev)
        for d, dev, there in x_peers:
            send(partial.at[:, there, :, right], stage_b.at[d - 1, :, :, at], s6.at[1], r6, 2 * part + 1, dev)

    def second_sums(part):
        begin, size = parts[part]
        at = pl.ds(begin, size)
        left, right = at, pl.ds(PART + begin, size)
        all_of(stage_a.at[:, :, :, at], r6.at[2 * part])
        total = partial[z, :, :, left].astype(f32)
        for d in range(3):
            total = total + stage_a[d, :, :, at].astype(f32)
        sum_a[:, :, at] = total.astype(bf16)
        for d, dev, there in x_peers:
            send(sum_a.at[there, :, at], final_a.at[d - 1, :, at], s6f.at[0], r6f, 0, dev)
        all_of(stage_b.at[:, :, :, at], r6.at[2 * part + 1])
        total = partial[:, x, :, right].astype(f32)
        for d in range(3):
            total = total + stage_b[d, :, :, at].astype(f32)
        sum_b[:, :, at] = total.astype(bf16)
        for d, dev, there in z_peers:
            send(sum_b.at[there, :, at], final_b.at[d - 1, :, at], s6f.at[1], r6f, 1, dev)

    for part, (begin, size) in enumerate(parts):
        partial_columns(begin, begin + size)
        partial_columns(PART + begin, PART + begin + size)
        first_sums(part)
    partial_columns(2 * PART, WIDTH)

    def combine_half(half):
        at = halves_of_rows[half]
        if half == 0:
            all_of(returned.at[pl.ds(0, GROUP)], r5.at[0])
        all_of(returned.at[pl.ds(0, EP - 1 - GROUP), :, at], r5.at[1 + half])
        for begin in range(0, HALF, 256):
            part_at = pl.ds(half * HALF + begin, 256)
            back = returned[:, :, part_at].reshape(SLOTS, 256)
            part = dot(comb_hi, back) + dot(comb_lo, back)
            routed_part[:, :, :, part_at] = part.astype(bf16).reshape(SIDE, 2, OWN, 256)
        send(routed_part.at[:, 1 - core, :, at], core_in.at[:, :, at], s7.at[0], r7, half, partner)

    def sum_over_tp(half):
        at = halves_of_rows[half]
        all_of(core_in.at[:, :, at], r7.at[half])
        core_sum[:, :, at] = (
            routed_part[:, core, :, at].astype(f32) + core_in[:, :, at].astype(f32)
        ).astype(bf16)
        for d, dev, there in y_peers:
            send(core_sum.at[there, :, at], routed_in.at[d - 1, :, at], s7.at[1], r7, 2, dev)

    def send_direct():
        for i, (dz, dx) in enumerate(OFFSETS):
            to_z, to_x = (z + dz) % SIDE, (x + dx) % SIDE
            send(
                partial.at[to_z, to_x, :, direct_cols], direct_in.at[i], s6d, r6d, 0,
                (to_z * SIDE + to_x, t),
            )

    combine_half(0)

    @pl.when(core == 0)
    def _():
        sum_over_tp(0)

    combine_half(1)

    @pl.when(core == 1)
    def _():
        second_sums(0)
        send_direct()
        sum_over_tp(0)

    sum_over_tp(1)

    @pl.when(core == 0)
    def _():
        send_direct()
        second_sums(0)

    second_sums(1)
    all_of(routed_in, r7.at[2])
    routed = core_sum[y].astype(f32) + jnp.sum(routed_in[...].astype(f32), axis=0) + after[own_rows, :]
    all_of(final_a, r6f.at[0])
    all_of(final_b, r6f.at[1])
    all_of(direct_in, r6d.at[0])
    own_direct = partial[z, x, :, direct_cols]
    for at, own, others in (
        (pl.ds(0, PART), sum_a[x], final_a), (pl.ds(PART, PART), sum_b[z], final_b),
        (direct_cols, own_direct, direct_in),
    ):
        shared = own.astype(f32) + jnp.sum(others[...].astype(f32), axis=0)
        begin, size = at.start, at.size
        out_ref[:, at] = (routed[:, begin : begin + size] + gate_value * shared).astype(bf16)

    all_of(own_resid.at[:, pl.ds(0, 7 * FEAT)], so.at[0])
    all_of(own_mixed.at[:, pl.ds(0, 7 * CH)], so.at[1])
    all_of(full.at[:, pl.ds(0, 4 * FEAT)], s1)
    all_of(mixed.at[:, pl.ds(0, 4 * CH)], s2)

    @pl.when(core == 1)
    def _():
        all_of(mixed.at[:, pl.ds(0, 6 * CH)], s2)

    all_of(resid_in.at[pl.ds(0, 15)], se)
    all_of(mixed_in.at[pl.ds(0, 15)], sl)
    all_of(slots_in.at[pl.ds(0, EP - 1 - GROUP)], s3.at[1])
    all_of(returned.at[pl.ds(0, GROUP)], s5.at[0])
    all_of(stage_a, s6.at[0])
    all_of(stage_b, s6.at[1])
    all_of(final_a, s6f.at[0])
    all_of(final_b, s6f.at[1])
    for half, at in enumerate(halves_of_rows):
        all_of(returned.at[pl.ds(0, EP - 1 - GROUP), :, at], s5.at[1 + half])
    all_of(direct_in, s6d)
    all_of(core_in, s7.at[0])
    all_of(routed_in, s7.at[1])


def write_out(out_ref, state_ref, out_hbm, state_hbm, sem):
    copies = [
        pltpu.make_async_copy(state_ref, state_hbm, sem.at[0]),
        pltpu.make_async_copy(out_ref, out_hbm, sem.at[1]),
    ]
    for c in copies:
        c.start()
    for c in copies:
        c.wait()


def per_device(
    residual, in_gain, in_weight, state, decay_rate, frequency, log_step, in_coef, out_coef,
    skip_gain, out_weight, mid_gain, gate_vector, routes, route_weight, expert_gate, expert_up,
    expert_down, shared_gate, shared_up, shared_down,
):
    vmem = pl.BlockSpec(memory_space=pltpu.VMEM)
    hbm = pl.BlockSpec(memory_space=pltpu.HBM)
    dma = pltpu.SemaphoreType.DMA
    in_coef_rows = jnp.swapaxes(in_coef, 2, 3).reshape(2, CH, STATE)
    out_coef_rows = out_coef.reshape(2, CH, STATE)
    call = pl.pallas_call(
        kernel,
        name="layer_step",
        out_shape=(
            pltpu.VMEM((OWN, WIDTH), bf16),
            pltpu.VMEM((2, ROWS, GS), f32),
        ),
        in_specs=[hbm] * 21,
        out_specs=(vmem, vmem),
        scratch_shapes=[
            pltpu.VMEM((ROWS, FEAT), bf16),
            pltpu.VMEM((1, WIDTH), f32),
            pltpu.VMEM((GROUPS, STATE), f32),
            pltpu.VMEM((GROUPS, STATE), f32),
            pltpu.VMEM((1, GROUPS), f32),
            pltpu.VMEM((2, CH, STATE), f32),
            pltpu.VMEM((2, CH, STATE), f32),
            pltpu.VMEM((1, CH), f32),
            pltpu.VMEM((1, WIDTH), f32),
            pltpu.VMEM((WIDTH // 128, 128), bf16),
            pltpu.VMEM((4, ROWS), jnp.int32),
            pltpu.VMEM((4, ROWS), f32),
            pltpu.VMEM((ROWS, WIDTH), bf16),
            pltpu.VMEM((WIDTH, CH), bf16),
            pltpu.VMEM((2, ROWS, GS), f32),
            pltpu.VMEM((MIX, WIDTH), bf16),
            pltpu.VMEM((WIDTH, FF), bf16),
            pltpu.VMEM((WIDTH, FF), bf16),
            pltpu.VMEM((FF, WIDTH), bf16),
            pltpu.VMEM((WIDTH, SF), bf16),
            pltpu.VMEM((WIDTH, SF), bf16),
            pltpu.VMEM((SF, WIDTH), bf16),
            pltpu.VMEM((OWN, WIDTH), bf16),
            pltpu.VMEM((OWN, MIX), bf16),
            pltpu.VMEM((ROWS, MIX), bf16),
            pltpu.VMEM((ROWS, WIDTH), f32),
            pltpu.VMEM((EP, CAP, WIDTH), bf16),
            pltpu.VMEM((EP, CAP, WIDTH), bf16),
            pltpu.VMEM((EP, OWN, WIDTH), bf16),
            pltpu.VMEM((EP, OWN, MIX), bf16),
            pltpu.VMEM((EP * OWN, WIDTH), f32),
            pltpu.VMEM((EP * OWN, WIDTH), bf16),
            pltpu.VMEM((SLOTS, FF), bf16),
            pltpu.VMEM((EP, CAP, WIDTH), bf16),
            pltpu.VMEM((EP, CAP, WIDTH), bf16),
            pltpu.VMEM((EP * OWN, SF), bf16),
            pltpu.VMEM((SIDE, SIDE, OWN, WIDTH), bf16),
            pltpu.VMEM((SIDE - 1, SIDE, OWN, PART), bf16),
            pltpu.VMEM((SIDE - 1, SIDE, OWN, PART), bf16),
            pltpu.VMEM((SIDE, OWN, PART), bf16),
            pltpu.VMEM((SIDE, OWN, PART), bf16),
            pltpu.VMEM((SIDE - 1, OWN, PART), bf16),
            pltpu.VMEM((SIDE - 1, OWN, PART), bf16),
            pltpu.VMEM((EP - 1, OWN, WIDTH - 2 * PART), bf16),
            pltpu.VMEM((SIDE, 2, OWN, WIDTH), bf16),
            pltpu.VMEM((SIDE, OWN, WIDTH), bf16),
            pltpu.VMEM((SIDE, OWN, WIDTH), bf16),
            pltpu.VMEM((SIDE - 1, OWN, WIDTH), bf16),
            dma((21,)),
            dma((2,)), dma((2,)),
            dma, dma((8,)),
            dma, dma((4,)),
            dma, dma((8,)),
            dma, dma((8,)),
            dma((2,)), dma((2,)),
            dma((3,)), dma((3,)),
            dma((2,)), dma((4,)),
            dma, dma((1,)),
            dma((2,)), dma((2,)),
            dma((2,)), dma((3,)),
        ],
        compiler_params=pltpu.CompilerParams(
            collective_id=0, has_side_effects=True, vmem_limit_bytes=VMEM_MIB * 1024 * 1024
        ),
    )
    operands = (
        residual, in_gain.reshape(1, WIDTH), in_weight, state, decay_rate, frequency,
        log_step.reshape(1, GROUPS), in_coef_rows, out_coef_rows, skip_gain.reshape(1, CH),
        out_weight, mid_gain.reshape(1, WIDTH), gate_vector.reshape(WIDTH // 128, 128), routes.T,
        route_weight.T, expert_gate[0], expert_up[0], expert_down[0], shared_gate, shared_up,
        shared_down,
    )
    results = call(*[pltpu.with_memory_space_constraint(a, pltpu.HBM) for a in operands])
    return pl.pallas_call(
        write_out,
        name="write_out",
        out_shape=(
            jax.ShapeDtypeStruct((OWN, WIDTH), bf16),
            jax.ShapeDtypeStruct((2, ROWS, GS), f32),
        ),
        in_specs=[vmem, vmem],
        out_specs=(hbm, hbm),
        scratch_shapes=[dma((2,))],
    )(*[pltpu.with_memory_space_constraint(a, pltpu.VMEM) for a in results])


def solution(mesh):
    return jax.shard_map(
        per_device,
        mesh=mesh,
        in_specs=(
            P("ep", "tp"), P(), P(None, "tp"), P(None, "ep", "tp"), P("tp", None), P("tp", None),
            P("tp"), P(None, "tp", None, None), P(None, "tp", None, None), P("tp"), P(), P(), P(),
            P("ep", None), P("ep", None), P(("ep", "tp"), None, None), P(("ep", "tp"), None, None),
            P(("ep", "tp"), None, None), P(None, "ep"), P(None, "ep"), P("ep", None),
        ),
        out_specs=(P(("ep", "tp"), None), P(None, "ep", "tp")),
        check_vma=False,
    )
```
